512 devices in a mesh: sp: 64 (over z, y), tp: 8 (over x, core).
Axes of the slice: x: 4, y: 8, z: 8, core: 2. Of those that a mesh axis runs over, the one named last changes fastest.
Arguments:
- tokens_in: bfloat16 [16384, 2048], P('sp', 'tp'), may hold values from -400 to 400
- norm_gain: float32 [2048], replicated, may hold values from 0.1 to 1.9
- w_query: bfloat16 [2048, 1024], P('sp', 'tp'), may hold values from -0.125 to 0.125
- w_forget: bfloat16 [2048, 1024], P('sp', 'tp'), may hold values from -0.125 to 0.125
- w_input: bfloat16 [2048, 1024], P('sp', 'tp'), may hold values from -0.125 to 0.125
- w_rgate: bfloat16 [2048, 1024], P('sp', 'tp'), may hold values from -0.125 to 0.125
- w_pool_in: bfloat16 [2048, 1024], P('sp', 'tp'), may hold values from -0.125 to 0.125
- w_pgate: bfloat16 [2048, 1024], P('sp', 'tp'), may hold values from -0.125 to 0.125
- floor_rate: float32 [1024], P('tp'), as said below
- extra_logdecay: float32 [16384, 8], P('sp', 'tp'), as said below
- state_gain: float32 [1024], P('tp'), may hold values from 0.1 to 1.9
- pool_mix: bfloat16 [8, 128, 128], P('tp'), may hold values from -0.5 to 0.5
- pool_gain: float32 [1024], P('tp'), may hold values from 0.1 to 1.9
- out_rec: bfloat16 [1024, 2048], P('tp', 'sp'), may hold values from -0.125 to 0.125
- out_pool: bfloat16 [1024, 2048], P('tp', 'sp'), may hold values from -0.125 to 0.125
- post_gain: float32 [2048], replicated, may hold values from 0.1 to 1.9
Outputs:
- mixed_out: bfloat16 [16384, 2048], P(('sp', 'tp'))
The draws below stay inside these ranges and needn't reach their ends.
Inputs may be any that keep to these rules, and one draw needn't show every extreme that they name: `floor_rate`: every entry is positive. `extra_logdecay`: every entry is at most zero.
All inputs are finite; a program needn't handle non-finite values.
Results may differ from the reference program's by a relative error of at most 0.015.
Values may be sent and summed in bfloat16 or wider, within the bound.
A program may use at most 64 MiB of HBM per device.

```python
import math
import jax
import jax.numpy as jnp
from jax import lax

D = 2048
HEADS = 8
DK = 128
BLOCK = 64
TOK_DEV = 256
W = 1024
TOKENS = 16384
N_TP = 8


def draw_tokens_in(key, part):
    first, second, third = jax.random.split(jax.random.fold_in(key, 3), 3)
    row_scale = jnp.exp(jax.random.uniform(first, (TOKENS, 1), jnp.float32) * math.log(10.0))
    col_scale = jnp.exp(jax.random.uniform(second, (1, D), jnp.float32) * math.log(10.0))
    starting_shift_amount = jax.random.normal(third, (TOKENS, D), jnp.float32)
    starting_shift_amount = jnp.clip(starting_shift_amount, -4.0, 4.0)
    return (starting_shift_amount * row_scale * col_scale).astype(jnp.bfloat16)


def draw_floor_rate(key, part):
    first, second = jax.random.split(jax.random.fold_in(key, 11), 2)
    ranks = jax.random.permutation(first, HEADS)
    uniform = jax.random.uniform(second, (HEADS, DK), jnp.float32)
    kind = jnp.where(ranks < HEADS // 4, 0, jnp.where(ranks < HEADS // 2, 1, 2))
    fast = jnp.exp(math.log(0.02) + uniform * math.log(4.0))
    medium_low = min(1.0 / TOK_DEV, 0.01)
    medium = jnp.exp(math.log(medium_low) + uniform * math.log(8.0))
    slow = jnp.exp(jnp.log(0.3 / TOKENS) + uniform * math.log(4.0 / 0.3))
    rate = jnp.where(kind[:, None] == 0, fast, jnp.where(kind[:, None] == 1, medium, slow))
    rate = jnp.minimum(rate, 0.08)
    return rate.reshape(HEADS * DK).astype(jnp.float32)


def draw_extra_logdecay(key, part):
    first, second, third = jax.random.split(jax.random.fold_in(key, 17), 3)
    devices = TOKENS // TOK_DEV
    factor = jnp.exp(math.log(0.3) + jax.random.uniform(first, (devices,), jnp.float32) * math.log(10.0))
    starting_shift_amount = -jnp.repeat(factor, TOK_DEV)[:, None] / TOKENS * jnp.ones((1, HEADS), jnp.float32)
    averaging_locations = jax.random.randint(second, (4, HEADS), 0, TOKENS)
    sigmoid_weighting = jnp.log(jax.random.uniform(third, (4, HEADS), jnp.float32, 0.5, 0.8))
    sequence_step_number = jnp.arange(TOKENS)[:, None, None]
    packet_clusters = jnp.sum(jnp.where(sequence_step_number == averaging_locations[None, :, :], sigmoid_weighting[None, :, :], 0.0), axis=1)
    return (starting_shift_amount + packet_clusters).astype(jnp.float32)


def shard_levels(rng, dims, pieces, least, largest):
    gain = 1.0
    for axis_at, blocks in pieces:
        heights = jax.random.uniform(jax.random.fold_in(jax.random.fold_in(rng, 6), axis_at), (blocks,), jnp.float32, least / len(pieces), largest / len(pieces))
        gain = gain * jnp.repeat(jnp.exp(heights), dims[axis_at] // blocks).reshape((-1,) + (1,) * (len(dims) - 1 - axis_at))
    return gain


def normal_values(rng, dims, width, bound, cuts=(), held_as=jnp.bfloat16):
    drawn = jax.random.normal(rng, dims, jnp.float32) * width
    if len(cuts) > 0:
        drawn = shard_levels(rng, dims, cuts, -0.22, 0.18) * drawn
    return jnp.clip(drawn, min=-bound, max=bound).astype(held_as)


def setup_inputs(seed: int = 0) -> dict:
    arg_keys = jax.random.split(jax.random.key(seed), 17)
    return {
        "tokens_in": draw_tokens_in(jax.random.fold_in(arg_keys[16], 71), 0),
        "norm_gain": jnp.clip(1.0 + 0.18 * jax.random.normal(arg_keys[1], (D,), jnp.float32), 0.1, 1.9),
        "w_query": normal_values(arg_keys[2], (D, W), D ** -0.5, 0.125, ((0, 64), (1, 8))),
        "w_forget": normal_values(arg_keys[3], (D, W), D ** -0.5, 0.125, ((0, 64), (1, 8))),
        "w_input": normal_values(arg_keys[4], (D, W), D ** -0.5, 0.125, ((0, 64), (1, 8))),
        "w_rgate": normal_values(arg_keys[5], (D, W), D ** -0.5, 0.125, ((0, 64), (1, 8))),
        "w_pool_in": normal_values(arg_keys[6], (D, W), D ** -0.5, 0.125, ((0, 64), (1, 8))),
        "w_pgate": normal_values(arg_keys[7], (D, W), D ** -0.5, 0.125, ((0, 64), (1, 8))),
        "floor_rate": draw_floor_rate(jax.random.fold_in(arg_keys[16], 71), 0),
        "extra_logdecay": draw_extra_logdecay(jax.random.fold_in(arg_keys[16], 71), 0),
        "state_gain": jnp.clip(1.0 + 0.18 * jax.random.normal(arg_keys[10], (W,), jnp.float32), 0.1, 1.9),
        "pool_mix": normal_values(arg_keys[11], (HEADS, DK, DK), DK ** -0.5, 0.5, ((0, 8),)),
        "pool_gain": jnp.clip(1.0 + 0.18 * jax.random.normal(arg_keys[12], (W,), jnp.float32), 0.1, 1.9),
        "out_rec": normal_values(arg_keys[13], (W, D), (2 * W) ** -0.5, 0.125, ((0, 8), (1, 64))),
        "out_pool": normal_values(arg_keys[14], (W, D), (2 * W) ** -0.5, 0.125, ((0, 8), (1, 64))),
        "post_gain": jnp.clip(1.0 + 0.18 * jax.random.normal(arg_keys[15], (D,), jnp.float32), 0.1, 1.9),
    }


eps = 1e-06
coarsest_scale_depth = lax.Precision.HIGHEST

def recurrence(query, key_gate, inputs, log_forget):
    blocks = TOKENS // BLOCK

    def to_blocks(array):
        return array.reshape(blocks, BLOCK, HEADS, DK).transpose(0, 2, 1, 3)
    causal = jnp.arange(BLOCK)[:, None] >= jnp.arange(BLOCK)[None, :]

    def advance(carried_memory_matrix, member):
        probe_segment, key_piece, input_piece, gc = member
        prefix_sum_vector = jnp.cumsum(gc, axis=1)
        last_index = prefix_sum_vector[:, -1]
        cross_segment_contribution = jnp.einsum('abz,azy->aby', probe_segment * jnp.exp(prefix_sum_vector), carried_memory_matrix, precision=coarsest_scale_depth)
        diff = prefix_sum_vector[:, :, None, :] - prefix_sum_vector[:, None, :, :]
        weight = jnp.where(causal[None, :, :, None], jnp.exp(jnp.minimum(diff, 0.0)), 0.0)
        scores = jnp.einsum('htk,hsk,htsk->hts', probe_segment, key_piece, weight, precision=coarsest_scale_depth)
        final_result = cross_segment_contribution + jnp.einsum('hts,hsv->htv', scores, input_piece, precision=coarsest_scale_depth)
        carried_memory_matrix = jnp.exp(last_index)[..., None] * carried_memory_matrix + jnp.einsum('njp,njq->npq', key_piece * jnp.exp(last_index[:, None, :] - prefix_sum_vector), input_piece, precision=coarsest_scale_depth)
        return (carried_memory_matrix, final_result)
    start = jnp.zeros((HEADS, DK, DK), jnp.float32)
    qs = query.astype(jnp.float32) * DK ** (-0.5)
    _, final_result = lax.scan(advance, start, (to_blocks(qs), to_blocks(key_gate), to_blocks(inputs.astype(jnp.float32)), to_blocks(log_forget)))
    return final_result.transpose(0, 2, 1, 3).reshape(TOKENS, HEADS * DK)

def reference(tokens_in, norm_gain, w_query, w_forget, w_input, w_rgate, w_pool_in, w_pgate, floor_rate, extra_logdecay, state_gain, pool_mix, pool_gain, out_rec, out_pool, post_gain):
    wide = tokens_in.astype(jnp.float32)
    inv_rms = lax.rsqrt(lax.optimization_barrier(jnp.mean(wide * wide, axis=1, keepdims=True)) + eps)
    scaled = (wide * norm_gain).astype(jnp.bfloat16)

    def project(weight):
        return (jnp.dot(scaled, weight, preferred_element_type=jnp.float32) * inv_rms).astype(jnp.bfloat16)
    query = project(w_query)
    forget = project(w_forget)
    inputs = project(w_input)
    rgate = project(w_rgate)
    pool_in = project(w_pool_in)
    pgate = project(w_pgate)
    forget32 = forget.astype(jnp.float32)
    key_gate = -jnp.expm1(-floor_rate)[None, :] * jax.nn.sigmoid(-forget32)
    log_forget = jnp.log1p(-key_gate) + jnp.repeat(extra_logdecay, DK, axis=1)
    recurrent_output = recurrence(query, key_gate, inputs, log_forget)
    grouped = recurrent_output.reshape(TOKENS, HEADS, DK)
    normed = grouped * lax.rsqrt(lax.optimization_barrier(jnp.mean(grouped * grouped, axis=2, keepdims=True)) + eps)
    y_rec = (normed.reshape(TOKENS, HEADS * DK) * state_gain * jax.nn.silu(rgate.astype(jnp.float32))).astype(jnp.bfloat16)
    group = (jnp.arange(HEADS * DK) // DK).astype(jnp.int32)
    window = jnp.power(2, 1 + group % 4).astype(jnp.int32)
    pool32 = pool_in.astype(jnp.float32)
    extended = jnp.concatenate([jnp.zeros((16, HEADS * DK), jnp.float32), pool32], axis=0)
    total = jnp.zeros((TOKENS, HEADS * DK), jnp.float32)
    for offset in range(16):
        rows_back = extended[16 - offset:16 - offset + TOKENS]
        total = total + jnp.where((offset < window)[None, :], rows_back, 0.0)
    sequence_step_number = jnp.arange(TOKENS).astype(jnp.int32)
    count = jnp.minimum(sequence_step_number[:, None] + 1, window[None, :]).astype(jnp.float32)
    mixed = (total / count - pool32).astype(jnp.bfloat16)
    mapped = jnp.einsum('tgc,gcd->tgd', mixed.reshape(TOKENS, HEADS, DK).astype(jnp.float32), pool_mix.astype(jnp.float32)).reshape(TOKENS, HEADS * DK)
    y_pool = (mapped * pool_gain * jax.nn.silu(pgate.astype(jnp.float32))).astype(jnp.bfloat16)
    share = HEADS * DK // N_TP
    summed = jnp.zeros((TOKENS, D), jnp.float32)
    for member in range(N_TP):
        lower = member * share
        left = jnp.concatenate([y_rec[:, lower:lower + share], y_pool[:, lower:lower + share]], axis=1)
        right = jnp.concatenate([out_rec[lower:lower + share], out_pool[lower:lower + share]], axis=0)
        partial_sum = jnp.dot(left, right, preferred_element_type=jnp.float32).astype(jnp.bfloat16)
        summed = summed + partial_sum.astype(jnp.float32)
    final = summed * lax.rsqrt(lax.optimization_barrier(jnp.mean(summed * summed, axis=1, keepdims=True)) + eps) * post_gain
    return final.astype(jnp.bfloat16)
```

```python
import functools

import jax
import jax.numpy as jnp
from jax import lax
from jax.experimental import pallas as pl
from jax.experimental.pallas import tpu as pltpu
from jax.sharding import Mesh
from jax.sharding import PartitionSpec as P

SP = ("sp_0", "sp_1")
TP = ("tp_0", "tp_1")
SP_TP = ("sp_0", "sp_1", "tp_0", "tp_1")
Z, Y, X, C = "sp_0", "sp_1", "tp_0", "tp_1"
MESH = pl.DeviceIdType.MESH
EPS = 1e-06
DK = 128
NR = 8
NX = 4
T = 256
D = 2048
OWN = T // (2 * NX)
F32 = jnp.float32
BF16 = jnp.bfloat16
ORDER = (4, 3, 5, 2, 6, 1, 7)


def mm(a, b, ca=1, cb=0):
    return lax.dot_general(a, b, (((ca,), (cb,)), ((), ())), preferred_element_type=F32)


def halves(a):
    hi = a.astype(BF16)
    return hi, (a - hi.astype(F32)).astype(BF16)


def mm3(a, b, ca=1, cb=0):
    ah, al = halves(a)
    bh, bl = halves(b)
    return mm(ah, bh, ca, cb) + (mm(ah, bl, ca, cb) + mm(al, bh, ca, cb))


def mm2(a, b, ca=1, cb=0):
    ah, al = halves(a)
    return mm(ah, b, ca, cb) + mm(al, b, ca, cb)


def silu(a):
    return a / (1.0 + jnp.exp(-a))


def around(value, count):
    return lax.rem(value + 2 * count, count)


class Ring:
    def __init__(self, part, axis, me, sign, send, recv):
        self.part, self.axis, self.me, self.sign, self.send, self.recv = part, axis, me, sign, send, recv

    def copy(self, step, back, origin):
        sign = -self.sign if back else self.sign
        at = NR // 2 + step if back else step
        block = self.part(origin)
        return pltpu.make_async_remote_copy(
            src_ref=block,
            dst_ref=block,
            send_sem=self.send.at[at],
            recv_sem=self.recv.at[at],
            device_id={self.axis: around(self.me + sign, NR)},
            device_id_type=MESH,
        )

    def origin(self, step, back):
        sign = -self.sign if back else self.sign
        return around(self.me - sign * step, NR)

    def steps(self, back):
        return NR // 2 - 1 if back else NR // 2

    def start(self, step):
        for back in (False, True):
            if step < self.steps(back):
                self.copy(step, back, self.origin(step, back)).start()

    def arrive(self, step):
        for back in (False, True):
            if step < self.steps(back):
                self.copy(step, back, self.origin(step + 1, back)).wait_recv()

    def drain(self):
        for back in (False, True):
            for step in range(self.steps(back)):
                self.copy(step, back, self.origin(step, back)).wait_send()


class Direct:
    def __init__(self, part, axis, me, send, recv):
        self.part, self.axis, self.me, self.send, self.recv = part, axis, me, send, recv

    def copy(self, distance, origin):
        block = self.part(origin)
        return pltpu.make_async_remote_copy(
            src_ref=block,
            dst_ref=block,
            send_sem=self.send.at[distance],
            recv_sem=self.recv.at[distance],
            device_id={self.axis: around(self.me + distance, NR)},
            device_id_type=MESH,
        )

    def start(self):
        for distance in ORDER:
            self.copy(distance, self.me).start()

    def arrive(self):
        for distance in range(1, NR):
            self.copy(distance, around(self.me - distance, NR)).wait_recv()

    def drain(self):
        for distance in range(1, NR):
            self.copy(distance, self.me).wait_send()


def layer(
    tok, wq, wf, wi, wr, wp, wg, orec, opool,
    ngain, rate, extra, sgain, pmix, pgain, post,
    out,
    g0a, g0b, g1a, g1b, g2a, g2b, xg, sc,
    st1, st2, rows_out, rows_in, yb, sib_out, sib_in, red_out, red_in,
    lsem, p1s, p1r, p2s, p2r, ts, tr, ss, sr, ps, pr, bs, br, xs, xr,
):
    z, y, x, c = lax.axis_index(Z), lax.axis_index(Y), lax.axis_index(X), lax.axis_index(C)
    tp = 2 * x + c
    sign = 1 - 2 * c
    other = 1 - c

    local = [
        pltpu.make_async_copy(src, dst, lsem.at[k])
        for k, (src, dst) in enumerate(
            (
                (wf, g0a.at[z, y]),
                (wi, g0b.at[z, y]),
                (tok, xg.at[tp]),
                (wq, g1a.at[z, y, :, 0:DK]),
                (wr, g1a.at[z, y, :, DK : 2 * DK]),
                (wp, g1b.at[z, y, :, 0:DK]),
                (wg, g1b.at[z, y, :, DK : 2 * DK]),
                (orec, g2a.at[z, y]),
                (opool, g2b.at[z, y]),
            )
        )
    ]
    for copy in local:
        copy.start()

    after_y = around(y + 1, NR)
    after_z = jnp.where(y == NR - 1, around(z + 1, NR), z)
    before_y = around(y - 1, NR)
    before_z = jnp.where(y == 0, around(z - 1, NR), z)
    barrier = pltpu.get_barrier_semaphore()
    for k in range(1, NR):
        pl.semaphore_signal(barrier, 1, device_id={Y: around(y + k, NR)}, device_id_type=MESH)
        pl.semaphore_signal(barrier, 1, device_id={Z: around(z + k, NR)}, device_id_type=MESH)
    for k in range(1, NX):
        pl.semaphore_signal(barrier, 1, device_id={X: around(x + k, NX)}, device_id_type=MESH)
    pl.semaphore_signal(barrier, 1, device_id={C: other}, device_id_type=MESH)
    pl.semaphore_signal(barrier, 1, device_id={Z: before_z, Y: before_y}, device_id_type=MESH)
    pl.semaphore_wait(barrier, 2 * (NR - 1) + NX - 1 + 2)

    groups = ((g0a, g0b), (g1a, g1b), (g2a, g2b))
    first, second = [], []
    for k, (ga, gb) in enumerate(groups):
        first.append(Direct(lambda o, g=ga: g.at[z, o], Y, y, p1s.at[2 * k], p1r.at[2 * k]))
        first.append(Direct(lambda o, g=gb: g.at[o, y], Z, z, p1s.at[2 * k + 1], p1r.at[2 * k + 1]))
        second.append(Ring(lambda o, g=ga: g.at[o], Z, z, sign, p2s.at[2 * k], p2r.at[2 * k]))
        second.append(
            Ring(lambda o, g=gb: g.at[:, o], Y, y, sign, p2s.at[2 * k + 1], p2r.at[2 * k + 1])
        )

    def tok_copy(at, slot, where):
        return pltpu.make_async_remote_copy(
            src_ref=xg.at[slot],
            dst_ref=xg.at[slot],
            send_sem=ts.at[at],
            recv_sem=tr.at[at],
            device_id=where,
            device_id_type=MESH,
        )

    def tok_out(distance):
        return tok_copy(distance, tp, {X: around(x + distance, NX)})

    def tok_from(distance):
        return 2 * around(x - distance, NX)

    local[0].wait()
    first[0].start()
    local[1].wait()
    first[1].start()
    local[2].wait()
    for distance in (2, 1, 3):
        tok_out(distance).start()
    tok_copy(0, tp, {C: other}).start()
    for k in range(3, 7):
        local[k].wait()
    first[2].start()
    first[3].start()

    first[0].arrive()
    second[0].start(0)
    first[1].arrive()
    second[1].start(0)
    for k in range(7, 9):
        local[k].wait()
    first[2].arrive()
    second[2].start(0)
    first[3].arrive()
    second[3].start(0)
    first[4].start()
    first[5].start()

    def relay(group, step):
        for ring in second[2 * group : 2 * group + 2]:
            ring.arrive(step)
            if step + 1 < NR // 2:
                ring.start(step + 1)

    for distance in (1, 3, 2):
        tok_copy(distance, tok_from(distance) + c, {X: around(x + distance, NX)}).wait_recv()
        tok_copy(NX + distance, tok_from(distance) + c, {C: other}).start()
    relay(0, 0)
    tok_copy(0, 2 * x + other, {C: other}).wait_recv()
    for distance in range(1, NX):
        tok_copy(NX + distance, tok_from(distance) + other, {C: other}).wait_recv()
    squares = jnp.zeros((T, 1), F32)
    for k in range(2 * NX):
        block = xg[k].astype(F32)
        squares = squares + jnp.sum(block * block, axis=1, keepdims=True)
        at = slice(k * (D // (2 * NX)), (k + 1) * (D // (2 * NX)))
        sc[:, at] = (block * ngain[:, at]).astype(BF16)
    inv_rms = lax.rsqrt(squares * (1.0 / D) + EPS)
    relay(1, 0)
    relay(0, 1)
    relay(1, 1)
    relay(0, 2)
    relay(1, 2)
    first[4].arrive()
    second[4].start(0)
    first[5].arrive()
    second[5].start(0)
    relay(0, 3)

    scaled = sc[...]
    forget = (mm(scaled, g0a[...].reshape(D, DK)) * inv_rms).astype(BF16).astype(F32)
    value = (mm(scaled, g0b[...].reshape(D, DK)) * inv_rms).astype(BF16)
    r = rate[...]
    series = r * (1.0 - r / 2 * (1.0 - r / 3 * (1.0 - r / 4 * (1.0 - r / 5 * (1.0 - r / 6)))))
    reach = jnp.where(r < 0.1, series, 1.0 - jnp.exp(-r))
    key = reach * (1.0 / (1.0 + jnp.exp(forget)))
    more = lax.dot_general(
        extra[...],
        jnp.ones((1, DK), F32),
        (((0,), (0,)), ((), ())),
        precision=lax.Precision.HIGHEST,
        preferred_element_type=F32,
    )
    logs = jnp.log1p(-key) + more
    row = lax.broadcasted_iota(jnp.int32, (T, T), 0)
    col = lax.broadcasted_iota(jnp.int32, (T, T), 1)
    lower = jnp.where(row >= col, 1.0, 0.0)
    cum = jnp.dot(lower, logs, precision=lax.Precision.HIGHEST, preferred_element_type=F32)
    last = cum[T - 1 : T, :]
    memory = mm2(key * jnp.exp(last - cum), value, 0, 0).T

    def to_message(state, total):
        hi = total.astype(BF16)
        rest = total - hi.astype(F32)
        mid = rest.astype(BF16)
        low = (rest - mid.astype(F32)).astype(BF16)
        place = lax.broadcasted_iota(jnp.int32, (16, DK), 0)
        parts = jnp.where(
            place == 0,
            hi.astype(F32),
            jnp.where(place == 1, mid.astype(F32), jnp.where(place == 2, low.astype(F32), 0.0)),
        )
        return jnp.concatenate([state.astype(BF16), parts.astype(BF16)], axis=0)

    def from_message(ref, k):
        whole = ref[k].astype(F32)
        return whole[:DK], jnp.sum(whole[DK:], axis=0, keepdims=True)

    st1[y] = to_message(memory, last)
    over_y = Direct(lambda o: st1.at[o], Y, y, ss.at[0], sr.at[0])
    over_y.start()
    relay(1, 3)

    qr = mm(scaled, g1a[...].reshape(D, 2 * DK)) * inv_rms
    query = qr[:, :DK].astype(BF16).astype(F32) * DK ** (-0.5)
    rgate = qr[:, DK:].astype(BF16).astype(F32)
    pp = mm(scaled, g1b[...].reshape(D, 2 * DK)) * inv_rms
    pool = pp[:, :DK].astype(BF16)
    pgate = pp[:, DK:].astype(BF16).astype(F32)
    rows_out[...] = pool[T - 16 :, :]
    shift = pltpu.make_async_remote_copy(
        src_ref=rows_out,
        dst_ref=rows_in,
        send_sem=ps.at[0],
        recv_sem=pr.at[0],
        device_id={Z: after_z, Y: after_y},
        device_id_type=MESH,
    )
    shift.start()
    relay(2, 0)

    value32 = value.astype(F32)
    in_block = lax.rem(lax.broadcasted_iota(jnp.int32, (T, 1), 0), 8)
    decay = jnp.exp(logs)
    weight = query
    rec = jnp.sum(query * key, axis=1, keepdims=True) * value32
    for d in range(1, 8):
        weight = weight * (decay if d == 1 else pltpu.roll(decay, d - 1, 0))
        score = jnp.sum(weight * pltpu.roll(key, d, 0), axis=1, keepdims=True)
        rec = rec + jnp.where(in_block >= d, score, 0.0) * pltpu.roll(value32, d, 0)
    relay(2, 1)
    scores = jnp.zeros((T, T), F32)
    for half in (8, 16, 32, 64, 128):
        apart = cum.reshape(T // (2 * half), 2 * half, DK)
        apart = jnp.abs(apart - apart[:, half - 1 : half, :]).reshape(T, DK)
        fade = jnp.exp(-apart)
        level = mm3(query * fade, key * fade, 1, 1)
        mask = (row // (2 * half) == col // (2 * half)) & (row // half > col // half)
        scores = jnp.where(mask, level, scores)
    rec = rec + mm2(scores, value)

    def chain(ref, place, count):
        state, total = jnp.zeros((DK, DK), F32), jnp.zeros((1, DK), F32)
        inside, before = state, total
        for k in range(count):
            new_state, new_total = from_message(ref, k)
            state = jnp.exp(new_total) * state + new_state
            total = total + new_total
            inside = jnp.where(k < place, state, inside)
            before = jnp.where(k < place, total, before)
        return state, total, inside, before

    over_y.arrive()
    state, total, inside, before = chain(st1, y, NR)
    st2[z] = to_message(state, total)
    over_z = Direct(lambda o: st2.at[o], Z, z, ss.at[1], sr.at[1])
    over_z.start()
    relay(2, 2)

    shift.wait_recv()
    at_start = (z == 0) & (y == 0)
    earlier = jnp.where(at_start, 0.0, rows_in[...].astype(F32))
    pool32 = pool.astype(F32)
    two = jnp.concatenate([earlier, pool32], axis=0)
    two = two + pltpu.roll(two, 1, 0)
    four = two + pltpu.roll(two, 2, 0)
    eight = four + pltpu.roll(four, 4, 0)
    sixteen = eight + pltpu.roll(eight, 8, 0)
    kind = lax.rem(tp, 4)
    sums = jnp.where(kind == 0, two, jnp.where(kind == 1, four, jnp.where(kind == 2, eight, sixteen)))
    width = jnp.where(kind == 0, 2, jnp.where(kind == 1, 4, jnp.where(kind == 2, 8, 16)))
    place = (z * NR + y) * T + lax.broadcasted_iota(jnp.int32, (T, 1), 0)
    count = jnp.minimum(place + 1, width).astype(F32)
    mixed = (sums[16:] / count - pool32).astype(BF16)
    y_pool = (mm(mixed, pmix[...]) * pgain[...] * silu(pgate)).astype(BF16)
    gate = sgain[...] * silu(rgate)
    faded = query * jnp.exp(cum)
    relay(2, 3)

    over_z.arrive()
    _, _, outer, _ = chain(st2, z, NR)
    incoming = jnp.exp(before) * outer + inside
    rec = rec + mm3(faded, incoming, 1, 1)
    normed = rec * lax.rsqrt(jnp.mean(rec * rec, axis=1, keepdims=True) + EPS)
    y_rec = (normed * gate).astype(BF16)

    yb[...] = jnp.concatenate([y_rec, y_pool], axis=1).reshape(NX, 2, OWN, 2 * DK)

    def project(k, parity):
        left = yb[k, parity]
        return mm(left[:, :DK], g2a[...].reshape(D, DK), 1, 1) + mm(
            left[:, DK:], g2b[...].reshape(D, DK), 1, 1
        )

    def sib_copy(k):
        return pltpu.make_async_remote_copy(
            src_ref=sib_out.at[k],
            dst_ref=sib_in.at[k],
            send_sem=bs.at[k],
            recv_sem=br.at[k],
            device_id={C: other},
            device_id_type=MESH,
        )

    theirs = yb[:, other].reshape(NX * OWN, 2 * DK)
    mine = yb[:, c].reshape(NX * OWN, 2 * DK)
    for half in range(2):
        left = theirs[half * 2 * OWN : (half + 1) * 2 * OWN]
        part = mm(left[:, :DK], g2a[...].reshape(D, DK), 1, 1) + mm(
            left[:, DK:], g2b[...].reshape(D, DK), 1, 1
        )
        for k in range(2):
            sib_out[2 * half + k] = part[k * OWN : (k + 1) * OWN].astype(BF16)
            sib_copy(2 * half + k).start()

    def red_copy(distance):
        return pltpu.make_async_remote_copy(
            src_ref=red_out.at[around(x + distance, NX)],
            dst_ref=red_in.at[distance - 1],
            send_sem=xs.at[distance - 1],
            recv_sem=xr.at[distance - 1],
            device_id={X: around(x + distance, NX)},
            device_id_type=MESH,
        )

    part = mm(mine[:, :DK], g2a[...].reshape(D, DK), 1, 1) + mm(
        mine[:, DK:], g2b[...].reshape(D, DK), 1, 1
    )
    for k in range(NX):
        sib_copy(k).wait_recv()
        red_out[k] = (part[k * OWN : (k + 1) * OWN] + sib_in[k].astype(F32)).astype(BF16)
    for distance in (2, 1, 3):
        red_copy(distance).start()
    summed = red_out[x].astype(F32)
    for distance in (1, 3, 2):
        red_copy(distance).wait_recv()
        summed = summed + red_in[distance - 1].astype(F32)
    scale = lax.rsqrt(jnp.mean(summed * summed, axis=1, keepdims=True) + EPS)
    out[...] = (summed * scale * post[...]).astype(BF16)

    for stream in first:
        stream.drain()
    for stream in second:
        stream.drain()
    over_y.drain()
    over_z.drain()
    for distance in range(1, NX):
        tok_out(distance).wait_send()
        tok_copy(NX + distance, tok_from(distance) + c, {C: other}).wait_send()
        red_copy(distance).wait_send()
    tok_copy(0, tp, {C: other}).wait_send()
    for k in range(NX):
        sib_copy(k).wait_send()
    shift.wait_send()


def per_device(
    tokens_in, norm_gain, w_query, w_forget, w_input, w_rgate, w_pool_in, w_pgate,
    floor_rate, extra_logdecay, state_gain, pool_mix, pool_gain, out_rec, out_pool, post_gain,
):
    anywhere = pl.BlockSpec(memory_space=pl.ANY)
    close = pl.BlockSpec(memory_space=pltpu.VMEM)
    dma = pltpu.SemaphoreType.DMA
    return pl.pallas_call(
        layer,
        name="layer",
        out_shape=jax.ShapeDtypeStruct((OWN, D), BF16),
        in_specs=[anywhere] * 9 + [close] * 7,
        out_specs=close,
        scratch_shapes=[
            pltpu.VMEM((NR, NR, D // 64, DK), BF16),
            pltpu.VMEM((NR, NR, D // 64, DK), BF16),
            pltpu.VMEM((NR, NR, D // 64, 2 * DK), BF16),
            pltpu.VMEM((NR, NR, D // 64, 2 * DK), BF16),
            pltpu.VMEM((NR, NR, D // 64, DK), BF16),
            pltpu.VMEM((NR, NR, D // 64, DK), BF16),
            pltpu.VMEM((2 * NX, T, D // (2 * NX)), BF16),
            pltpu.VMEM((T, D), BF16),
            pltpu.VMEM((NR, DK + 16, DK), BF16),
            pltpu.VMEM((NR, DK + 16, DK), BF16),
            pltpu.VMEM((16, DK), BF16),
            pltpu.VMEM((16, DK), BF16),
            pltpu.VMEM((NX, 2, OWN, 2 * DK), BF16),
            pltpu.VMEM((NX, OWN, D), BF16),
            pltpu.VMEM((NX, OWN, D), BF16),
            pltpu.VMEM((NX, OWN, D), BF16),
            pltpu.VMEM((NX - 1, OWN, D), BF16),
            dma((9,)),
            dma((6, NR)),
            dma((6, NR)),
            dma((6, NR)),
            dma((6, NR)),
            dma((2 * NX,)),
            dma((2 * NX,)),
            dma((2, NR)),
            dma((2, NR)),
            dma((1,)),
            dma((1,)),
            dma((NX,)),
            dma((NX,)),
            dma((NX,)),
            dma((NX,)),
        ],
        compiler_params=pltpu.CompilerParams(
            collective_id=0, has_side_effects=True, vmem_limit_bytes=56 * 1024 * 1024
        ),
    )(
        tokens_in,
        w_query,
        w_forget,
        w_input,
        w_rgate,
        w_pool_in,
        w_pgate,
        out_rec.T,
        out_pool.T,
        norm_gain.reshape(1, -1),
        floor_rate.reshape(1, -1),
        extra_logdecay.reshape(1, -1),
        state_gain.reshape(1, -1),
        pool_mix.reshape(DK, DK),
        pool_gain.reshape(1, -1),
        post_gain.reshape(1, -1),
    )


def solution(mesh):
    torus = Mesh(mesh.devices.reshape(8, 8, 4, 2), ("sp_0", "sp_1", "tp_0", "tp_1"))
    return jax.shard_map(
        per_device,
        mesh=torus,
        in_specs=(
            P(SP, TP),
            P(),
            P(SP, TP),
            P(SP, TP),
            P(SP, TP),
            P(SP, TP),
            P(SP, TP),
            P(SP, TP),
            P(TP),
            P(SP, TP),
            P(TP),
            P(TP, None, None),
            P(TP),
            P(TP, SP),
            P(TP, SP),
            P(),
        ),
        out_specs=P(SP_TP, None),
        check_vma=False,
    )
```

```python
import functools

import jax
import jax.numpy as jnp
from jax import lax
from jax.experimental import pallas as pl
from jax.experimental.pallas import tpu as pltpu
from jax.sharding import Mesh
from jax.sharding import PartitionSpec as P

SP = ("sp_0", "sp_1")
TP = ("tp_0", "tp_1")
SP_TP = ("sp_0", "sp_1", "tp_0", "tp_1")
Z, Y, X, C = "sp_0", "sp_1", "tp_0", "tp_1"
MESH = pl.DeviceIdType.MESH
EPS = 1e-06
DK = 128
NR = 8
NX = 4
T = 256
D = 2048
OWN = T // (2 * NX)
F32 = jnp.float32
BF16 = jnp.bfloat16
ORDER = (4, 3, 5, 2, 6, 1, 7)


def mm(a, b, ca=1, cb=0):
    return lax.dot_general(a, b, (((ca,), (cb,)), ((), ())), preferred_element_type=F32)


def halves(a):
    hi = a.astype(BF16)
    return hi, (a - hi.astype(F32)).astype(BF16)


def mm3(a, b, ca=1, cb=0):
    ah, al = halves(a)
    bh, bl = halves(b)
    return mm(ah, bh, ca, cb) + (mm(ah, bl, ca, cb) + mm(al, bh, ca, cb))


def mm2(a, b, ca=1, cb=0):
    ah, al = halves(a)
    return mm(ah, b, ca, cb) + mm(al, b, ca, cb)


def silu(a):
    return a / (1.0 + jnp.exp(-a))


def around(value, count):
    return lax.rem(value + 2 * count, count)


class Ring:
    def __init__(self, part, axis, me, sign, send, recv):
        self.part, self.axis, self.me, self.sign, self.send, self.recv = part, axis, me, sign, send, recv

    def copy(self, step, back, origin):
        sign = -self.sign if back else self.sign
        at = NR // 2 + step if back else step
        block = self.part(origin)
        return pltpu.make_async_remote_copy(
            src_ref=block,
            dst_ref=block,
            send_sem=self.send.at[at],
            recv_sem=self.recv.at[at],
            device_id={self.axis: around(self.me + sign, NR)},
            device_id_type=MESH,
        )

    def origin(self, step, back):
        sign = -self.sign if back else self.sign
        return around(self.me - sign * step, NR)

    def steps(self, back):
        return NR // 2 - 1 if back else NR // 2

    def start(self, step):
        for back in (False, True):
            if step < self.steps(back):
                self.copy(step, back, self.origin(step, back)).start()

    def arrive(self, step):
        for back in (False, True):
            if step < self.steps(back):
                self.copy(step, back, self.origin(step + 1, back)).wait_recv()

    def drain(self):
        for back in (False, True):
            for step in range(self.steps(back)):
                self.copy(step, back, self.origin(step, back)).wait_send()


class Direct:
    def __init__(self, part, axis, me, send, recv):
        self.part, self.axis, self.me, self.send, self.recv = part, axis, me, send, recv

    def copy(self, distance, origin):
        block = self.part(origin)
        return pltpu.make_async_remote_copy(
            src_ref=block,
            dst_ref=block,
            send_sem=self.send.at[distance],
            recv_sem=self.recv.at[distance],
            device_id={self.axis: around(self.me + distance, NR)},
            device_id_type=MESH,
        )

    def start(self):
        for distance in ORDER:
            self.copy(distance, self.me).start()

    def arrive(self):
        for distance in range(1, NR):
            self.copy(distance, around(self.me - distance, NR)).wait_recv()

    def drain(self):
        for distance in range(1, NR):
            self.copy(distance, self.me).wait_send()


class Swap:
    def __init__(self, out, held, axis, me, send, recv):
        self.out, self.held, self.axis, self.me, self.send, self.recv = out, held, axis, me, send, recv

    def copy(self, distance, origin):
        other = around(self.me + distance, NR)
        return pltpu.make_async_remote_copy(
            src_ref=self.out.at[other],
            dst_ref=self.held.at[origin],
            send_sem=self.send.at[distance],
            recv_sem=self.recv.at[distance],
            device_id={self.axis: other},
            device_id_type=MESH,
        )

    def start(self):
        for distance in ORDER:
            self.copy(distance, self.me).start()

    def arrive(self):
        for distance in range(1, NR):
            self.copy(distance, around(self.me - distance, NR)).wait_recv()

    def drain(self):
        for distance in range(1, NR):
            self.copy(distance, self.me).wait_send()


def log_rows(total):
    hi = total.astype(BF16)
    rest = total - hi.astype(F32)
    mid = rest.astype(BF16)
    low = (rest - mid.astype(F32)).astype(BF16)
    place = lax.broadcasted_iota(jnp.int32, (16, DK), 0)
    parts = jnp.where(place == 1, mid.astype(F32), jnp.where(place == 2, low.astype(F32), 0.0))
    return jnp.where(place == 0, hi.astype(F32), parts).astype(BF16)


def from_message(ref, k):
    whole = ref[k].astype(F32)
    return whole[:16], jnp.sum(whole[16:], axis=0, keepdims=True)


def layer(
    tok, wq, wf, wi, wr, wp, wg, orec, opool,
    ngain_in, rate_in, extra_in, sgain_in, pmix_in, pgain_in, post_in,
    out,
    g0a, g0b, g1a, g1b, xg, sc,
    ngain, rate, extra, sgain, pmix, pgain, post,
    st_out, st1, st2, st3_out, st3, rows_out, rows_in, yb, sib_out, sib_in, red_out, red_in, mid_in,
    lsem, vsem, p1s, p1r, p2s, p2r, ts, tr, ss, sr, ps, pr, bs, br, xs, xr,
):
    scope = jax.named_scope
    z, y, x, c = lax.axis_index(Z), lax.axis_index(Y), lax.axis_index(X), lax.axis_index(C)
    tp = 2 * x + c
    sign = 1 - 2 * c
    other = 1 - c

    local = [
        pltpu.make_async_copy(src, dst, lsem.at[k])
        for k, (src, dst) in enumerate(
            (
                (wf, g0a.at[z, y]),
                (wi, g0b.at[z, y]),
                (tok, xg.at[tp]),
                (wq, g1a.at[0, z, y]),
                (wr, g1a.at[1, z, y]),
                (orec, g1a.at[2, z, y]),
                (wp, g1b.at[0, z, y]),
                (wg, g1b.at[1, z, y]),
                (opool, g1b.at[2, z, y]),
            )
        )
    ]
    vectors = [
        pltpu.make_async_copy(src, dst, vsem.at[k])
        for k, (src, dst) in enumerate(
            (
                (ngain_in, ngain),
                (rate_in, rate),
                (extra_in, extra),
                (sgain_in, sgain),
                (pmix_in, pmix),
                (pgain_in, pgain),
                (post_in, post),
            )
        )
    ]
    for copy in local + vectors:
        copy.start()

    after_y = around(y + 1, NR)
    after_z = jnp.where(y == NR - 1, around(z + 1, NR), z)
    before_y = around(y - 1, NR)
    before_z = jnp.where(y == 0, around(z - 1, NR), z)
    with scope("barrier"):
        barrier = pltpu.get_barrier_semaphore()
        for k in ORDER:
            pl.semaphore_signal(barrier, 1, device_id={Y: around(y + k, NR)}, device_id_type=MESH)
            pl.semaphore_signal(barrier, 1, device_id={Z: around(z + k, NR)}, device_id_type=MESH)
        for k in range(1, NX):
            pl.semaphore_signal(barrier, 1, device_id={X: around(x + k, NX)}, device_id_type=MESH)
        pl.semaphore_signal(barrier, 1, device_id={C: other}, device_id_type=MESH)
        pl.semaphore_signal(barrier, 1, device_id={Z: before_z, Y: before_y}, device_id_type=MESH)
        pl.semaphore_wait(barrier, 2 * (NR - 1) + NX - 1 + 2)

    first = [
        Direct(lambda o: g0a.at[z, o], Y, y, p1s.at[0], p1r.at[0]),
        Direct(lambda o: g0b.at[o, y], Z, z, p1s.at[1], p1r.at[1]),
        Direct(lambda o: g1a.at[:, z, o], Y, y, p1s.at[2], p1r.at[2]),
        Direct(lambda o: g1b.at[:, o, y], Z, z, p1s.at[3], p1r.at[3]),
    ]
    streams = [
        (
            Ring(lambda o: g0a.at[o], Z, z, sign, p2s.at[0], p2r.at[0]),
            Ring(lambda o: g0b.at[:, o], Y, y, sign, p2s.at[1], p2r.at[1]),
        )
    ] + [
        (
            Ring(lambda o, k=k: g1a.at[k, o], Z, z, sign, p2s.at[2 * k + 2], p2r.at[2 * k + 2]),
            Ring(lambda o, k=k: g1b.at[k, :, o], Y, y, sign, p2s.at[2 * k + 3], p2r.at[2 * k + 3]),
        )
        for k in range(3)
    ]

    def start(k, step):
        for ring in streams[k]:
            ring.start(step)

    def relay(k, step):
        with scope("relay%d%d" % (k, step)):
            for ring in streams[k]:
                ring.arrive(step)
                if step + 1 < NR // 2:
                    ring.start(step + 1)

    def tok_copy(at, slot, where):
        return pltpu.make_async_remote_copy(
            src_ref=xg.at[slot],
            dst_ref=xg.at[slot],
            send_sem=ts.at[at],
            recv_sem=tr.at[at],
            device_id=where,
            device_id_type=MESH,
        )

    def tok_out(distance):
        return tok_copy(distance, tp, {X: around(x + distance, NX)})

    def tok_from(distance):
        return 2 * around(x - distance, NX)

    with scope("sends"):
        local[0].wait()
        first[0].start()
        local[1].wait()
        first[1].start()
        local[2].wait()
        for distance in (2, 1, 3):
            tok_out(distance).start()
        tok_copy(0, tp, {C: other}).start()
        for k in range(3, 6):
            local[k].wait()
        first[2].start()
        for k in range(6, 9):
            local[k].wait()
        first[3].start()
        for copy in vectors:
            copy.wait()

    with scope("first0"):
        first[0].arrive()
        streams[0][0].start(0)
        first[1].arrive()
        streams[0][1].start(0)
    with scope("first1"):
        first[2].arrive()
        streams[1][0].start(0)
        first[3].arrive()
        streams[1][1].start(0)
    with scope("tokens"):
        for distance in (1, 3, 2):
            tok_copy(distance, tok_from(distance) + c, {X: around(x + distance, NX)}).wait_recv()
            tok_copy(NX + distance, tok_from(distance) + c, {C: other}).start()
    relay(0, 0)
    with scope("tokens2"):
        tok_copy(0, 2 * x + other, {C: other}).wait_recv()
        for distance in range(1, NX):
            tok_copy(NX + distance, tok_from(distance) + other, {C: other}).wait_recv()
    with scope("scale"):
        squares = jnp.zeros((T, 1), F32)
        for k in range(2 * NX):
            block = xg[k].astype(F32)
            squares = squares + jnp.sum(block * block, axis=1, keepdims=True)
            at = slice(k * (D // (2 * NX)), (k + 1) * (D // (2 * NX)))
            sc[:, at] = (block * ngain[:, at]).astype(BF16)
        inv_rms = lax.rsqrt(squares * (1.0 / D) + EPS)
    relay(1, 0)
    relay(0, 1)
    relay(1, 1)
    relay(0, 2)
    relay(1, 2)
    start(2, 0)
    relay(0, 3)

    with scope("gates"):
        scaled = sc[...]
        forget = (mm(scaled, g0a[...].reshape(D, DK)) * inv_rms).astype(BF16).astype(F32)
        value = (mm(scaled, g0b[...].reshape(D, DK)) * inv_rms).astype(BF16)
        r = rate[...]
        series = r * (1.0 - r / 2 * (1.0 - r / 3 * (1.0 - r / 4 * (1.0 - r / 5 * (1.0 - r / 6)))))
        reach = jnp.where(r < 0.1, series, 1.0 - jnp.exp(-r))
        key = reach * (1.0 / (1.0 + jnp.exp(forget)))
        more = lax.dot_general(
            extra[...],
            jnp.ones((1, DK), F32),
            (((0,), (0,)), ((), ())),
            precision=lax.Precision.HIGHEST,
            preferred_element_type=F32,
        )
        logs = jnp.log1p(-key) + more
        row = lax.broadcasted_iota(jnp.int32, (T, T), 0)
        col = lax.broadcasted_iota(jnp.int32, (T, T), 1)
        lower = jnp.where(row >= col, 1.0, 0.0)
        cum = jnp.dot(lower, logs, precision=lax.Precision.HIGHEST, preferred_element_type=F32)
        last = cum[T - 1 : T, :]
        memory = mm2(key * jnp.exp(last - cum), value, 0, 0).T
        st_out[:, 0:16] = memory.astype(BF16).reshape(NR, 16, DK)
        st_out[:, 16:32] = jnp.broadcast_to(log_rows(last)[None], (NR, 16, DK))

    to_slices = Swap(st_out, st1, Y, y, ss.at[0], sr.at[0])
    over_z = Direct(lambda o: st2.at[o], Z, z, ss.at[1], sr.at[1])
    back = Swap(st3_out, st3, Y, y, ss.at[2], sr.at[2])
    to_slices.start()
    st1[y] = st_out[y]
    relay(1, 3)
    start(3, 0)

    with scope("proj_qp"):
        query = (mm(scaled, g1a[0].reshape(D, DK)) * inv_rms).astype(BF16)
        query = query.astype(F32) * DK ** (-0.5)
        pool = (mm(scaled, g1b[0].reshape(D, DK)) * inv_rms).astype(BF16)
        rows_out[...] = pool[T - 16 :, :]
    shift = pltpu.make_async_remote_copy(
        src_ref=rows_out,
        dst_ref=rows_in,
        send_sem=ps.at[0],
        recv_sem=pr.at[0],
        device_id={Z: after_z, Y: after_y},
        device_id_type=MESH,
    )
    shift.start()
    relay(2, 0)

    with scope("wait_y"):
        to_slices.arrive()
    with scope("chain_y"):
        state, total = jnp.zeros((16, DK), F32), jnp.zeros((1, DK), F32)
        inside, before = [], []
        for k in range(NR):
            inside.append(state)
            before.append(total)
            new_state, new_total = from_message(st1, k)
            state = jnp.exp(new_total) * state + new_state
            total = total + new_total
        st2[z] = jnp.concatenate([state.astype(BF16), log_rows(total)], axis=0)
    over_z.start()
    relay(3, 0)

    with scope("diag"):
        value32 = value.astype(F32)
        in_block = lax.rem(lax.broadcasted_iota(jnp.int32, (T, 1), 0), 8)
        decay = jnp.exp(logs)
        weight = query
        rec = jnp.sum(query * key, axis=1, keepdims=True) * value32
        for d in range(1, 8):
            weight = weight * (decay if d == 1 else pltpu.roll(decay, d - 1, 0))
            score = jnp.sum(weight * pltpu.roll(key, d, 0), axis=1, keepdims=True)
            rec = rec + jnp.where(in_block >= d, score, 0.0) * pltpu.roll(value32, d, 0)
    relay(2, 1)
    with scope("wait_z"):
        over_z.arrive()
    with scope("chain_z"):
        state = jnp.zeros((16, DK), F32)
        outer = state
        for k in range(NR):
            new_state, new_total = from_message(st2, k)
            state = jnp.exp(new_total) * state + new_state
            outer = jnp.where(k < z, state, outer)
        for k in range(NR):
            st3_out[k] = (jnp.exp(before[k]) * outer + inside[k]).astype(BF16)
    back.start()
    st3[y] = st3_out[y]
    relay(3, 1)
    with scope("levels"):
        scores = jnp.zeros((T, T), F32)
        for half in (8, 16, 32, 64, 128):
            apart = cum.reshape(T // (2 * half), 2 * half, DK)
            apart = jnp.abs(apart - apart[:, half - 1 : half, :]).reshape(T, DK)
            fade = jnp.exp(-apart)
            level = mm3(query * fade, key * fade, 1, 1)
            mask = (row // (2 * half) == col // (2 * half)) & (row // half > col // half)
            scores = jnp.where(mask, level, scores)
        rec = rec + mm2(scores, value)
    relay(2, 2)
    with scope("pool"):
        shift.wait_recv()
        at_start = (z == 0) & (y == 0)
        earlier = jnp.where(at_start, 0.0, rows_in[...].astype(F32))
        pool32 = pool.astype(F32)
        two = jnp.concatenate([earlier, pool32], axis=0)
        two = two + pltpu.roll(two, 1, 0)
        four = two + pltpu.roll(two, 2, 0)
        eight = four + pltpu.roll(four, 4, 0)
        sixteen = eight + pltpu.roll(eight, 8, 0)
        kind = lax.rem(tp, 4)
        sums = jnp.where(kind == 2, eight, sixteen)
        sums = jnp.where(kind == 0, two, jnp.where(kind == 1, four, sums))
        width = jnp.where(kind == 0, 2, jnp.where(kind == 1, 4, jnp.where(kind == 2, 8, 16)))
        place = (z * NR + y) * T + lax.broadcasted_iota(jnp.int32, (T, 1), 0)
        count = jnp.minimum(place + 1, width).astype(F32)
        mixed = (sums[16:] / count - pool32).astype(BF16)
        mapped = mm(mixed, pmix[...]) * pgain[...]
        faded = query * jnp.exp(cum)
    relay(3, 2)
    relay(2, 3)
    with scope("proj_rg"):
        rgate = (mm(scaled, g1a[1].reshape(D, DK)) * inv_rms).astype(BF16).astype(F32)
        pgate = (mm(scaled, g1b[1].reshape(D, DK)) * inv_rms).astype(BF16).astype(F32)
        y_pool = (mapped * silu(pgate)).astype(BF16)
        gate = sgain[...] * silu(rgate)
    relay(3, 3)
    with scope("wait_back"):
        back.arrive()
    with scope("rec"):
        rec = rec + mm2(faded, st3[...].reshape(DK, DK), 1, 1)
        normed = rec * lax.rsqrt(jnp.mean(rec * rec, axis=1, keepdims=True) + EPS)
        y_rec = (normed * gate).astype(BF16)
        yb[...] = jnp.concatenate([y_rec, y_pool], axis=1).reshape(NX, 2, OWN, 2 * DK)

    half_d = D // 2

    def project(parity, side):
        left = yb[:, parity].reshape(NX * OWN, 2 * DK)
        at = slice(side * (NR // 2), (side + 1) * (NR // 2))
        return mm(left[:, :DK], g1a[2, at].reshape(half_d, DK), 1, 1) + mm(
            left[:, DK:], g1b[2, at].reshape(half_d, DK), 1, 1
        )

    def sib_copy(side):
        return pltpu.make_async_remote_copy(
            src_ref=sib_out.at[side],
            dst_ref=sib_in.at[side],
            send_sem=bs.at[side],
            recv_sem=br.at[side],
            device_id={C: other},
            device_id_type=MESH,
        )

    def red_copy(at, src, dst, step):
        return pltpu.make_async_remote_copy(
            src_ref=src,
            dst_ref=dst,
            send_sem=xs.at[at],
            recv_sem=xr.at[at],
            device_id={X: around(x + step, NX)},
            device_id_type=MESH,
        )

    right, left, across = around(x + 1, NX), around(x - 1, NX), around(x + 2, NX)
    steps = (1, -1)
    over = [red_copy(k, red_out.at[k, across], mid_in.at[k], steps[k]) for k in range(2)]
    near = [red_copy(2 + k, red_out.at[1 - k, (right, left)[k]], red_in.at[k], steps[k]) for k in range(2)]
    merged = [red_copy(4 + k, red_out.at[k, (right, left)[k]], red_in.at[2 + k], steps[k]) for k in range(2)]
    with scope("proj_sib"):
        for side in range(2):
            sib_out[side] = project(other, side).astype(BF16).reshape(NX, OWN, half_d)
            sib_copy(side).start()
    with scope("proj_mine"):
        for side in range(2):
            part = project(c, side).reshape(NX, OWN, half_d)
            sib_copy(side).wait_recv()
            red_out[side] = (part + sib_in[side].astype(F32)).astype(BF16)
            over[side].start()
        for k in range(2):
            near[k].start()
    with scope("red_mid"):
        for k in range(2):
            over[k].wait_recv()
            place = (right, left)[k]
            red_out[k, place] = (red_out[k, place].astype(F32) + mid_in[k].astype(F32)).astype(BF16)
            merged[k].start()
    with scope("red_wait"):
        for k in range(2):
            near[k].wait_recv()
        for k in range(2):
            merged[k].wait_recv()
    with scope("final"):
        low = red_out[0, x].astype(F32) + red_in[2].astype(F32) + red_in[1].astype(F32)
        high = red_out[1, x].astype(F32) + red_in[0].astype(F32) + red_in[3].astype(F32)
        squares = jnp.sum(low * low, axis=1, keepdims=True) + jnp.sum(high * high, axis=1, keepdims=True)
        scale = lax.rsqrt(squares * (1.0 / D) + EPS)
        out[:, :half_d] = (low * scale * post[:, :half_d]).astype(BF16)
        out[:, half_d:] = (high * scale * post[:, half_d:]).astype(BF16)

    with scope("drain"):
        for stream in first + [ring for pair in streams for ring in pair] + [to_slices, over_z, back]:
            stream.drain()
        for distance in range(1, NX):
            tok_out(distance).wait_send()
            tok_copy(NX + distance, tok_from(distance) + c, {C: other}).wait_send()
        tok_copy(0, tp, {C: other}).wait_send()
        for k in range(2):
            sib_copy(k).wait_send()
        for copy in over + near + merged:
            copy.wait_send()
        shift.wait_send()


def per_device(
    tokens_in, norm_gain, w_query, w_forget, w_input, w_rgate, w_pool_in, w_pgate,
    floor_rate, extra_logdecay, state_gain, pool_mix, pool_gain, out_rec, out_pool, post_gain,
):
    anywhere = pl.BlockSpec(memory_space=pl.ANY)
    dma = pltpu.SemaphoreType.DMA
    rows = D // 64
    return pl.pallas_call(
        layer,
        name="layer",
        out_shape=jax.ShapeDtypeStruct((OWN, D), BF16),
        in_specs=[anywhere] * 16,
        out_specs=pl.BlockSpec(memory_space=pltpu.VMEM),
        scratch_shapes=[
            pltpu.VMEM((NR, NR, rows, DK), BF16),
            pltpu.VMEM((NR, NR, rows, DK), BF16),
            pltpu.VMEM((3, NR, NR, rows, DK), BF16),
            pltpu.VMEM((3, NR, NR, rows, DK), BF16),
            pltpu.VMEM((2 * NX, T, D // (2 * NX)), BF16),
            pltpu.VMEM((T, D), BF16),
            pltpu.VMEM((1, D), F32),
            pltpu.VMEM((1, DK), F32),
            pltpu.VMEM((1, T), F32),
            pltpu.VMEM((1, DK), F32),
            pltpu.VMEM((DK, DK), BF16),
            pltpu.VMEM((1, DK), F32),
            pltpu.VMEM((1, D), F32),
            pltpu.VMEM((NR, 32, DK), BF16),
            pltpu.VMEM((NR, 32, DK), BF16),
            pltpu.VMEM((NR, 32, DK), BF16),
            pltpu.VMEM((NR, 16, DK), BF16),
            pltpu.VMEM((NR, 16, DK), BF16),
            pltpu.VMEM((16, DK), BF16),
            pltpu.VMEM((16, DK), BF16),
            pltpu.VMEM((NX, 2, OWN, 2 * DK), BF16),
            pltpu.VMEM((2, NX, OWN, D // 2), BF16),
            pltpu.VMEM((2, NX, OWN, D // 2), BF16),
            pltpu.VMEM((2, NX, OWN, D // 2), BF16),
            pltpu.VMEM((4, OWN, D // 2), BF16),
            pltpu.VMEM((2, OWN, D // 2), BF16),
            dma((9,)),
            dma((7,)),
            dma((4, NR)),
            dma((4, NR)),
            dma((8, NR)),
            dma((8, NR)),
            dma((2 * NX,)),
            dma((2 * NX,)),
            dma((3, NR)),
            dma((3, NR)),
            dma((1,)),
            dma((1,)),
            dma((2,)),
            dma((2,)),
            dma((6,)),
            dma((6,)),
        ],
        compiler_params=pltpu.CompilerParams(
            collective_id=0, has_side_effects=True, vmem_limit_bytes=60 * 1024 * 1024
        ),
    )(
        tokens_in,
        w_query,
        w_forget,
        w_input,
        w_rgate,
        w_pool_in,
        w_pgate,
        out_rec.T,
        out_pool.T,
        norm_gain.reshape(1, -1),
        floor_rate.reshape(1, -1),
        extra_logdecay.reshape(1, -1),
        state_gain.reshape(1, -1),
        pool_mix.reshape(DK, DK),
        pool_gain.reshape(1, -1),
        post_gain.reshape(1, -1),
    )


def solution(mesh):
    torus = Mesh(mesh.devices.reshape(8, 8, 4, 2), ("sp_0", "sp_1", "tp_0", "tp_1"))
    return jax.shard_map(
        per_device,
        mesh=torus,
        in_specs=(
            P(SP, TP),
            P(),
            P(SP, TP),
            P(SP, TP),
            P(SP, TP),
            P(SP, TP),
            P(SP, TP),
            P(SP, TP),
            P(TP),
            P(SP, TP),
            P(TP),
            P(TP, None, None),
            P(TP),
            P(TP, SP),
            P(TP, SP),
            P(),
        ),
        out_specs=P(SP_TP, None),
        check_vma=False,
    )
```

```python
import functools

import jax
import jax.numpy as jnp
from jax import lax
from jax.experimental import pallas as pl
from jax.experimental.pallas import tpu as pltpu
from jax.sharding import Mesh
from jax.sharding import PartitionSpec as P

SP = ("sp_0", "sp_1")
TP = ("tp_0", "tp_1")
SP_TP = ("sp_0", "sp_1", "tp_0", "tp_1")
Z, Y, X, C = "sp_0", "sp_1", "tp_0", "tp_1"
MESH = pl.DeviceIdType.MESH
EPS = 1e-06
DK = 128
NR = 8
NX = 4
T = 256
D = 2048
OWN = T // (2 * NX)
F32 = jnp.float32
BF16 = jnp.bfloat16
CUTS = 2
SPAN = NR // CUTS
ORDER = (4, 3, 5, 2, 6, 1, 7)


def mm(a, b, ca=1, cb=0):
    return lax.dot_general(a, b, (((ca,), (cb,)), ((), ())), preferred_element_type=F32)


def halves(a):
    hi = a.astype(BF16)
    return hi, (a - hi.astype(F32)).astype(BF16)


def mm3(a, b, ca=1, cb=0):
    ah, al = halves(a)
    bh, bl = halves(b)
    return mm(ah, bh, ca, cb) + (mm(ah, bl, ca, cb) + mm(al, bh, ca, cb))


def mm2(a, b, ca=1, cb=0):
    ah, al = halves(a)
    return mm(ah, b, ca, cb) + mm(al, b, ca, cb)


def silu(a):
    return a / (1.0 + jnp.exp(-a))


def around(value, count):
    return lax.rem(value + 2 * count, count)


class Ring:
    def __init__(self, part, axis, me, sign, send, recv):
        self.part, self.axis, self.me, self.sign, self.send, self.recv = part, axis, me, sign, send, recv

    def copy(self, step, back, cut, origin):
        sign = -self.sign if back else self.sign
        at = CUTS * (NR // 2 + step if back else step) + cut
        block = self.part(origin, cut)
        return pltpu.make_async_remote_copy(
            src_ref=block,
            dst_ref=block,
            send_sem=self.send.at[at],
            recv_sem=self.recv.at[at],
            device_id={self.axis: around(self.me + sign, NR)},
            device_id_type=MESH,
        )

    def origin(self, step, back):
        sign = -self.sign if back else self.sign
        return around(self.me - sign * step, NR)

    def steps(self, back):
        return NR // 2 - 1 if back else NR // 2

    def start(self, step, back, cut):
        if step < self.steps(back):
            self.copy(step, back, cut, self.origin(step, back)).start()

    def relay(self, step, back, cut):
        if step < self.steps(back):
            self.copy(step, back, cut, self.origin(step + 1, back)).wait_recv()
            self.start(step + 1, back, cut)

    def drain(self):
        for back in (False, True):
            for step in range(self.steps(back)):
                for cut in range(CUTS):
                    self.copy(step, back, cut, self.origin(step, back)).wait_send()


class Direct:
    def __init__(self, part, axis, me, send, recv):
        self.part, self.axis, self.me, self.send, self.recv = part, axis, me, send, recv

    def copy(self, distance, origin):
        block = self.part(origin)
        return pltpu.make_async_remote_copy(
            src_ref=block,
            dst_ref=block,
            send_sem=self.send.at[distance],
            recv_sem=self.recv.at[distance],
            device_id={self.axis: around(self.me + distance, NR)},
            device_id_type=MESH,
        )

    def start(self):
        for distance in ORDER:
            self.copy(distance, self.me).start()

    def arrive(self):
        for distance in range(1, NR):
            self.copy(distance, around(self.me - distance, NR)).wait_recv()

    def drain(self):
        for distance in range(1, NR):
            self.copy(distance, self.me).wait_send()


class Swap:
    def __init__(self, out, held, axis, me, send, recv):
        self.out, self.held, self.axis, self.me, self.send, self.recv = out, held, axis, me, send, recv

    def copy(self, distance, origin):
        other = around(self.me + distance, NR)
        return pltpu.make_async_remote_copy(
            src_ref=self.out.at[other],
            dst_ref=self.held.at[origin],
            send_sem=self.send.at[distance],
            recv_sem=self.recv.at[distance],
            device_id={self.axis: other},
            device_id_type=MESH,
        )

    def start(self):
        for distance in ORDER:
            self.copy(distance, self.me).start()

    def arrive(self):
        for distance in range(1, NR):
            self.copy(distance, around(self.me - distance, NR)).wait_recv()

    def drain(self):
        for distance in range(1, NR):
            self.copy(distance, self.me).wait_send()


def log_rows(total):
    hi = total.astype(BF16)
    rest = total - hi.astype(F32)
    mid = rest.astype(BF16)
    low = (rest - mid.astype(F32)).astype(BF16)
    place = lax.broadcasted_iota(jnp.int32, (16, DK), 0)
    parts = jnp.where(place == 1, mid.astype(F32), jnp.where(place == 2, low.astype(F32), 0.0))
    return jnp.where(place == 0, hi.astype(F32), parts).astype(BF16)


def from_message(ref, k):
    whole = ref[k].astype(F32)
    return whole[:16], jnp.sum(whole[16:], axis=0, keepdims=True)


def layer(
    tok, wq, wf, wi, wr, wp, wg, orec, opool,
    ngain_in, rate_in, extra_in, sgain_in, pmix_in, pgain_in, post_in,
    out,
    g0a, g0b, g1a, g1b, xg, sc,
    ngain, rate, extra, sgain, pmix, pgain, post,
    st_out, st1, st2, st3_out, st3, rows_out, rows_in, yb, sib_out, sib_in, red_out, red_in, mid_in,
    lsem, vsem, p1s, p1r, p2s, p2r, ts, tr, ss, sr, ps, pr, bs, br, xs, xr,
):
    scope = jax.named_scope
    z, y, x, c = lax.axis_index(Z), lax.axis_index(Y), lax.axis_index(X), lax.axis_index(C)
    tp = 2 * x + c
    sign = 1 - 2 * c
    other = 1 - c

    after_y = around(y + 1, NR)
    after_z = jnp.where(y == NR - 1, around(z + 1, NR), z)
    before_y = around(y - 1, NR)
    before_z = jnp.where(y == 0, around(z - 1, NR), z)
    with scope("barrier"):
        barrier = pltpu.get_barrier_semaphore()
        for k in ORDER:
            pl.semaphore_signal(barrier, 1, device_id={Y: around(y + k, NR)}, device_id_type=MESH)
            pl.semaphore_signal(barrier, 1, device_id={Z: around(z + k, NR)}, device_id_type=MESH)
        for k in range(1, NX):
            pl.semaphore_signal(barrier, 1, device_id={X: around(x + k, NX)}, device_id_type=MESH)
        pl.semaphore_signal(barrier, 1, device_id={C: other}, device_id_type=MESH)
        pl.semaphore_signal(barrier, 1, device_id={Z: before_z, Y: before_y}, device_id_type=MESH)

    local = [
        pltpu.make_async_copy(src, dst, lsem.at[k])
        for k, (src, dst) in enumerate(
            (
                (wf, g0a.at[z, y]),
                (wi, g0b.at[z, y]),
                (tok, xg.at[tp]),
                (wq, g1a.at[0, z, y]),
                (wr, g1a.at[1, z, y]),
                (orec, g1a.at[2, z, y]),
                (wp, g1b.at[0, z, y]),
                (wg, g1b.at[1, z, y]),
                (opool, g1b.at[2, z, y]),
            )
        )
    ]
    vectors = [
        pltpu.make_async_copy(src, dst, vsem.at[k])
        for k, (src, dst) in enumerate(
            (
                (ngain_in, ngain),
                (rate_in, rate),
                (extra_in, extra),
                (sgain_in, sgain),
                (pmix_in, pmix),
                (pgain_in, pgain),
                (post_in, post),
            )
        )
    ]
    for copy in local + vectors:
        copy.start()
    with scope("barrier"):
        pl.semaphore_wait(barrier, 2 * (NR - 1) + NX - 1 + 2)

    first = [
        (
            Direct(lambda o: g0a.at[z, o], Y, y, p1s.at[0], p1r.at[0]),
            Direct(lambda o: g0b.at[o, y], Z, z, p1s.at[1], p1r.at[1]),
        )
    ] + [
        (
            Direct(lambda o, k=k: g1a.at[k, z, o], Y, y, p1s.at[2 * k + 2], p1r.at[2 * k + 2]),
            Direct(lambda o, k=k: g1b.at[k, o, y], Z, z, p1s.at[2 * k + 3], p1r.at[2 * k + 3]),
        )
        for k in range(3)
    ]

    def cut_of(cut):
        return pl.ds(SPAN * cut, SPAN)

    streams = [
        (
            Ring(lambda o, u: g0a.at[o, cut_of(u)], Z, z, sign, p2s.at[0], p2r.at[0]),
            Ring(lambda o, u: g0b.at[cut_of(u), o], Y, y, sign, p2s.at[1], p2r.at[1]),
        )
    ] + [
        (
            Ring(lambda o, u, k=k: g1a.at[k, o, cut_of(u)], Z, z, sign, p2s.at[2 * k + 2], p2r.at[2 * k + 2]),
            Ring(lambda o, u, k=k: g1b.at[k, cut_of(u), o], Y, y, sign, p2s.at[2 * k + 3], p2r.at[2 * k + 3]),
        )
        for k in range(3)
    ]

    def start(k):
        with scope("first%d" % k):
            for wide, ring in zip(first[k], streams[k]):
                wide.arrive()
                for cut in range(CUTS):
                    for back in (False, True):
                        ring.start(0, back, cut)

    def relay(k, step):
        with scope("relay%d%d" % (k, step)):
            for cut in range(CUTS):
                for back in (False, True):
                    for ring in streams[k]:
                        ring.relay(step, back, cut)

    def tok_copy(at, slot, where):
        return pltpu.make_async_remote_copy(
            src_ref=xg.at[slot],
            dst_ref=xg.at[slot],
            send_sem=ts.at[at],
            recv_sem=tr.at[at],
            device_id=where,
            device_id_type=MESH,
        )

    def tok_out(distance):
        return tok_copy(distance, tp, {X: around(x + distance, NX)})

    def tok_from(distance):
        return 2 * around(x - distance, NX)

    with scope("sends"):
        local[0].wait()
        first[0][0].start()
        local[1].wait()
        first[0][1].start()
        local[2].wait()
        for distance in (2, 1, 3):
            tok_out(distance).start()
        tok_copy(0, tp, {C: other}).start()
        for k in range(2):
            local[3 + k].wait()
            first[1 + k][0].start()
            local[6 + k].wait()
            first[1 + k][1].start()
        local[5].wait()
        local[8].wait()
        for copy in vectors:
            copy.wait()

    start(0)
    start(1)
    first[3][0].start()
    first[3][1].start()
    with scope("tokens"):
        for distance in (1, 3, 2):
            tok_copy(distance, tok_from(distance) + c, {X: around(x + distance, NX)}).wait_recv()
            tok_copy(NX + distance, tok_from(distance) + c, {C: other}).start()
    relay(0, 0)
    with scope("tokens2"):
        tok_copy(0, 2 * x + other, {C: other}).wait_recv()
        for distance in range(1, NX):
            tok_copy(NX + distance, tok_from(distance) + other, {C: other}).wait_recv()
    with scope("scale"):
        squares = jnp.zeros((T, 1), F32)
        for k in range(2 * NX):
            block = xg[k].astype(F32)
            squares = squares + jnp.sum(block * block, axis=1, keepdims=True)
            at = slice(k * (D // (2 * NX)), (k + 1) * (D // (2 * NX)))
            sc[:, at] = (block * ngain[:, at]).astype(BF16)
        inv_rms = lax.rsqrt(squares * (1.0 / D) + EPS)
    relay(1, 0)
    relay(0, 1)
    relay(1, 1)
    relay(0, 2)
    start(2)
    relay(1, 2)
    start(3)
    relay(0, 3)

    with scope("proj_fv"):
        scaled = sc[...]
        forget = (mm(scaled, g0a[...].reshape(D, DK)) * inv_rms).astype(BF16).astype(F32)
        value = (mm(scaled, g0b[...].reshape(D, DK)) * inv_rms).astype(BF16)
    relay(2, 0)
    with scope("gates"):
        r = rate[...]
        series = r * (1.0 - r / 2 * (1.0 - r / 3 * (1.0 - r / 4 * (1.0 - r / 5 * (1.0 - r / 6)))))
        reach = jnp.where(r < 0.1, series, 1.0 - jnp.exp(-r))
        key = reach * (1.0 / (1.0 + jnp.exp(forget)))
        more = lax.dot_general(
            extra[...],
            jnp.ones((1, DK), F32),
            (((0,), (0,)), ((), ())),
            precision=lax.Precision.HIGHEST,
            preferred_element_type=F32,
        )
        logs = jnp.log1p(-key) + more
        row = lax.broadcasted_iota(jnp.int32, (T, T), 0)
        col = lax.broadcasted_iota(jnp.int32, (T, T), 1)
        lower = jnp.where(row >= col, 1.0, 0.0)
        cum = jnp.dot(lower, logs, precision=lax.Precision.HIGHEST, preferred_element_type=F32)
        last = cum[T - 1 : T, :]
        memory = mm2(key * jnp.exp(last - cum), value, 0, 0).T
        st_out[:, 0:16] = memory.astype(BF16).reshape(NR, 16, DK)
        st_out[:, 16:32] = jnp.broadcast_to(log_rows(last)[None], (NR, 16, DK))

    to_slices = Swap(st_out, st1, Y, y, ss.at[0], sr.at[0])
    over_z = Direct(lambda o: st2.at[o], Z, z, ss.at[1], sr.at[1])
    back = Swap(st3_out, st3, Y, y, ss.at[2], sr.at[2])
    to_slices.start()
    st1[y] = st_out[y]
    relay(1, 3)
    relay(3, 0)

    with scope("proj_qp"):
        query = (mm(scaled, g1a[0].reshape(D, DK)) * inv_rms).astype(BF16)
        query = query.astype(F32) * DK ** (-0.5)
        pool = (mm(scaled, g1b[0].reshape(D, DK)) * inv_rms).astype(BF16)
        rows_out[...] = pool[T - 16 :, :]
    shift = pltpu.make_async_remote_copy(
        src_ref=rows_out,
        dst_ref=rows_in,
        send_sem=ps.at[0],
        recv_sem=pr.at[0],
        device_id={Z: after_z, Y: after_y},
        device_id_type=MESH,
    )
    shift.start()
    relay(2, 1)

    with scope("wait_y"):
        to_slices.arrive()
    with scope("chain_y"):
        state, total = jnp.zeros((16, DK), F32), jnp.zeros((1, DK), F32)
        inside, before = [], []
        for k in range(NR):
            inside.append(state)
            before.append(total)
            new_state, new_total = from_message(st1, k)
            state = jnp.exp(new_total) * state + new_state
            total = total + new_total
        st2[z] = jnp.concatenate([state.astype(BF16), log_rows(total)], axis=0)
    over_z.start()
    relay(3, 1)

    with scope("diag"):
        value32 = value.astype(F32)
        in_block = lax.rem(lax.broadcasted_iota(jnp.int32, (T, 1), 0), 8)
        decay = jnp.exp(logs)
        weight = query
        rec = jnp.sum(query * key, axis=1, keepdims=True) * value32
        for d in range(1, 8):
            weight = weight * (decay if d == 1 else pltpu.roll(decay, d - 1, 0))
            score = jnp.sum(weight * pltpu.roll(key, d, 0), axis=1, keepdims=True)
            rec = rec + jnp.where(in_block >= d, score, 0.0) * pltpu.roll(value32, d, 0)
    relay(2, 2)
    with scope("wait_z"):
        over_z.arrive()
    with scope("chain_z"):
        state = jnp.zeros((16, DK), F32)
        outer = state
        for k in range(NR):
            new_state, new_total = from_message(st2, k)
            state = jnp.exp(new_total) * state + new_state
            outer = jnp.where(k < z, state, outer)
        for k in range(NR):
            st3_out[k] = (jnp.exp(before[k]) * outer + inside[k]).astype(BF16)
    back.start()
    st3[y] = st3_out[y]
    relay(3, 2)
    with scope("levels"):
        scores = jnp.zeros((T, T), F32)
        for half in (8, 16, 32, 64, 128):
            apart = cum.reshape(T // (2 * half), 2 * half, DK)
            apart = jnp.abs(apart - apart[:, half - 1 : half, :]).reshape(T, DK)
            fade = jnp.exp(-apart)
            level = mm3(query * fade, key * fade, 1, 1)
            mask = (row // (2 * half) == col // (2 * half)) & (row // half > col // half)
            scores = jnp.where(mask, level, scores)
        rec = rec + mm2(scores, value)
    with scope("pool"):
        shift.wait_recv()
        at_start = (z == 0) & (y == 0)
        earlier = jnp.where(at_start, 0.0, rows_in[...].astype(F32))
        pool32 = pool.astype(F32)
        two = jnp.concatenate([earlier, pool32], axis=0)
        two = two + pltpu.roll(two, 1, 0)
        four = two + pltpu.roll(two, 2, 0)
        eight = four + pltpu.roll(four, 4, 0)
        sixteen = eight + pltpu.roll(eight, 8, 0)
        kind = lax.rem(tp, 4)
        sums = jnp.where(kind == 2, eight, sixteen)
        sums = jnp.where(kind == 0, two, jnp.where(kind == 1, four, sums))
        width = jnp.where(kind == 0, 2, jnp.where(kind == 1, 4, jnp.where(kind == 2, 8, 16)))
        place = (z * NR + y) * T + lax.broadcasted_iota(jnp.int32, (T, 1), 0)
        count = jnp.minimum(place + 1, width).astype(F32)
        mixed = (sums[16:] / count - pool32).astype(BF16)
        mapped = mm(mixed, pmix[...]) * pgain[...]
        faded = query * jnp.exp(cum)
    relay(2, 3)
    with scope("proj_rg"):
        rgate = (mm(scaled, g1a[1].reshape(D, DK)) * inv_rms).astype(BF16).astype(F32)
        pgate = (mm(scaled, g1b[1].reshape(D, DK)) * inv_rms).astype(BF16).astype(F32)
        y_pool = (mapped * silu(pgate)).astype(BF16)
        gate = sgain[...] * silu(rgate)
    relay(3, 3)
    with scope("wait_back"):
        back.arrive()
    with scope("rec"):
        rec = rec + mm2(faded, st3[...].reshape(DK, DK), 1, 1)
        normed = rec * lax.rsqrt(jnp.mean(rec * rec, axis=1, keepdims=True) + EPS)
        y_rec = (normed * gate).astype(BF16)
        yb[...] = jnp.concatenate([y_rec, y_pool], axis=1).reshape(NX, 2, OWN, 2 * DK)

    half_d = D // 2

    def project(parity, side):
        left = yb[:, parity].reshape(NX * OWN, 2 * DK)
        at = slice(side * (NR // 2), (side + 1) * (NR // 2))
        return mm(left[:, :DK], g1a[2, at].reshape(half_d, DK), 1, 1) + mm(
            left[:, DK:], g1b[2, at].reshape(half_d, DK), 1, 1
        )

    def sib_copy(side):
        return pltpu.make_async_remote_copy(
            src_ref=sib_out.at[side],
            dst_ref=sib_in.at[side],
            send_sem=bs.at[side],
            recv_sem=br.at[side],
            device_id={C: other},
            device_id_type=MESH,
        )

    def red_copy(at, src, dst, step):
        return pltpu.make_async_remote_copy(
            src_ref=src,
            dst_ref=dst,
            send_sem=xs.at[at],
            recv_sem=xr.at[at],
            device_id={X: around(x + step, NX)},
            device_id_type=MESH,
        )

    right, left, across = around(x + 1, NX), around(x - 1, NX), around(x + 2, NX)
    steps = (1, -1)
    piece = [pl.ds(0, OWN // 2), pl.ds(OWN // 2, OWN // 2)]
    over = [
        [red_copy(2 * k + u, red_out.at[k, across, piece[u]], mid_in.at[k, piece[u]], steps[k]) for u in range(2)]
        for k in range(2)
    ]
    near = [red_copy(4 + k, red_out.at[1 - k, (right, left)[k]], red_in.at[k], steps[k]) for k in range(2)]
    merged = [
        [
            red_copy(6 + 2 * k + u, red_out.at[k, (right, left)[k], piece[u]], red_in.at[2 + k, piece[u]], steps[k])
            for u in range(2)
        ]
        for k in range(2)
    ]
    with scope("proj_sib"):
        for side in range(2):
            sib_out[side] = project(other, side).astype(BF16).reshape(NX, OWN, half_d)
            sib_copy(side).start()
    with scope("proj_mine"):
        for side in range(2):
            part = project(c, side).reshape(NX, OWN, half_d)
            sib_copy(side).wait_recv()
            red_out[side] = (part + sib_in[side].astype(F32)).astype(BF16)
            for u in range(2):
                over[side][u].start()
        for k in range(2):
            near[k].start()
    with scope("red_mid"):
        for u in range(2):
            for k in range(2):
                over[k][u].wait_recv()
                place = (right, left)[k]
                red_out[k, place, piece[u]] = (
                    red_out[k, place, piece[u]].astype(F32) + mid_in[k, piece[u]].astype(F32)
                ).astype(BF16)
                merged[k][u].start()
    with scope("red_wait"):
        for k in range(2):
            near[k].wait_recv()
        for k in range(2):
            for u in range(2):
                merged[k][u].wait_recv()
    with scope("final"):
        low = red_out[0, x].astype(F32) + red_in[2].astype(F32) + red_in[1].astype(F32)
        high = red_out[1, x].astype(F32) + red_in[0].astype(F32) + red_in[3].astype(F32)
        squares = jnp.sum(low * low, axis=1, keepdims=True) + jnp.sum(high * high, axis=1, keepdims=True)
        scale = lax.rsqrt(squares * (1.0 / D) + EPS)
        out[:, :half_d] = (low * scale * post[:, :half_d]).astype(BF16)
        out[:, half_d:] = (high * scale * post[:, half_d:]).astype(BF16)

    with scope("drain"):
        for stream in [one for pair in first + streams for one in pair] + [to_slices, over_z, back]:
            stream.drain()
        for distance in range(1, NX):
            tok_out(distance).wait_send()
            tok_copy(NX + distance, tok_from(distance) + c, {C: other}).wait_send()
        tok_copy(0, tp, {C: other}).wait_send()
        for k in range(2):
            sib_copy(k).wait_send()
        for copy in over[0] + over[1] + near + merged[0] + merged[1]:
            copy.wait_send()
        shift.wait_send()


def per_device(
    tokens_in, norm_gain, w_query, w_forget, w_input, w_rgate, w_pool_in, w_pgate,
    floor_rate, extra_logdecay, state_gain, pool_mix, pool_gain, out_rec, out_pool, post_gain,
):
    anywhere = pl.BlockSpec(memory_space=pl.ANY)
    dma = pltpu.SemaphoreType.DMA
    rows = D // 64
    run = pl.pallas_call(
        layer,
        name="layer",
        out_shape=jax.ShapeDtypeStruct((OWN, D), BF16),
        in_specs=[anywhere] * 16,
        out_specs=pl.BlockSpec(memory_space=pltpu.VMEM),
        scratch_shapes=[
            pltpu.VMEM((NR, NR, rows, DK), BF16),
            pltpu.VMEM((NR, NR, rows, DK), BF16),
            pltpu.VMEM((3, NR, NR, rows, DK), BF16),
            pltpu.VMEM((3, NR, NR, rows, DK), BF16),
            pltpu.VMEM((2 * NX, T, D // (2 * NX)), BF16),
            pltpu.VMEM((T, D), BF16),
            pltpu.VMEM((1, D), F32),
            pltpu.VMEM((1, DK), F32),
            pltpu.VMEM((1, T), F32),
            pltpu.VMEM((1, DK), F32),
            pltpu.VMEM((DK, DK), BF16),
            pltpu.VMEM((1, DK), F32),
            pltpu.VMEM((1, D), F32),
            pltpu.VMEM((NR, 32, DK), BF16),
            pltpu.VMEM((NR, 32, DK), BF16),
            pltpu.VMEM((NR, 32, DK), BF16),
            pltpu.VMEM((NR, 16, DK), BF16),
            pltpu.VMEM((NR, 16, DK), BF16),
            pltpu.VMEM((16, DK), BF16),
            pltpu.VMEM((16, DK), BF16),
            pltpu.VMEM((NX, 2, OWN, 2 * DK), BF16),
            pltpu.VMEM((2, NX, OWN, D // 2), BF16),
            pltpu.VMEM((2, NX, OWN, D // 2), BF16),
            pltpu.VMEM((2, NX, OWN, D // 2), BF16),
            pltpu.VMEM((4, OWN, D // 2), BF16),
            pltpu.VMEM((2, OWN, D // 2), BF16),
            dma((9,)),
            dma((7,)),
            dma((8, NR)),
            dma((8, NR)),
            dma((8, CUTS * NR)),
            dma((8, CUTS * NR)),
            dma((2 * NX,)),
            dma((2 * NX,)),
            dma((3, NR)),
            dma((3, NR)),
            dma((1,)),
            dma((1,)),
            dma((2,)),
            dma((2,)),
            dma((10,)),
            dma((10,)),
        ],
        compiler_params=pltpu.CompilerParams(
            collective_id=0, has_side_effects=True, vmem_limit_bytes=32 * 1024 * 1024
        ),
    )
    operands = (
        tokens_in,
        w_query,
        w_forget,
        w_input,
        w_rgate,
        w_pool_in,
        w_pgate,
        out_rec.T,
        out_pool.T,
        norm_gain.reshape(1, -1),
        floor_rate.reshape(1, -1),
        extra_logdecay.reshape(1, -1),
        state_gain.reshape(1, -1),
        pool_mix.reshape(DK, DK),
        pool_gain.reshape(1, -1),
        post_gain.reshape(1, -1),
    )
    return run(*[pltpu.with_memory_space_constraint(a, pltpu.HBM) for a in operands])


def solution(mesh):
    torus = Mesh(mesh.devices.reshape(8, 8, 4, 2), ("sp_0", "sp_1", "tp_0", "tp_1"))
    return jax.shard_map(
        per_device,
        mesh=torus,
        in_specs=(
            P(SP, TP),
            P(),
            P(SP, TP),
            P(SP, TP),
            P(SP, TP),
            P(SP, TP),
            P(SP, TP),
            P(SP, TP),
            P(TP),
            P(SP, TP),
            P(TP),
            P(TP, None, None),
            P(TP),
            P(TP, SP),
            P(TP, SP),
            P(),
        ),
        out_specs=P(SP_TP, None),
        check_vma=False,
    )
```

```python
import functools

import jax
import jax.numpy as jnp
from jax import lax
from jax.experimental import pallas as pl
from jax.experimental.pallas import tpu as pltpu
from jax.sharding import Mesh
from jax.sharding import PartitionSpec as P

SP = ("sp_0", "sp_1")
TP = ("tp_0", "tp_1")
SP_TP = ("sp_0", "sp_1", "tp_0", "tp_1")
Z, Y, X, C = "sp_0", "sp_1", "tp_0", "tp_1"
MESH = pl.DeviceIdType.MESH
EPS = 1e-06
DK = 128
NR = 8
NX = 4
T = 256
D = 2048
OWN = T // (2 * NX)
F32 = jnp.float32
BF16 = jnp.bfloat16
CUTS = 2
SPAN = NR // CUTS
ORDER = (4, 3, 5, 2, 6, 1, 7)


def mm(a, b, ca=1, cb=0):
    return lax.dot_general(a, b, (((ca,), (cb,)), ((), ())), preferred_element_type=F32)


def halves(a):
    hi = a.astype(BF16)
    return hi, (a - hi.astype(F32)).astype(BF16)


def mm3(a, b, ca=1, cb=0):
    ah, al = halves(a)
    bh, bl = halves(b)
    return mm(ah, bh, ca, cb) + (mm(ah, bl, ca, cb) + mm(al, bh, ca, cb))


def mm2(a, b, ca=1, cb=0):
    ah, al = halves(a)
    return mm(ah, b, ca, cb) + mm(al, b, ca, cb)


def silu(a):
    return a / (1.0 + jnp.exp(-a))


def around(value, count):
    return lax.rem(value + 2 * count, count)


def remote(src, dst, send, recv, where):
    return pltpu.make_async_remote_copy(
        src_ref=src, dst_ref=dst, send_sem=send, recv_sem=recv, device_id=where, device_id_type=MESH
    )


class Stream:
    def __init__(self, at, wide, long, w, l, sign, sems):
        self.at, self.wide, self.long, self.w, self.l, self.sign = at, wide, long, w, l, sign
        self.send1, self.send2, self.recv1, self.recv2 = sems

    def first_copy(self, distance, origin, recv):
        block = self.at(pl.ds(origin, 1), pl.ds(self.l, 1))
        return remote(block, block, self.send1, recv, {self.wide: around(self.w + distance, NR)})

    def first_start(self):
        for distance in ORDER:
            self.first_copy(distance, self.w, self.recv1).start()

    def first_arrive(self):
        view = self.at(pl.ds(0, NR - 1), pl.ds(self.l, 1))
        remote(view, view, self.send1, self.recv1, {self.wide: around(self.w + 1, NR)}).wait_recv()

    def drain(self):
        view = self.at(pl.ds(0, NR - 1), pl.ds(self.l, 1))
        remote(view, view, self.send1, self.send1, {self.wide: around(self.w + 1, NR)}).wait_send()
        view = self.at(pl.ds(0, NR), pl.ds(0, NR - 1))
        remote(view, view, self.send2, self.send2, {self.long: around(self.l + 1, NR)}).wait_send()

    def origin(self, step, back):
        sign = -self.sign if back else self.sign
        return around(self.l - sign * step, NR)

    def steps(self, back):
        return NR // 2 - 1 if back else NR // 2

    def sem(self, step, back, cut):
        if step == self.steps(back) - 1:
            return self.recv2.at[1 if back else 0]
        return self.recv2.at[2 + CUTS * (NR // 2 - 1 + step if back else step) + cut]

    def copy(self, step, back, cut, origin):
        sign = -self.sign if back else self.sign
        block = self.at(pl.ds(SPAN * cut, SPAN), pl.ds(origin, 1))
        where = {self.long: around(self.l + sign, NR)}
        return remote(block, block, self.send2, self.sem(step, back, cut), where)

    def start(self, step, back, cut):
        if step < self.steps(back):
            self.copy(step, back, cut, self.origin(step, back)).start()

    def relay(self, step, back, cut):
        if step < self.steps(back) - 1:
            self.copy(step, back, cut, self.origin(step + 1, back)).wait_recv()
            self.start(step + 1, back, cut)
        elif step == self.steps(back) - 1 and cut == CUTS - 1:
            block = self.at(pl.ds(0, NR), pl.ds(self.origin(step + 1, back), 1))
            where = {self.long: around(self.l + self.sign, NR)}
            remote(block, block, self.send2, self.sem(step, back, cut), where).wait_recv()


class FastStream(Stream):
    def first_start(self):
        pair, twin = self.w // 2, self.w + 1 - 2 * lax.rem(self.w, 2)
        for ahead in (2, 1, 3):
            for k in range(2):
                place = 2 * lax.rem(pair + ahead, NR // 2) + k
                block = self.at(pl.ds(self.w, 1), pl.ds(self.l, 1))
                remote(block, block, self.send1, self.recv1.at[NR // 2 - ahead], {self.wide: place}).start()
        block = self.at(pl.ds(self.w, 1), pl.ds(self.l, 1))
        remote(block, block, self.send1, self.recv1.at[0], {self.wide: twin}).start()

    def pair_at(self, ahead):
        return 2 * lax.rem(self.w // 2 + ahead, NR // 2)

    def first_arrive(self, ahead):
        twin = self.w + 1 - 2 * lax.rem(self.w, 2)
        if ahead == 0:
            view = self.at(pl.ds(twin, 1), pl.ds(self.l, 1))
        else:
            view = self.at(pl.ds(self.pair_at(ahead), 2), pl.ds(self.l, 1))
        remote(view, view, self.send1, self.recv1.at[ahead], {self.wide: twin}).wait_recv()

    def hop(self, ahead, origin, move, sem):
        block = self.at(pl.ds(self.pair_at(ahead), 2), pl.ds(origin, 1))
        where = {self.long: around(self.l + self.sign * move, NR)}
        return remote(block, block, self.send2, self.recv2.at[sem], where)

    def send_own(self, ahead):
        for move, sem in ((2, 5 + ahead), (-2, 9 + ahead), (1, 0), (-1, 3)):
            self.hop(ahead, self.l, move, sem).start()

    def send_on(self, ahead):
        origin = around(self.l - 2 * self.sign, NR)
        self.hop(ahead, origin, 2, 5 + ahead).wait_recv()
        self.hop(ahead, origin, 2, 2).start()
        self.hop(ahead, origin, 1, 1).start()
        origin = around(self.l + 2 * self.sign, NR)
        self.hop(ahead, origin, -2, 9 + ahead).wait_recv()
        self.hop(ahead, origin, -1, 4).start()

    def finish(self):
        for move, sem in ((1, 0), (-1, 3), (3, 1), (-3, 4), (4, 2)):
            block = self.at(pl.ds(0, NR), pl.ds(around(self.l - self.sign * move, NR), 1))
            where = {self.long: around(self.l + self.sign, NR)}
            remote(block, block, self.send2, self.recv2.at[sem], where).wait_recv()


class Direct:
    def __init__(self, held, axis, me, send, recv, out=None):
        self.out, self.held, self.axis, self.me, self.send, self.recv = out, held, axis, me, send, recv

    def start(self):
        for distance in ORDER:
            place = around(self.me + distance, NR)
            src = self.held.at[self.me] if self.out is None else self.out.at[place]
            remote(src, self.held.at[self.me], self.send, self.recv, {self.axis: place}).start()

    def whole(self):
        view = self.held.at[pl.ds(0, NR - 1)]
        return remote(view, view, self.send, self.recv, {self.axis: around(self.me + 1, NR)})

    def arrive(self):
        self.whole().wait_recv()

    def drain(self):
        self.whole().wait_send()


def log_rows(total):
    hi = total.astype(BF16)
    rest = total - hi.astype(F32)
    mid = rest.astype(BF16)
    low = (rest - mid.astype(F32)).astype(BF16)
    place = lax.broadcasted_iota(jnp.int32, (16, DK), 0)
    parts = jnp.where(place == 1, mid.astype(F32), jnp.where(place == 2, low.astype(F32), 0.0))
    return jnp.where(place == 0, hi.astype(F32), parts).astype(BF16)


def from_message(ref, k):
    whole = ref[k].astype(F32)
    return whole[:16], jnp.sum(whole[16:], axis=0, keepdims=True)


def layer(
    tok, wq, wf, wi, wr, wp, wg, orec, opool,
    ngain_in, rate_in, extra_in, sgain_in, pmix_in, pgain_in, post_in,
    out,
    g0a, g0b, g1a, g1b, xg, sc,
    ngain, rate, extra, sgain, pmix, pgain, post,
    st_out, st1, st2, st3_out, st3, rows_out, rows_in, yb, sib_out, sib_in, red_out, red_in, mid_in,
    lsem, vsem, f1r, f2r, p1s, p1r, p2s, p2r, ts, tr, ss, sr, ps, pr, bs, br, xs, xr,
):
    scope = jax.named_scope
    z, y, x, c = lax.axis_index(Z), lax.axis_index(Y), lax.axis_index(X), lax.axis_index(C)
    tp = 2 * x + c
    sign = 1 - 2 * c
    other = 1 - c

    after_y = around(y + 1, NR)
    after_z = jnp.where(y == NR - 1, around(z + 1, NR), z)
    before_y = around(y - 1, NR)
    before_z = jnp.where(y == 0, around(z - 1, NR), z)
    with scope("barrier"):
        barrier = pltpu.get_barrier_semaphore()
        for k in ORDER:
            pl.semaphore_signal(barrier, 1, device_id={Y: around(y + k, NR)}, device_id_type=MESH)
            pl.semaphore_signal(barrier, 1, device_id={Z: around(z + k, NR)}, device_id_type=MESH)
        for k in range(1, NX):
            pl.semaphore_signal(barrier, 1, device_id={X: around(x + k, NX)}, device_id_type=MESH)
        pl.semaphore_signal(barrier, 1, device_id={C: other}, device_id_type=MESH)
        pl.semaphore_signal(barrier, 1, device_id={Z: before_z, Y: before_y}, device_id_type=MESH)

    local = [
        pltpu.make_async_copy(src, dst, lsem.at[k])
        for k, (src, dst) in enumerate(
            (
                (wf, g0a.at[z, y]),
                (wi, g0b.at[z, y]),
                (tok, xg.at[tp]),
                (wq, g1a.at[0, z, y]),
                (wr, g1a.at[1, z, y]),
                (orec, g1a.at[2, z, y]),
                (wp, g1b.at[0, z, y]),
                (wg, g1b.at[1, z, y]),
                (opool, g1b.at[2, z, y]),
            )
        )
    ]
    vectors = [
        pltpu.make_async_copy(src, dst, vsem.at[k])
        for k, (src, dst) in enumerate(
            (
                (ngain_in, ngain),
                (rate_in, rate),
                (extra_in, extra),
                (sgain_in, sgain),
                (pmix_in, pmix),
                (pgain_in, pgain),
                (post_in, post),
            )
        )
    ]
    for copy in local + vectors:
        copy.start()
    with scope("barrier"):
        pl.semaphore_wait(barrier, 2 * (NR - 1) + NX - 1 + 2)

    def stream(kind, buffer, flip, at, recv1, recv2):
        sems = (p1s.at[at], p2s.at[at], recv1, recv2)
        if flip:
            return kind(lambda w, l: buffer.at[w, l], Z, Y, z, y, sign, sems)
        return kind(lambda w, l: buffer.at[l, w], Y, Z, y, z, sign, sems)

    fast = [
        stream(FastStream, buffer, flip, flip, f1r.at[flip], f2r.at[flip])
        for flip, buffer in enumerate((g0a, g0b))
    ]
    streams = [
        [
            stream(Stream, buffer.at[k], flip, 2 * k + 2 + flip, p1r.at[2 * k + flip], p2r.at[2 * k + flip])
            for flip, buffer in enumerate((g1a, g1b))
        ]
        for k in range(3)
    ]
    streams = [fast] + streams

    def start(k):
        with scope("first%d" % k):
            for one in streams[k]:
                one.first_arrive()
                for cut in range(CUTS):
                    for back in (False, True):
                        one.start(0, back, cut)

    def relay(k, step):
        with scope("relay%d%d" % (k, step)):
            for cut in range(CUTS):
                for back in (False, True):
                    for one in streams[k]:
                        one.relay(step, back, cut)

    def first_start(k):
        for one in streams[k]:
            one.first_start()

    def tok_copy(at, slot, where):
        return remote(xg.at[slot], xg.at[slot], ts.at[0], tr.at[at], where)

    def tok_from(distance):
        return 2 * around(x - distance, NX)

    with scope("sends"):
        local[0].wait()
        fast[0].first_start()
        local[1].wait()
        fast[1].first_start()
        local[2].wait()
        for distance in (2, 1, 3):
            tok_copy(distance, tp, {X: around(x + distance, NX)}).start()
        tok_copy(0, tp, {C: other}).start()
        for k in range(3, 9):
            local[k].wait()
        first_start(1)
        first_start(2)
        for copy in vectors:
            copy.wait()

    for ahead in (0, 1, 3, 2):
        with scope("own%d" % ahead):
            for one in fast:
                one.first_arrive(ahead)
                one.send_own(ahead)
    with scope("tokens"):
        for distance in (1, 3, 2):
            tok_copy(distance, tok_from(distance) + c, {X: around(x + distance, NX)}).wait_recv()
            tok_copy(0, tok_from(distance) + c, {C: other}).start()
    for ahead in (0, 1, 3, 2):
        with scope("on%d" % ahead):
            for one in fast:
                one.send_on(ahead)
    start(1)
    first_start(3)
    start(2)
    with scope("tokens2"):
        four = xg.at[pl.ds(0, NX)]
        remote(four, four, ts.at[0], tr.at[0], {C: other}).wait_recv()
    with scope("scale"):
        squares = jnp.zeros((T, 1), F32)
        for k in range(2 * NX):
            block = xg[k].astype(F32)
            squares = squares + jnp.sum(block * block, axis=1, keepdims=True)
            at = slice(k * (D // (2 * NX)), (k + 1) * (D // (2 * NX)))
            sc[:, at] = (block * ngain[:, at]).astype(BF16)
        inv_rms = lax.rsqrt(squares * (1.0 / D) + EPS)
    with scope("finish"):
        for one in fast:
            one.finish()

    with scope("proj_fv"):
        scaled = sc[...]
        forget = (mm(scaled, g0a[...].reshape(D, DK)) * inv_rms).astype(BF16).astype(F32)
        value = (mm(scaled, g0b[...].reshape(D, DK)) * inv_rms).astype(BF16)
    relay(1, 0)
    with scope("gates"):
        r = rate[...]
        series = r * (1.0 - r / 2 * (1.0 - r / 3 * (1.0 - r / 4 * (1.0 - r / 5 * (1.0 - r / 6)))))
        reach = jnp.where(r < 0.1, series, 1.0 - jnp.exp(-r))
        key = reach * (1.0 / (1.0 + jnp.exp(forget)))
        more = lax.dot_general(
            extra[...],
            jnp.ones((1, DK), F32),
            (((0,), (0,)), ((), ())),
            precision=lax.Precision.HIGHEST,
            preferred_element_type=F32,
        )
        logs = jnp.log1p(-key) + more
        row = lax.broadcasted_iota(jnp.int32, (T, T), 0)
        col = lax.broadcasted_iota(jnp.int32, (T, T), 1)
        lower = jnp.where(row >= col, 1.0, 0.0)
        cum = jnp.dot(lower, logs, precision=lax.Precision.HIGHEST, preferred_element_type=F32)
        last = cum[T - 1 : T, :]
        memory = mm2(key * jnp.exp(last - cum), value, 0, 0).T
        st_out[:, 0:16] = memory.astype(BF16).reshape(NR, 16, DK)
        st_out[:, 16:32] = jnp.broadcast_to(log_rows(last)[None], (NR, 16, DK))

    to_slices = Direct(st1, Y, y, ss.at[0], sr.at[0], st_out)
    over_z = Direct(st2, Z, z, ss.at[1], sr.at[1])
    back = Direct(st3, Y, y, ss.at[2], sr.at[2], st3_out)
    to_slices.start()
    st1[y] = st_out[y]
    relay(2, 0)
    start(3)
    relay(1, 1)
    relay(2, 1)
    relay(3, 0)
    with scope("wait_y"):
        to_slices.arrive()
    with scope("chain_y"):
        state, total = jnp.zeros((16, DK), F32), jnp.zeros((1, DK), F32)
        inside, before = [], []
        for k in range(NR):
            inside.append(state)
            before.append(total)
            new_state, new_total = from_message(st1, k)
            state = jnp.exp(new_total) * state + new_state
            total = total + new_total
        st2[z] = jnp.concatenate([state.astype(BF16), log_rows(total)], axis=0)
    over_z.start()
    relay(1, 2)
    relay(2, 2)
    relay(3, 1)
    relay(1, 3)

    with scope("wait_z"):
        over_z.arrive()
    with scope("chain_z"):
        state = jnp.zeros((16, DK), F32)
        outer = state
        for k in range(NR):
            new_state, new_total = from_message(st2, k)
            state = jnp.exp(new_total) * state + new_state
            outer = jnp.where(k < z, state, outer)
        for k in range(NR):
            st3_out[k] = (jnp.exp(before[k]) * outer + inside[k]).astype(BF16)
    back.start()
    st3[y] = st3_out[y]
    with scope("proj_qp"):
        query = (mm(scaled, g1a[0].reshape(D, DK)) * inv_rms).astype(BF16)
        query = query.astype(F32) * DK ** (-0.5)
        pool = (mm(scaled, g1b[0].reshape(D, DK)) * inv_rms).astype(BF16)
        rows_out[...] = pool[T - 16 :, :]
    shift = remote(rows_out, rows_in, ps.at[0], pr.at[0], {Z: after_z, Y: after_y})
    shift.start()
    relay(3, 2)
    with scope("diag"):
        value32 = value.astype(F32)
        in_block = lax.rem(lax.broadcasted_iota(jnp.int32, (T, 1), 0), 8)
        decay = jnp.exp(logs)
        weight = query
        rec = jnp.sum(query * key, axis=1, keepdims=True) * value32
        for d in range(1, 8):
            weight = weight * (decay if d == 1 else pltpu.roll(decay, d - 1, 0))
            score = jnp.sum(weight * pltpu.roll(key, d, 0), axis=1, keepdims=True)
            rec = rec + jnp.where(in_block >= d, score, 0.0) * pltpu.roll(value32, d, 0)
    with scope("levels"):
        scores = jnp.zeros((T, T), F32)
        for half in (8, 16, 32, 64, 128):
            apart = cum.reshape(T // (2 * half), 2 * half, DK)
            apart = jnp.abs(apart - apart[:, half - 1 : half, :]).reshape(T, DK)
            fade = jnp.exp(-apart)
            level = mm3(query * fade, key * fade, 1, 1)
            mask = (row // (2 * half) == col // (2 * half)) & (row // half > col // half)
            scores = jnp.where(mask, level, scores)
        rec = rec + mm2(scores, value)
    with scope("pool"):
        shift.wait_recv()
        at_start = (z == 0) & (y == 0)
        earlier = jnp.where(at_start, 0.0, rows_in[...].astype(F32))
        pool32 = pool.astype(F32)
        two = jnp.concatenate([earlier, pool32], axis=0)
        two = two + pltpu.roll(two, 1, 0)
        four = two + pltpu.roll(two, 2, 0)
        eight = four + pltpu.roll(four, 4, 0)
        sixteen = eight + pltpu.roll(eight, 8, 0)
        kind = lax.rem(tp, 4)
        sums = jnp.where(kind == 2, eight, sixteen)
        sums = jnp.where(kind == 0, two, jnp.where(kind == 1, four, sums))
        width = jnp.where(kind == 0, 2, jnp.where(kind == 1, 4, jnp.where(kind == 2, 8, 16)))
        place = (z * NR + y) * T + lax.broadcasted_iota(jnp.int32, (T, 1), 0)
        count = jnp.minimum(place + 1, width).astype(F32)
        mixed = (sums[16:] / count - pool32).astype(BF16)
        mapped = mm(mixed, pmix[...]) * pgain[...]
        faded = query * jnp.exp(cum)
    relay(2, 3)
    with scope("proj_rg"):
        rgate = (mm(scaled, g1a[1].reshape(D, DK)) * inv_rms).astype(BF16).astype(F32)
        pgate = (mm(scaled, g1b[1].reshape(D, DK)) * inv_rms).astype(BF16).astype(F32)
        y_pool = (mapped * silu(pgate)).astype(BF16)
        gate = sgain[...] * silu(rgate)
    relay(3, 3)
    with scope("wait_back"):
        back.arrive()
    with scope("rec"):
        rec = rec + mm2(faded, st3[...].reshape(DK, DK), 1, 1)
        normed = rec * lax.rsqrt(jnp.mean(rec * rec, axis=1, keepdims=True) + EPS)
        y_rec = (normed * gate).astype(BF16)
        yb[...] = jnp.concatenate([y_rec, y_pool], axis=1).reshape(NX, 2, OWN, 2 * DK)

    half_d = D // 2

    def project(parity, side):
        left = yb[:, parity].reshape(NX * OWN, 2 * DK)
        at = slice(side * (NR // 2), (side + 1) * (NR // 2))
        return mm(left[:, :DK], g1a[2, at].reshape(half_d, DK), 1, 1) + mm(
            left[:, DK:], g1b[2, at].reshape(half_d, DK), 1, 1
        )

    def sib_copy(side):
        return remote(sib_out.at[side], sib_in.at[side], bs.at[0], br.at[side], {C: other})

    def red_copy(at, src, dst, step):
        return remote(src, dst, xs.at[0], xr.at[at], {X: around(x + step, NX)})

    right, left, across = around(x + 1, NX), around(x - 1, NX), around(x + 2, NX)
    steps = (1, -1)
    piece = [pl.ds(0, OWN // 2), pl.ds(OWN // 2, OWN // 2)]
    over = [
        [red_copy(2 * k + u, red_out.at[k, across, piece[u]], mid_in.at[k, piece[u]], steps[k]) for u in range(2)]
        for k in range(2)
    ]
    near = [red_copy(4, red_out.at[1 - k, (right, left)[k]], red_in.at[k], steps[k]) for k in range(2)]
    merged = [
        [
            red_copy(4, red_out.at[k, (right, left)[k], piece[u]], red_in.at[2 + k, piece[u]], steps[k])
            for u in range(2)
        ]
        for k in range(2)
    ]
    with scope("proj_sib"):
        for side in range(2):
            sib_out[side] = project(other, side).astype(BF16).reshape(NX, OWN, half_d)
            sib_copy(side).start()
    with scope("proj_mine"):
        for side in range(2):
            part = project(c, side).reshape(NX, OWN, half_d)
            sib_copy(side).wait_recv()
            red_out[side] = (part + sib_in[side].astype(F32)).astype(BF16)
            for u in range(2):
                over[side][u].start()
        for k in range(2):
            near[k].start()
    with scope("red_mid"):
        for u in range(2):
            for k in range(2):
                over[k][u].wait_recv()
                place = (right, left)[k]
                red_out[k, place, piece[u]] = (
                    red_out[k, place, piece[u]].astype(F32) + mid_in[k, piece[u]].astype(F32)
                ).astype(BF16)
                merged[k][u].start()
    with scope("red_wait"):
        red_copy(4, red_in, red_in, 1).wait_recv()
    with scope("final"):
        low = red_out[0, x].astype(F32) + red_in[2].astype(F32) + red_in[1].astype(F32)
        high = red_out[1, x].astype(F32) + red_in[0].astype(F32) + red_in[3].astype(F32)
        squares = jnp.sum(low * low, axis=1, keepdims=True) + jnp.sum(high * high, axis=1, keepdims=True)
        scale = lax.rsqrt(squares * (1.0 / D) + EPS)
        out[:, :half_d] = (low * scale * post[:, :half_d]).astype(BF16)
        out[:, half_d:] = (high * scale * post[:, half_d:]).astype(BF16)

    with scope("drain"):
        for one in [one for pair in streams for one in pair] + [to_slices, over_z, back]:
            one.drain()
        seven = xg.at[pl.ds(0, 2 * NX - 1)]
        remote(seven, seven, ts.at[0], tr.at[0], {C: other}).wait_send()
        remote(sib_out, sib_out, bs.at[0], br.at[0], {C: other}).wait_send()
        six = red_out.at[:, pl.ds(0, NX - 1)]
        remote(six, six, xs.at[0], xr.at[0], {X: right}).wait_send()
        shift.wait_send()


def per_device(
    tokens_in, norm_gain, w_query, w_forget, w_input, w_rgate, w_pool_in, w_pgate,
    floor_rate, extra_logdecay, state_gain, pool_mix, pool_gain, out_rec, out_pool, post_gain,
):
    anywhere = pl.BlockSpec(memory_space=pl.ANY)
    dma = pltpu.SemaphoreType.DMA
    rows = D // 64
    run = pl.pallas_call(
        layer,
        name="layer",
        out_shape=jax.ShapeDtypeStruct((OWN, D), BF16),
        in_specs=[anywhere] * 16,
        out_specs=pl.BlockSpec(memory_space=pltpu.VMEM),
        scratch_shapes=[
            pltpu.VMEM((NR, NR, rows, DK), BF16),
            pltpu.VMEM((NR, NR, rows, DK), BF16),
            pltpu.VMEM((3, NR, NR, rows, DK), BF16),
            pltpu.VMEM((3, NR, NR, rows, DK), BF16),
            pltpu.VMEM((2 * NX, T, D // (2 * NX)), BF16),
            pltpu.VMEM((T, D), BF16),
            pltpu.VMEM((1, D), F32),
            pltpu.VMEM((1, DK), F32),
            pltpu.VMEM((1, T), F32),
            pltpu.VMEM((1, DK), F32),
            pltpu.VMEM((DK, DK), BF16),
            pltpu.VMEM((1, DK), F32),
            pltpu.VMEM((1, D), F32),
            pltpu.VMEM((NR, 32, DK), BF16),
            pltpu.VMEM((NR, 32, DK), BF16),
            pltpu.VMEM((NR, 32, DK), BF16),
            pltpu.VMEM((NR, 16, DK), BF16),
            pltpu.VMEM((NR, 16, DK), BF16),
            pltpu.VMEM((16, DK), BF16),
            pltpu.VMEM((16, DK), BF16),
            pltpu.VMEM((NX, 2, OWN, 2 * DK), BF16),
            pltpu.VMEM((2, NX, OWN, D // 2), BF16),
            pltpu.VMEM((2, NX, OWN, D // 2), BF16),
            pltpu.VMEM((2, NX, OWN, D // 2), BF16),
            pltpu.VMEM((4, OWN, D // 2), BF16),
            pltpu.VMEM((2, OWN, D // 2), BF16),
            dma((9,)),
            dma((7,)),
            dma((2, NR // 2)),
            dma((2, 13)),
            dma((8,)),
            dma((6,)),
            dma((8,)),
            dma((6, 2 + CUTS * (NR - 3))),
            dma((1,)),
            dma((NX,)),
            dma((3,)),
            dma((3,)),
            dma((1,)),
            dma((1,)),
            dma((1,)),
            dma((2,)),
            dma((1,)),
            dma((5,)),
        ],
        compiler_params=pltpu.CompilerParams(
            collective_id=0, has_side_effects=True, vmem_limit_bytes=32 * 1024 * 1024
        ),
    )
    operands = (
        tokens_in,
        w_query,
        w_forget,
        w_input,
        w_rgate,
        w_pool_in,
        w_pgate,
        out_rec.T,
        out_pool.T,
        norm_gain.reshape(1, -1),
        floor_rate.reshape(1, -1),
        extra_logdecay.reshape(1, -1),
        state_gain.reshape(1, -1),
        pool_mix.reshape(DK, DK),
        pool_gain.reshape(1, -1),
        post_gain.reshape(1, -1),
    )
    return run(*[pltpu.with_memory_space_constraint(a, pltpu.HBM) for a in operands])


def solution(mesh):
    torus = Mesh(mesh.devices.reshape(8, 8, 4, 2), ("sp_0", "sp_1", "tp_0", "tp_1"))
    return jax.shard_map(
        per_device,
        mesh=torus,
        in_specs=(
            P(SP, TP),
            P(),
            P(SP, TP),
            P(SP, TP),
            P(SP, TP),
            P(SP, TP),
            P(SP, TP),
            P(SP, TP),
            P(TP),
            P(SP, TP),
            P(TP),
            P(TP, None, None),
            P(TP),
            P(TP, SP),
            P(TP, SP),
            P(),
        ),
        out_specs=P(SP_TP, None),
        check_vma=False,
    )
```

```python
import functools

import jax
import jax.numpy as jnp
from jax import lax
from jax.experimental import pallas as pl
from jax.experimental.pallas import tpu as pltpu
from jax.sharding import Mesh
from jax.sharding import PartitionSpec as P

SP = ("sp_0", "sp_1")
TP = ("tp_0", "tp_1")
SP_TP = ("sp_0", "sp_1", "tp_0", "tp_1")
Z, Y, X, C = "sp_0", "sp_1", "tp_0", "tp_1"
MESH = pl.DeviceIdType.MESH
EPS = 1e-06
DK = 128
NR = 8
NX = 4
T = 256
D = 2048
OWN = T // (2 * NX)
F32 = jnp.float32
BF16 = jnp.bfloat16
CUTS = 2
SPAN = NR // CUTS
ORDER = (4, 3, 5, 2, 6, 1, 7)


def mm(a, b, ca=1, cb=0):
    return lax.dot_general(a, b, (((ca,), (cb,)), ((), ())), preferred_element_type=F32)


def halves(a):
    hi = a.astype(BF16)
    return hi, (a - hi.astype(F32)).astype(BF16)


def mm3(a, b, ca=1, cb=0):
    ah, al = halves(a)
    bh, bl = halves(b)
    return mm(ah, bh, ca, cb) + (mm(ah, bl, ca, cb) + mm(al, bh, ca, cb))


def mm2(a, b, ca=1, cb=0):
    ah, al = halves(a)
    return mm(ah, b, ca, cb) + mm(al, b, ca, cb)


def silu(a):
    return a / (1.0 + jnp.exp(-a))


def around(value, count):
    return lax.rem(value + 2 * count, count)


def remote(src, dst, send, recv, where):
    return pltpu.make_async_remote_copy(
        src_ref=src, dst_ref=dst, send_sem=send, recv_sem=recv, device_id=where, device_id_type=MESH
    )


class Stream:
    def __init__(self, at, wide, long, w, l, sign, sems):
        self.at, self.wide, self.long, self.w, self.l, self.sign = at, wide, long, w, l, sign
        self.send1, self.send2, self.recv1, self.recv2 = sems

    def drain(self):
        view = self.at(pl.ds(0, NR), pl.ds(0, NR - 1))
        remote(view, view, self.send2, self.send2, {self.long: around(self.l + 1, NR)}).wait_send()

    def origin(self, step, back):
        sign = -self.sign if back else self.sign
        return around(self.l - sign * step, NR)

    def steps(self, back):
        return NR // 2 - 1 if back else NR // 2

    def sem(self, step, back, cut):
        if step == self.steps(back) - 1:
            return self.recv2.at[1 if back else 0]
        return self.recv2.at[2 + CUTS * (NR // 2 - 1 + step if back else step) + cut]

    def copy(self, step, back, cut, origin):
        sign = -self.sign if back else self.sign
        block = self.at(pl.ds(SPAN * cut, SPAN), pl.ds(origin, 1))
        where = {self.long: around(self.l + sign, NR)}
        return remote(block, block, self.send2, self.sem(step, back, cut), where)

    def start(self, step, back, cut):
        if step < self.steps(back):
            self.copy(step, back, cut, self.origin(step, back)).start()

    def relay(self, step, back, cut):
        if step < self.steps(back) - 1:
            self.copy(step, back, cut, self.origin(step + 1, back)).wait_recv()
            self.start(step + 1, back, cut)
        elif step == self.steps(back) - 1 and cut == CUTS - 1:
            block = self.at(pl.ds(0, NR), pl.ds(self.origin(step + 1, back), 1))
            where = {self.long: around(self.l + self.sign, NR)}
            remote(block, block, self.send2, self.sem(step, back, cut), where).wait_recv()


class Leaps:
    def __init__(self, part, axis, me, sign, send, recv):
        self.part, self.axis, self.me, self.sign, self.send, self.recv = part, axis, me, sign, send, recv

    def copy(self, move, origin, sem, count=1):
        block = self.part(origin, count)
        where = {self.axis: around(self.me + self.sign * move, NR)}
        return remote(block, block, self.send, self.recv.at[sem], where)

    def start(self):
        for move, sem in ((2, 0), (-2, 1), (1, 2), (-1, 2)):
            self.copy(move, self.me, sem).start()

    def go_on(self):
        origin = around(self.me - 2 * self.sign, NR)
        self.copy(2, origin, 0).wait_recv()
        self.copy(2, origin, 2).start()
        self.copy(1, origin, 2).start()
        origin = around(self.me + 2 * self.sign, NR)
        self.copy(-2, origin, 1).wait_recv()
        self.copy(-1, origin, 2).start()

    def arrive(self):
        self.copy(1, 0, 2, 5).wait_recv()

    def drain(self):
        self.copy(1, 0, 2, 7).wait_send()


class FastStream(Stream):
    def drain(self):
        view = self.at(pl.ds(0, NR - 1), pl.ds(self.l, 1))
        remote(view, view, self.send1, self.send1, {self.wide: around(self.w + 1, NR)}).wait_send()
        Stream.drain(self)

    def first_start(self):
        pair, twin = self.w // 2, self.w + 1 - 2 * lax.rem(self.w, 2)
        block = self.at(pl.ds(self.w, 1), pl.ds(self.l, 1))
        remote(block, block, self.send1, self.recv1.at[0], {self.wide: twin}).start()
        for ahead in (2, 1, 3):
            for k in range(2):
                place = 2 * lax.rem(pair + ahead, NR // 2) + k
                remote(block, block, self.send1, self.recv1.at[NR // 2 - ahead], {self.wide: place}).start()

    def pair_at(self, ahead):
        return 2 * lax.rem(self.w // 2 + ahead, NR // 2)

    def first_arrive(self, ahead):
        twin = self.w + 1 - 2 * lax.rem(self.w, 2)
        if ahead == 0:
            view = self.at(pl.ds(twin, 1), pl.ds(self.l, 1))
        else:
            view = self.at(pl.ds(self.pair_at(ahead), 2), pl.ds(self.l, 1))
        remote(view, view, self.send1, self.recv1.at[ahead], {self.wide: twin}).wait_recv()

    def hop(self, ahead, origin, move, sem):
        block = self.at(pl.ds(self.pair_at(ahead), 2), pl.ds(origin, 1))
        where = {self.long: around(self.l + self.sign * move, NR)}
        return remote(block, block, self.send2, self.recv2.at[sem], where)

    def send_own(self, ahead):
        for move, sem in ((2, 5 + ahead), (-2, 9 + ahead), (1, 0), (-1, 3)):
            self.hop(ahead, self.l, move, sem).start()

    def send_on(self, ahead):
        origin = around(self.l - 2 * self.sign, NR)
        self.hop(ahead, origin, 2, 5 + ahead).wait_recv()
        self.hop(ahead, origin, 2, 2).start()
        self.hop(ahead, origin, 1, 1).start()
        origin = around(self.l + 2 * self.sign, NR)
        self.hop(ahead, origin, -2, 9 + ahead).wait_recv()
        self.hop(ahead, origin, -1, 4).start()

    def finish(self):
        for move, sem in ((1, 0), (-1, 3), (3, 1), (-3, 4), (4, 2)):
            block = self.at(pl.ds(0, NR), pl.ds(around(self.l - self.sign * move, NR), 1))
            where = {self.long: around(self.l + self.sign, NR)}
            remote(block, block, self.send2, self.recv2.at[sem], where).wait_recv()


class Direct:
    def __init__(self, held, axis, me, send, recv, out=None):
        self.out, self.held, self.axis, self.me, self.send, self.recv = out, held, axis, me, send, recv

    def start(self):
        for distance in ORDER:
            place = around(self.me + distance, NR)
            src = self.held.at[self.me] if self.out is None else self.out.at[place]
            remote(src, self.held.at[self.me], self.send, self.recv, {self.axis: place}).start()

    def whole(self):
        view = self.held.at[pl.ds(0, NR - 1)]
        return remote(view, view, self.send, self.recv, {self.axis: around(self.me + 1, NR)})

    def arrive(self):
        self.whole().wait_recv()

    def drain(self):
        self.whole().wait_send()


def log_rows(total):
    hi = total.astype(BF16)
    rest = total - hi.astype(F32)
    mid = rest.astype(BF16)
    low = (rest - mid.astype(F32)).astype(BF16)
    place = lax.broadcasted_iota(jnp.int32, (16, DK), 0)
    parts = jnp.where(place == 1, mid.astype(F32), jnp.where(place == 2, low.astype(F32), 0.0))
    return jnp.where(place == 0, hi.astype(F32), parts).astype(BF16)


def from_message(ref, k):
    whole = ref[k].astype(F32)
    return whole[:16], jnp.sum(whole[16:], axis=0, keepdims=True)


def layer(
    tok, wq, wf, wi, wr, wp, wg, orec, opool,
    ngain_in, rate_in, extra_in, sgain_in, pmix_in, pgain_in, post_in,
    out,
    g0a, g0b, g1a, g1b, xg, sc,
    ngain, rate, extra, sgain, pmix, pgain, post,
    st_out, st1, st2, st3_out, st3, rows_out, rows_in, yb, early, sib_out, sib_in, red_out, red_in, mid_in,
    lsem, vsem, f1r, f2r, p1s, p1r, p2s, p2r, ts, tr, ss, sr, ps, pr, bs, br, xs, xr,
):
    scope = jax.named_scope
    z, y, x, c = lax.axis_index(Z), lax.axis_index(Y), lax.axis_index(X), lax.axis_index(C)
    tp = 2 * x + c
    sign = 1 - 2 * c
    other = 1 - c

    after_y = around(y + 1, NR)
    after_z = jnp.where(y == NR - 1, around(z + 1, NR), z)
    before_y = around(y - 1, NR)
    before_z = jnp.where(y == 0, around(z - 1, NR), z)
    with scope("barrier"):
        barrier = pltpu.get_barrier_semaphore()
        for k in ORDER:
            pl.semaphore_signal(barrier, 1, device_id={Y: around(y + k, NR)}, device_id_type=MESH)
            pl.semaphore_signal(barrier, 1, device_id={Z: around(z + k, NR)}, device_id_type=MESH)
        for k in range(1, NX):
            pl.semaphore_signal(barrier, 1, device_id={X: around(x + k, NX)}, device_id_type=MESH)
        pl.semaphore_signal(barrier, 1, device_id={C: other}, device_id_type=MESH)
        pl.semaphore_signal(barrier, 1, device_id={Z: before_z, Y: before_y}, device_id_type=MESH)

    local = [
        pltpu.make_async_copy(src, dst, lsem.at[k])
        for k, (src, dst) in enumerate(
            (
                (wf, g0a.at[z, y]),
                (wi, g0b.at[z, y]),
                (tok, xg.at[tp]),
                (wq, g1a.at[0, z, y]),
                (wr, g1a.at[1, z, y]),
                (orec, g1a.at[2, z, y]),
                (wp, g1b.at[0, z, y]),
                (wg, g1b.at[1, z, y]),
                (opool, g1b.at[2, z, y]),
            )
        )
    ]
    vectors = [
        pltpu.make_async_copy(src, dst, vsem.at[k])
        for k, (src, dst) in enumerate(
            (
                (ngain_in, ngain),
                (rate_in, rate),
                (extra_in, extra),
                (sgain_in, sgain),
                (pmix_in, pmix),
                (pgain_in, pgain),
                (post_in, post),
            )
        )
    ]
    for copy in local + vectors:
        copy.start()
    with scope("barrier"):
        pl.semaphore_wait(barrier, 2 * (NR - 1) + NX - 1 + 2)

    def stream(kind, buffer, flip, at, recv1, recv2):
        sems = (p1s.at[flip], p2s.at[at], recv1, recv2)
        if flip:
            return kind(lambda w, l: buffer.at[w, l], Z, Y, z, y, sign, sems)
        return kind(lambda w, l: buffer.at[l, w], Y, Z, y, z, sign, sems)

    fast = [
        stream(FastStream, buffer, flip, flip, f1r.at[flip], f2r.at[flip])
        for flip, buffer in enumerate((g0a, g0b))
    ]
    streams = [fast] + [
        [
            stream(Stream, buffer.at[k], flip, 2 * k + 2 + flip, None, p2r.at[2 * k + flip])
            for flip, buffer in enumerate((g1a, g1b))
        ]
        for k in range(3)
    ]
    rest = [
        Leaps(lambda o, n: g1a.at[:, z, pl.ds(o, n)], Y, y, sign, p1s.at[2], p1r.at[0]),
        Leaps(lambda o, n: g1b.at[:, pl.ds(o, n), y], Z, z, sign, p1s.at[3], p1r.at[1]),
    ]

    def start(k):
        with scope("first%d" % k):
            for cut in range(CUTS):
                for back in (False, True):
                    for one in streams[k]:
                        one.start(0, back, cut)

    def relay(k, step):
        with scope("relay%d%d" % (k, step)):
            for cut in range(CUTS):
                for back in (False, True):
                    for one in streams[k]:
                        one.relay(step, back, cut)

    def tok_copy(at, slot, where):
        return remote(xg.at[slot], xg.at[slot], ts.at[0], tr.at[at], where)

    def tok_from(distance):
        return 2 * around(x - distance, NX)

    with scope("sends"):
        local[0].wait()
        fast[0].first_start()
        local[1].wait()
        fast[1].first_start()
        local[2].wait()
        for distance in (2, 1, 3):
            tok_copy(distance, tp, {X: around(x + distance, NX)}).start()
        tok_copy(0, tp, {C: other}).start()
        for k in range(3, 9):
            local[k].wait()
        for one in rest:
            one.start()
        for copy in vectors:
            copy.wait()

    for ahead in (0, 1, 3, 2):
        with scope("own%d" % ahead):
            for one in fast:
                one.first_arrive(ahead)
                one.send_own(ahead)
    with scope("leap"):
        for one in rest:
            one.go_on()
    for ahead in (0, 1, 3, 2):
        with scope("on%d" % ahead):
            for one in fast:
                one.send_on(ahead)
    with scope("tokens"):
        for distance in (1, 3, 2):
            tok_copy(distance, tok_from(distance) + c, {X: around(x + distance, NX)}).wait_recv()
            tok_copy(0, tok_from(distance) + c, {C: other}).start()
    with scope("rest"):
        for one in rest:
            one.arrive()
    start(1)
    start(2)
    start(3)
    with scope("tokens2"):
        four = xg.at[pl.ds(0, NX)]
        remote(four, four, ts.at[0], tr.at[0], {C: other}).wait_recv()
    with scope("scale"):
        squares = jnp.zeros((T, 1), F32)
        for k in range(2 * NX):
            block = xg[k].astype(F32)
            squares = squares + jnp.sum(block * block, axis=1, keepdims=True)
            at = slice(k * (D // (2 * NX)), (k + 1) * (D // (2 * NX)))
            sc[:, at] = (block * ngain[:, at]).astype(BF16)
        inv_rms = lax.rsqrt(squares * (1.0 / D) + EPS)
    with scope("finish"):
        for one in fast:
            one.finish()

    with scope("proj_fv"):
        scaled = sc[...]
        forget = (mm(scaled, g0a[...].reshape(D, DK)) * inv_rms).astype(BF16).astype(F32)
        value = (mm(scaled, g0b[...].reshape(D, DK)) * inv_rms).astype(BF16)
    relay(1, 0)
    with scope("gates"):
        r = rate[...]
        series = r * (1.0 - r / 2 * (1.0 - r / 3 * (1.0 - r / 4 * (1.0 - r / 5 * (1.0 - r / 6)))))
        reach = jnp.where(r < 0.1, series, 1.0 - jnp.exp(-r))
        key = reach * (1.0 / (1.0 + jnp.exp(forget)))
        more = lax.dot_general(
            extra[...],
            jnp.ones((1, DK), F32),
            (((0,), (0,)), ((), ())),
            precision=lax.Precision.HIGHEST,
            preferred_element_type=F32,
        )
        logs = jnp.log1p(-key) + more
        row = lax.broadcasted_iota(jnp.int32, (T, T), 0)
        col = lax.broadcasted_iota(jnp.int32, (T, T), 1)
        lower = jnp.where(row >= col, 1.0, 0.0)
        cum = jnp.dot(lower, logs, precision=lax.Precision.HIGHEST, preferred_element_type=F32)
        last = cum[T - 1 : T, :]
        memory = mm2(key * jnp.exp(last - cum), value, 0, 0).T
        st_out[:, 0:16] = memory.astype(BF16).reshape(NR, 16, DK)
        st_out[:, 16:32] = jnp.broadcast_to(log_rows(last)[None], (NR, 16, DK))

    to_slices = Direct(st1, Y, y, ss.at[0], sr.at[0], st_out)
    over_z = Direct(st2, Z, z, ss.at[1], sr.at[1])
    back = Direct(st3, Y, y, ss.at[2], sr.at[2], st3_out)
    to_slices.start()
    st1[y] = st_out[y]
    relay(2, 0)
    relay(3, 0)
    relay(1, 1)
    relay(2, 1)
    with scope("wait_y"):
        to_slices.arrive()
    with scope("chain_y"):
        state, total = jnp.zeros((16, DK), F32), jnp.zeros((1, DK), F32)
        inside, before = [], []
        for k in range(NR):
            inside.append(state)
            before.append(total)
            new_state, new_total = from_message(st1, k)
            state = jnp.exp(new_total) * state + new_state
            total = total + new_total
        st2[z] = jnp.concatenate([state.astype(BF16), log_rows(total)], axis=0)
    over_z.start()
    relay(3, 1)
    relay(1, 2)
    relay(2, 2)
    with scope("wait_z"):
        over_z.arrive()
    with scope("chain_z"):
        state = jnp.zeros((16, DK), F32)
        outer = state
        for k in range(NR):
            new_state, new_total = from_message(st2, k)
            state = jnp.exp(new_total) * state + new_state
            outer = jnp.where(k < z, state, outer)
        for k in range(NR):
            st3_out[k] = (jnp.exp(before[k]) * outer + inside[k]).astype(BF16)
    back.start()
    st3[y] = st3_out[y]
    relay(3, 2)
    relay(1, 3)
    with scope("proj_qp"):
        query = (mm(scaled, g1a[0].reshape(D, DK)) * inv_rms).astype(BF16)
        query = query.astype(F32) * DK ** (-0.5)
        pool = (mm(scaled, g1b[0].reshape(D, DK)) * inv_rms).astype(BF16)
        rows_out[...] = pool[T - 16 :, :]
    shift = remote(rows_out, rows_in, ps.at[0], pr.at[0], {Z: after_z, Y: after_y})
    shift.start()
    relay(2, 3)
    with scope("diag"):
        value32 = value.astype(F32)
        in_block = lax.rem(lax.broadcasted_iota(jnp.int32, (T, 1), 0), 8)
        decay = jnp.exp(logs)
        weight = query
        rec = jnp.sum(query * key, axis=1, keepdims=True) * value32
        for d in range(1, 8):
            weight = weight * (decay if d == 1 else pltpu.roll(decay, d - 1, 0))
            score = jnp.sum(weight * pltpu.roll(key, d, 0), axis=1, keepdims=True)
            rec = rec + jnp.where(in_block >= d, score, 0.0) * pltpu.roll(value32, d, 0)
    with scope("levels"):
        scores = jnp.zeros((T, T), F32)
        for half in (8, 16, 32, 64, 128):
            apart = cum.reshape(T // (2 * half), 2 * half, DK)
            apart = jnp.abs(apart - apart[:, half - 1 : half, :]).reshape(T, DK)
            fade = jnp.exp(-apart)
            level = mm3(query * fade, key * fade, 1, 1)
            mask = (row // (2 * half) == col // (2 * half)) & (row // half > col // half)
            scores = jnp.where(mask, level, scores)
        rec = rec + mm2(scores, value)
    with scope("pool"):
        shift.wait_recv()
        at_start = (z == 0) & (y == 0)
        earlier = jnp.where(at_start, 0.0, rows_in[...].astype(F32))
        pool32 = pool.astype(F32)
        two = jnp.concatenate([earlier, pool32], axis=0)
        two = two + pltpu.roll(two, 1, 0)
        four = two + pltpu.roll(two, 2, 0)
        eight = four + pltpu.roll(four, 4, 0)
        sixteen = eight + pltpu.roll(eight, 8, 0)
        kind = lax.rem(tp, 4)
        sums = jnp.where(kind == 2, eight, sixteen)
        sums = jnp.where(kind == 0, two, jnp.where(kind == 1, four, sums))
        width = jnp.where(kind == 0, 2, jnp.where(kind == 1, 4, jnp.where(kind == 2, 8, 16)))
        place = (z * NR + y) * T + lax.broadcasted_iota(jnp.int32, (T, 1), 0)
        count = jnp.minimum(place + 1, width).astype(F32)
        mixed = (sums[16:] / count - pool32).astype(BF16)
        mapped = mm(mixed, pmix[...]) * pgain[...]
        faded = query * jnp.exp(cum)
    with scope("proj_rg"):
        rgate = (mm(scaled, g1a[1].reshape(D, DK)) * inv_rms).astype(BF16).astype(F32)
        pgate = (mm(scaled, g1b[1].reshape(D, DK)) * inv_rms).astype(BF16).astype(F32)
        y_pool = (mapped * silu(pgate)).astype(BF16)
        gate = sgain[...] * silu(rgate)
    relay(3, 3)
    half_d = D // 2

    def project(left, weight, side):
        at = slice(side * (NR // 2), (side + 1) * (NR // 2))
        return mm(left, weight[2, at].reshape(half_d, DK), 1, 1)

    with scope("pooled"):
        yb[...] = y_pool.reshape(NX, 2, OWN, DK)
        for k, parity in enumerate((other, c)):
            for side in range(2):
                early[k, side] = project(yb[:, parity].reshape(NX * OWN, DK), g1b, side)
    with scope("wait_back"):
        back.arrive()
    with scope("rec"):
        rec = rec + mm2(faded, st3[...].reshape(DK, DK), 1, 1)
        normed = rec * lax.rsqrt(jnp.mean(rec * rec, axis=1, keepdims=True) + EPS)
        y_rec = (normed * gate).astype(BF16)
        yb[...] = y_rec.reshape(NX, 2, OWN, DK)

    def sib_copy(side):
        return remote(sib_out.at[side], sib_in.at[side], bs.at[0], br.at[side], {C: other})

    def red_copy(at, src, dst, step):
        return remote(src, dst, xs.at[0], xr.at[at], {X: around(x + step, NX)})

    right, left, across = around(x + 1, NX), around(x - 1, NX), around(x + 2, NX)
    steps = (1, -1)
    piece = [pl.ds(0, OWN // 2), pl.ds(OWN // 2, OWN // 2)]
    over = [
        [red_copy(2 * k + u, red_out.at[k, across, piece[u]], mid_in.at[k, piece[u]], steps[k]) for u in range(2)]
        for k in range(2)
    ]
    near = [red_copy(4, red_out.at[1 - k, (right, left)[k]], red_in.at[k], steps[k]) for k in range(2)]
    merged = [
        [
            red_copy(4, red_out.at[k, (right, left)[k], piece[u]], red_in.at[2 + k, piece[u]], steps[k])
            for u in range(2)
        ]
        for k in range(2)
    ]
    with scope("proj_sib"):
        for side in range(2):
            part = early[0, side] + project(yb[:, other].reshape(NX * OWN, DK), g1a, side)
            sib_out[side] = part.astype(BF16).reshape(NX, OWN, half_d)
            sib_copy(side).start()
    with scope("proj_mine"):
        for side in range(2):
            part = early[1, side] + project(yb[:, c].reshape(NX * OWN, DK), g1a, side)
            part = part.reshape(NX, OWN, half_d)
            sib_copy(side).wait_recv()
            red_out[side] = (part + sib_in[side].astype(F32)).astype(BF16)
            for u in range(2):
                over[side][u].start()
        for k in range(2):
            near[k].start()
    with scope("red_mid"):
        for u in range(2):
            for k in range(2):
                over[k][u].wait_recv()
                place = (right, left)[k]
                red_out[k, place, piece[u]] = (
                    red_out[k, place, piece[u]].astype(F32) + mid_in[k, piece[u]].astype(F32)
                ).astype(BF16)
                merged[k][u].start()
    with scope("red_wait"):
        red_copy(4, red_in, red_in, 1).wait_recv()
    with scope("final"):
        low = red_out[0, x].astype(F32) + red_in[2].astype(F32) + red_in[1].astype(F32)
        high = red_out[1, x].astype(F32) + red_in[0].astype(F32) + red_in[3].astype(F32)
        squares = jnp.sum(low * low, axis=1, keepdims=True) + jnp.sum(high * high, axis=1, keepdims=True)
        scale = lax.rsqrt(squares * (1.0 / D) + EPS)
        out[:, :half_d] = (low * scale * post[:, :half_d]).astype(BF16)
        out[:, half_d:] = (high * scale * post[:, half_d:]).astype(BF16)

    with scope("drain"):
        for one in [one for pair in streams for one in pair] + rest + [to_slices, over_z, back]:
            one.drain()
        seven = xg.at[pl.ds(0, 2 * NX - 1)]
        remote(seven, seven, ts.at[0], tr.at[0], {C: other}).wait_send()
        remote(sib_out, sib_out, bs.at[0], br.at[0], {C: other}).wait_send()
        six = red_out.at[:, pl.ds(0, NX - 1)]
        remote(six, six, xs.at[0], xr.at[0], {X: right}).wait_send()
        shift.wait_send()


def per_device(
    tokens_in, norm_gain, w_query, w_forget, w_input, w_rgate, w_pool_in, w_pgate,
    floor_rate, extra_logdecay, state_gain, pool_mix, pool_gain, out_rec, out_pool, post_gain,
):
    anywhere = pl.BlockSpec(memory_space=pl.ANY)
    dma = pltpu.SemaphoreType.DMA
    rows = D // 64
    run = pl.pallas_call(
        layer,
        name="layer",
        out_shape=jax.ShapeDtypeStruct((OWN, D), BF16),
        in_specs=[anywhere] * 16,
        out_specs=pl.BlockSpec(memory_space=pltpu.VMEM),
        scratch_shapes=[
            pltpu.VMEM((NR, NR, rows, DK), BF16),
            pltpu.VMEM((NR, NR, rows, DK), BF16),
            pltpu.VMEM((3, NR, NR, rows, DK), BF16),
            pltpu.VMEM((3, NR, NR, rows, DK), BF16),
            pltpu.VMEM((2 * NX, T, D // (2 * NX)), BF16),
            pltpu.VMEM((T, D), BF16),
            pltpu.VMEM((1, D), F32),
            pltpu.VMEM((1, DK), F32),
            pltpu.VMEM((1, T), F32),
            pltpu.VMEM((1, DK), F32),
            pltpu.VMEM((DK, DK), BF16),
            pltpu.VMEM((1, DK), F32),
            pltpu.VMEM((1, D), F32),
            pltpu.VMEM((NR, 32, DK), BF16),
            pltpu.VMEM((NR, 32, DK), BF16),
            pltpu.VMEM((NR, 32, DK), BF16),
            pltpu.VMEM((NR, 16, DK), BF16),
            pltpu.VMEM((NR, 16, DK), BF16),
            pltpu.VMEM((16, DK), BF16),
            pltpu.VMEM((16, DK), BF16),
            pltpu.VMEM((NX, 2, OWN, DK), BF16),
            pltpu.VMEM((2, 2, NX * OWN, D // 2), F32),
            pltpu.VMEM((2, NX, OWN, D // 2), BF16),
            pltpu.VMEM((2, NX, OWN, D // 2), BF16),
            pltpu.VMEM((2, NX, OWN, D // 2), BF16),
            pltpu.VMEM((4, OWN, D // 2), BF16),
            pltpu.VMEM((2, OWN, D // 2), BF16),
            dma((9,)),
            dma((7,)),
            dma((2, NR // 2)),
            dma((2, 13)),
            dma((4,)),
            dma((2, 3)),
            dma((8,)),
            dma((6, 2 + CUTS * (NR - 3))),
            dma((1,)),
            dma((NX,)),
            dma((3,)),
            dma((3,)),
            dma((1,)),
            dma((1,)),
            dma((1,)),
            dma((2,)),
            dma((1,)),
            dma((5,)),
        ],
        compiler_params=pltpu.CompilerParams(
            collective_id=0, has_side_effects=True, vmem_limit_bytes=32 * 1024 * 1024
        ),
    )
    operands = (
        tokens_in,
        w_query,
        w_forget,
        w_input,
        w_rgate,
        w_pool_in,
        w_pgate,
        out_rec.T,
        out_pool.T,
        norm_gain.reshape(1, -1),
        floor_rate.reshape(1, -1),
        extra_logdecay.reshape(1, -1),
        state_gain.reshape(1, -1),
        pool_mix.reshape(DK, DK),
        pool_gain.reshape(1, -1),
        post_gain.reshape(1, -1),
    )
    return run(*[pltpu.with_memory_space_constraint(a, pltpu.HBM) for a in operands])


def solution(mesh):
    torus = Mesh(mesh.devices.reshape(8, 8, 4, 2), ("sp_0", "sp_1", "tp_0", "tp_1"))
    return jax.shard_map(
        per_device,
        mesh=torus,
        in_specs=(
            P(SP, TP),
            P(),
            P(SP, TP),
            P(SP, TP),
            P(SP, TP),
            P(SP, TP),
            P(SP, TP),
            P(SP, TP),
            P(TP),
            P(SP, TP),
            P(TP),
            P(TP, None, None),
            P(TP),
            P(TP, SP),
            P(TP, SP),
            P(),
        ),
        out_specs=P(SP_TP, None),
        check_vma=False,
    )
```

```python
import functools

import jax
import jax.numpy as jnp
from jax import lax
from jax.experimental import pallas as pl
from jax.experimental.pallas import tpu as pltpu
from jax.sharding import Mesh
from jax.sharding import PartitionSpec as P

SP = ("sp_0", "sp_1")
TP = ("tp_0", "tp_1")
SP_TP = ("sp_0", "sp_1", "tp_0", "tp_1")
Z, Y, X, C = "sp_0", "sp_1", "tp_0", "tp_1"
MESH = pl.DeviceIdType.MESH
EPS = 1e-06
DK = 128
NR = 8
NX = 4
T = 256
D = 2048
OWN = T // (2 * NX)
F32 = jnp.float32
BF16 = jnp.bfloat16
CUTS = 2
SPAN = NR // CUTS
ORDER = (4, 3, 5, 2, 6, 1, 7)


def mm(a, b, ca=1, cb=0):
    return lax.dot_general(a, b, (((ca,), (cb,)), ((), ())), preferred_element_type=F32)


def halves(a):
    hi = a.astype(BF16)
    return hi, (a - hi.astype(F32)).astype(BF16)


def mm2(a, b, ca=1, cb=0):
    ah, al = halves(a)
    return mm(ah, b, ca, cb) + mm(al, b, ca, cb)


def silu(a):
    return a / (1.0 + jnp.exp(-a))


def around(value, count):
    return lax.rem(value + 2 * count, count)


def remote(src, dst, send, recv, where):
    return pltpu.make_async_remote_copy(
        src_ref=src, dst_ref=dst, send_sem=send, recv_sem=recv, device_id=where, device_id_type=MESH
    )


class Stream:
    def __init__(self, at, wide, long, w, l, sign, sems):
        self.at, self.wide, self.long, self.w, self.l, self.sign = at, wide, long, w, l, sign
        self.send1, self.send2, self.recv1, self.recv2 = sems

    def drain(self):
        view = self.at(pl.ds(0, NR), pl.ds(0, NR - 1))
        remote(view, view, self.send2, self.send2, {self.long: around(self.l + 1, NR)}).wait_send()

    def origin(self, step, back):
        sign = -self.sign if back else self.sign
        return around(self.l - sign * step, NR)

    def steps(self, back):
        return NR // 2 - 1 if back else NR // 2

    def sem(self, step, back, cut):
        if step == self.steps(back) - 1:
            return self.recv2.at[1 if back else 0]
        return self.recv2.at[2 + CUTS * (NR // 2 - 1 + step if back else step) + cut]

    def copy(self, step, back, cut, origin):
        sign = -self.sign if back else self.sign
        block = self.at(pl.ds(SPAN * cut, SPAN), pl.ds(origin, 1))
        where = {self.long: around(self.l + sign, NR)}
        return remote(block, block, self.send2, self.sem(step, back, cut), where)

    def start(self, step, back, cut):
        if step < self.steps(back):
            self.copy(step, back, cut, self.origin(step, back)).start()

    def arrive(self, step, back, cut):
        last = step == self.steps(back) - 1
        if step < self.steps(back) and (not last or cut == CUTS - 1):
            view = self.at(pl.ds(0, NR), pl.ds(0, 2)) if last else self.at(pl.ds(0, 2 * SPAN), pl.ds(0, 1))
            where = {self.long: around(self.l + self.sign, NR)}
            remote(view, view, self.send2, self.sem(step, back, cut), where).wait_recv()


class Leaps:
    def __init__(self, part, axis, me, sign, send, recv):
        self.part, self.axis, self.me, self.sign, self.send, self.recv = part, axis, me, sign, send, recv

    def copy(self, move, origin, sem, count=1):
        block = self.part(origin, count)
        where = {self.axis: around(self.me + self.sign * move, NR)}
        return remote(block, block, self.send, self.recv.at[sem], where)

    def start(self):
        for move, sem in ((2, 0), (-2, 1), (1, 2), (-1, 2)):
            self.copy(move, self.me, sem).start()

    def go_on(self):
        origin = around(self.me - 2 * self.sign, NR)
        self.copy(2, origin, 0).wait_recv()
        self.copy(2, origin, 2).start()
        self.copy(1, origin, 2).start()
        origin = around(self.me + 2 * self.sign, NR)
        self.copy(-2, origin, 1).wait_recv()
        self.copy(-1, origin, 2).start()

    def arrive(self):
        self.copy(1, 0, 2, 5).wait_recv()

    def drain(self):
        self.copy(1, 0, 2, 7).wait_send()


class FastStream(Stream):
    def drain(self):
        view = self.at(pl.ds(0, NR - 1), pl.ds(self.l, 1))
        remote(view, view, self.send1, self.send1, {self.wide: around(self.w + 1, NR)}).wait_send()
        Stream.drain(self)

    def first_start(self):
        pair, twin = self.w // 2, self.w + 1 - 2 * lax.rem(self.w, 2)
        block = self.at(pl.ds(self.w, 1), pl.ds(self.l, 1))
        remote(block, block, self.send1, self.recv1.at[0], {self.wide: twin}).start()
        for ahead in (2, 1, 3):
            for k in range(2):
                place = 2 * lax.rem(pair + ahead, NR // 2) + k
                remote(block, block, self.send1, self.recv1.at[NR // 2 - ahead], {self.wide: place}).start()

    def pair_at(self, ahead):
        return 2 * lax.rem(self.w // 2 + ahead, NR // 2)

    def wait(self, view, sem):
        where = {self.long: around(self.l + self.sign, NR)}
        remote(view, view, self.send2, sem, where).wait_recv()

    def first_arrive(self, ahead):
        self.wait(self.at(pl.ds(0, 4 if ahead else 2), pl.ds(0, 1)), self.recv1.at[ahead])

    def arrive(self, ahead, back):
        self.wait(self.at(pl.ds(0, 4), pl.ds(0, 1)), self.recv2.at[(9 if back else 5) + ahead])

    def finish(self):
        for sem in (0, 3, 1, 4, 2):
            self.wait(self.at(pl.ds(0, NR), pl.ds(0, 2)), self.recv2.at[sem])

    def hop(self, ahead, origin, move, sem):
        block = self.at(pl.ds(self.pair_at(ahead), 2), pl.ds(origin, 1))
        where = {self.long: around(self.l + self.sign * move, NR)}
        return remote(block, block, self.send2, self.recv2.at[sem], where)

    def send_two(self, ahead):
        self.hop(ahead, self.l, 2, 5 + ahead).start()
        self.hop(ahead, self.l, -2, 9 + ahead).start()

    def send_one(self, ahead):
        self.hop(ahead, self.l, 1, 0).start()
        self.hop(ahead, self.l, -1, 3).start()

    def send_on(self, ahead, back):
        if back:
            self.hop(ahead, around(self.l + 2 * self.sign, NR), -1, 4).start()
        else:
            origin = around(self.l - 2 * self.sign, NR)
            self.hop(ahead, origin, 2, 2).start()
            self.hop(ahead, origin, 1, 1).start()


class Direct:
    def __init__(self, held, axis, me, send, recv, out=None):
        self.out, self.held, self.axis, self.me, self.send, self.recv = out, held, axis, me, send, recv

    def start(self):
        for distance in ORDER:
            place = around(self.me + distance, NR)
            src = self.held.at[self.me] if self.out is None else self.out.at[place]
            remote(src, self.held.at[self.me], self.send, self.recv, {self.axis: place}).start()

    def whole(self):
        view = self.held.at[pl.ds(0, NR - 1)]
        return remote(view, view, self.send, self.recv, {self.axis: around(self.me + 1, NR)})

    def arrive(self):
        self.whole().wait_recv()

    def drain(self):
        self.whole().wait_send()


def thirds(a):
    hi = a.astype(BF16)
    rest = a - hi.astype(F32)
    mid = rest.astype(BF16)
    return hi, mid, (rest - mid.astype(F32)).astype(BF16)


def log_rows(total):
    hi, mid, low = thirds(total)
    place = lax.broadcasted_iota(jnp.int32, (16, DK), 0)
    parts = jnp.where(place == 1, mid.astype(F32), jnp.where(place == 2, low.astype(F32), 0.0))
    return jnp.where(place == 0, hi.astype(F32), parts).astype(BF16)


def from_message(ref, k):
    whole = ref[k].astype(F32)
    return whole[:16], jnp.sum(whole[16:], axis=0, keepdims=True)


def layer(
    tok, wq, wf, wi, wr, wp, wg, orec, opool,
    ngain_in, rate_in, extra_in, sgain_in, pmix_in, pgain_in, post_in,
    out,
    g0a, g0b, g1a, g1b, xg, sc,
    ngain, rate, extra, sgain, pmix, pgain, post,
    st_out, st1, st2, st3_out, st3, rows_out, rows_in, yb, early, sib_out, sib_in, red_out, red_in, mid_in,
    lsem, vsem, f1r, f2r, p1s, p1r, p2s, p2r, ts, tr, ss, sr, ps, pr, bs, br, xs, xr,
):
    scope = jax.named_scope
    z, y, x, c = lax.axis_index(Z), lax.axis_index(Y), lax.axis_index(X), lax.axis_index(C)
    tp = 2 * x + c
    sign = 1 - 2 * c
    other = 1 - c

    after_y = around(y + 1, NR)
    after_z = jnp.where(y == NR - 1, around(z + 1, NR), z)
    before_y = around(y - 1, NR)
    before_z = jnp.where(y == 0, around(z - 1, NR), z)
    with scope("barrier"):
        barrier = pltpu.get_barrier_semaphore()
        for k in ORDER:
            pl.semaphore_signal(barrier, 1, device_id={Y: around(y + k, NR)}, device_id_type=MESH)
            pl.semaphore_signal(barrier, 1, device_id={Z: around(z + k, NR)}, device_id_type=MESH)
        for k in range(1, NX):
            pl.semaphore_signal(barrier, 1, device_id={X: around(x + k, NX)}, device_id_type=MESH)
        pl.semaphore_signal(barrier, 1, device_id={C: other}, device_id_type=MESH)
        pl.semaphore_signal(barrier, 1, device_id={Z: before_z, Y: before_y}, device_id_type=MESH)

    local = [
        pltpu.make_async_copy(src, dst, lsem.at[k])
        for k, src, dst in (
            (0, wf, g0a.at[z, y]),
            (1, wi, g0b.at[z, y]),
            (2, tok, xg.at[tp]),
            (3, wq, g1a.at[0, z, y]),
            (3, wr, g1a.at[1, z, y]),
            (3, orec, g1a.at[2, z, y]),
            (4, wp, g1b.at[0, z, y]),
            (4, wg, g1b.at[1, z, y]),
            (4, opool, g1b.at[2, z, y]),
        )
    ]
    vectors = [
        pltpu.make_async_copy(src, dst, vsem.at[k])
        for k, (src, dst) in enumerate(
            (
                (ngain_in, ngain),
                (rate_in, rate),
                (extra_in, extra),
                (sgain_in, sgain),
                (pmix_in, pmix),
                (pgain_in, pgain),
                (post_in, post),
            )
        )
    ]
    for copy in local + vectors:
        copy.start()
    with scope("barrier"):
        pl.semaphore_wait(barrier, 2 * (NR - 1) + NX - 1 + 2)

    def stream(kind, buffer, flip, at, recv1, recv2):
        sems = (p1s.at[flip], p2s.at[at], recv1, recv2)
        if flip:
            return kind(lambda w, l: buffer.at[w, l], Z, Y, z, y, sign, sems)
        return kind(lambda w, l: buffer.at[l, w], Y, Z, y, z, sign, sems)

    fast = [
        stream(FastStream, buffer, flip, flip, f1r, f2r)
        for flip, buffer in enumerate((g0a, g0b))
    ]
    streams = [fast] + [
        [
            stream(Stream, buffer.at[k], flip, 2 * k + 2 + flip, None, p2r.at[k])
            for flip, buffer in enumerate((g1a, g1b))
        ]
        for k in range(3)
    ]
    rest = [
        Leaps(lambda o, n: g1a.at[:, z, pl.ds(o, n)], Y, y, sign, p1s.at[2], p1r.at[0]),
        Leaps(lambda o, n: g1b.at[:, pl.ds(o, n), y], Z, z, sign, p1s.at[3], p1r.at[1]),
    ]

    def start(k):
        with scope("first%d" % k):
            for cut in range(CUTS):
                for back in (False, True):
                    for one in streams[k]:
                        one.start(0, back, cut)

    def relay(k, step):
        with scope("relay%d%d" % (k, step)):
            for cut in range(CUTS):
                for back in (False, True):
                    streams[k][0].arrive(step, back, cut)
                    for one in streams[k]:
                        one.start(step + 1, back, cut)

    def tok_copy(at, slot, where):
        return remote(xg.at[slot], xg.at[slot], ts.at[0], tr.at[at], where)

    def tok_from(distance):
        return 2 * around(x - distance, NX)

    with scope("sends"):
        local[0].wait()
        fast[0].first_start()
        local[1].wait()
        fast[1].first_start()
        local[2].wait()
        for distance in (2, 1, 3):
            tok_copy(distance, tp, {X: around(x + distance, NX)}).start()
        tok_copy(0, tp, {C: other}).start()
        pltpu.make_async_copy(g1a.at[:, z, y], g1a.at[:, z, y], lsem.at[3]).wait()
        pltpu.make_async_copy(g1b.at[:, z, y], g1b.at[:, z, y], lsem.at[4]).wait()
        for one in rest:
            one.start()
        for copy in vectors:
            copy.wait()

    for ahead in (0, 1, 3, 2):
        with scope("own%d" % ahead):
            fast[0].first_arrive(ahead)
            for one in fast:
                one.send_two(ahead)
    for ahead in (0, 1, 3, 2):
        for one in fast:
            one.send_one(ahead)
    with scope("leap"):
        for one in rest:
            one.go_on()
    for ahead in (0, 1, 3, 2):
        with scope("on%d" % ahead):
            for back in (False, True):
                fast[0].arrive(ahead, back)
                for one in fast:
                    one.send_on(ahead, back)
    with scope("tokens"):
        for distance in (1, 3, 2):
            tok_copy(distance, tok_from(distance) + c, {X: around(x + distance, NX)}).wait_recv()
            tok_copy(0, tok_from(distance) + c, {C: other}).start()
    with scope("rest"):
        for one in rest:
            one.arrive()
    start(1)
    start(2)
    start(3)
    with scope("tokens2"):
        four = xg.at[pl.ds(0, NX)]
        remote(four, four, ts.at[0], tr.at[0], {C: other}).wait_recv()
    with scope("scale"):
        squares = jnp.zeros((T, 1), F32)
        for k in range(2 * NX):
            block = xg[k].astype(F32)
            squares = squares + jnp.sum(block * block, axis=1, keepdims=True)
            at = slice(k * (D // (2 * NX)), (k + 1) * (D // (2 * NX)))
            sc[:, at] = (block * ngain[:, at]).astype(BF16)
        inv_rms = lax.rsqrt(squares * (1.0 / D) + EPS)
        more = lax.dot_general(
            extra[...],
            jnp.ones((1, DK), F32),
            (((0,), (0,)), ((), ())),
            precision=lax.Precision.HIGHEST,
            preferred_element_type=F32,
        )
        row = lax.broadcasted_iota(jnp.int32, (T, T), 0)
        col = lax.broadcasted_iota(jnp.int32, (T, T), 1)
        lower = jnp.where(row >= col, 1.0, 0.0).astype(BF16)
    with scope("finish"):
        fast[0].finish()

    with scope("proj_fv"):
        scaled = sc[...]
        forget = (mm(scaled, g0a[...].reshape(D, DK)) * inv_rms).astype(BF16).astype(F32)
        value = (mm(scaled, g0b[...].reshape(D, DK)) * inv_rms).astype(BF16)
    with scope("gates"):
        r = rate[...]
        series = r * (1.0 - r / 2 * (1.0 - r / 3 * (1.0 - r / 4 * (1.0 - r / 5 * (1.0 - r / 6)))))
        reach = jnp.where(r < 0.1, series, 1.0 - jnp.exp(-r))
        key = reach * (1.0 / (1.0 + jnp.exp(forget)))
        logs = jnp.log1p(-key) + more
        cum = mm(lower, jnp.concatenate(thirds(logs), axis=1))
        cum = cum[:, :DK] + (cum[:, DK : 2 * DK] + cum[:, 2 * DK :])
        last = cum[T - 1 : T, :]
        hi, low = halves(key * jnp.exp(last - cum))
        memory = mm(value, hi, 0, 0) + mm(value, low, 0, 0)
        st_out[:, 0:16] = memory.astype(BF16).reshape(NR, 16, DK)
        st_out[:, 16:32] = jnp.broadcast_to(log_rows(last)[None], (NR, 16, DK))

    to_slices = Direct(st1, Y, y, ss.at[0], sr.at[0], st_out)
    over_z = Direct(st2, Z, z, ss.at[1], sr.at[1])
    back = Direct(st3, Y, y, ss.at[2], sr.at[2], st3_out)
    to_slices.start()
    st1[y] = st_out[y]
    relay(1, 0)
    relay(2, 0)
    relay(3, 0)
    relay(1, 1)
    with scope("wait_y"):
        to_slices.arrive()
    with scope("chain_y"):
        state, total = jnp.zeros((16, DK), F32), jnp.zeros((1, DK), F32)
        inside, before = [], []
        for k in range(NR):
            inside.append(state)
            before.append(total)
            new_state, new_total = from_message(st1, k)
            state = jnp.exp(new_total) * state + new_state
            total = total + new_total
        st2[z] = jnp.concatenate([state.astype(BF16), log_rows(total)], axis=0)
    over_z.start()
    relay(2, 1)
    relay(3, 1)
    relay(1, 2)
    with scope("wait_z"):
        over_z.arrive()
    with scope("chain_z"):
        state = jnp.zeros((16, DK), F32)
        outer = state
        for k in range(NR):
            new_state, new_total = from_message(st2, k)
            state = jnp.exp(new_total) * state + new_state
            outer = jnp.where(k < z, state, outer)
        for k in range(NR):
            st3_out[k] = (jnp.exp(before[k]) * outer + inside[k]).astype(BF16)
    back.start()
    st3[y] = st3_out[y]
    relay(2, 2)
    relay(1, 3)
    with scope("proj_p"):
        pool = (mm(scaled, g1b[0].reshape(D, DK)) * inv_rms).astype(BF16)
        rows_out[...] = pool[T - 16 :, :]
    shift = remote(rows_out, rows_in, ps.at[0], pr.at[0], {Z: after_z, Y: after_y})
    shift.start()
    relay(3, 2)
    with scope("proj_q"):
        query = (mm(scaled, g1a[0].reshape(D, DK)) * inv_rms).astype(BF16)
        query = query.astype(F32) * DK ** (-0.5)
    with scope("diag"):
        value32 = value.astype(F32)
        in_block = lax.rem(lax.broadcasted_iota(jnp.int32, (T, 1), 0), 8)
        decay = jnp.exp(logs)
        weight = query
        rec = jnp.sum(query * key, axis=1, keepdims=True) * value32
        for d in range(1, 8):
            weight = weight * (decay if d == 1 else pltpu.roll(decay, d - 1, 0))
            score = jnp.sum(weight * pltpu.roll(key, d, 0), axis=1, keepdims=True)
            rec = rec + jnp.where(in_block >= d, score, 0.0) * pltpu.roll(value32, d, 0)
    with scope("levels"):
        scores = jnp.zeros((T, T), F32)
        for half in (8, 16, 32, 64, 128):
            apart = cum.reshape(T // (2 * half), 2 * half, DK)
            apart = jnp.abs(apart - apart[:, half - 1 : half, :]).reshape(T, DK)
            fade = jnp.exp(-apart)
            level = mm((query * fade).astype(BF16), (key * fade).astype(BF16), 1, 1)
            mask = (row // (2 * half) == col // (2 * half)) & (row // half > col // half)
            scores = jnp.where(mask, level, scores)
        rec = rec + mm2(scores, value)
    relay(2, 3)
    with scope("proj_rg"):
        rgate = (mm(scaled, g1a[1].reshape(D, DK)) * inv_rms).astype(BF16).astype(F32)
        pgate = (mm(scaled, g1b[1].reshape(D, DK)) * inv_rms).astype(BF16).astype(F32)
        gate = sgain[...] * silu(rgate)
    with scope("pool"):
        shift.wait_recv()
        at_start = (z == 0) & (y == 0)
        earlier = jnp.where(at_start, 0.0, rows_in[...].astype(F32))
        pool32 = pool.astype(F32)
        two = jnp.concatenate([earlier, pool32], axis=0)
        two = two + pltpu.roll(two, 1, 0)
        four = two + pltpu.roll(two, 2, 0)
        eight = four + pltpu.roll(four, 4, 0)
        sixteen = eight + pltpu.roll(eight, 8, 0)
        kind = lax.rem(tp, 4)
        sums = jnp.where(kind == 2, eight, sixteen)
        sums = jnp.where(kind == 0, two, jnp.where(kind == 1, four, sums))
        width = jnp.where(kind == 0, 2, jnp.where(kind == 1, 4, jnp.where(kind == 2, 8, 16)))
        place = (z * NR + y) * T + lax.broadcasted_iota(jnp.int32, (T, 1), 0)
        count = jnp.minimum(place + 1, width).astype(F32)
        mixed = (sums[16:] / count - pool32).astype(BF16)
        mapped = mm(mixed, pmix[...]) * pgain[...]
        faded = query * jnp.exp(cum)
        y_pool = (mapped * silu(pgate)).astype(BF16)
    relay(3, 3)
    half_d = D // 2

    def project(left, weight, side):
        at = slice(side * (NR // 2), (side + 1) * (NR // 2))
        return mm(left, weight[2, at].reshape(half_d, DK), 1, 1)

    with scope("pooled"):
        yb[...] = y_pool.reshape(NX, 2, OWN, DK)
        for k, parity in enumerate((other, c)):
            for side in range(2):
                early[k, side] = project(yb[:, parity].reshape(NX * OWN, DK), g1b, side)
    with scope("wait_back"):
        back.arrive()
    with scope("rec"):
        rec = rec + mm2(faded, st3[...].reshape(DK, DK), 1, 1)
        normed = rec * lax.rsqrt(jnp.mean(rec * rec, axis=1, keepdims=True) + EPS)
        y_rec = (normed * gate).astype(BF16)
        yb[...] = y_rec.reshape(NX, 2, OWN, DK)

    def sib_copy(side):
        return remote(sib_out.at[side], sib_in.at[side], bs.at[0], br.at[side], {C: other})

    def red_copy(at, src, dst, step):
        return remote(src, dst, xs.at[0], xr.at[at], {X: around(x + step, NX)})

    right, left, across = around(x + 1, NX), around(x - 1, NX), around(x + 2, NX)
    steps = (1, -1)
    piece = [pl.ds(0, OWN // 2), pl.ds(OWN // 2, OWN // 2)]
    over = [
        [red_copy(2 * k + u, red_out.at[k, across, piece[u]], mid_in.at[k, piece[u]], steps[k]) for u in range(2)]
        for k in range(2)
    ]
    near = [red_copy(4, red_out.at[1 - k, (right, left)[k]], red_in.at[k], steps[k]) for k in range(2)]
    merged = [
        [
            red_copy(4, red_out.at[k, (right, left)[k], piece[u]], red_in.at[2 + k, piece[u]], steps[k])
            for u in range(2)
        ]
        for k in range(2)
    ]
    with scope("proj_sib"):
        for side in range(2):
            part = early[0, side] + project(yb[:, other].reshape(NX * OWN, DK), g1a, side)
            sib_out[side] = part.astype(BF16).reshape(NX, OWN, half_d)
            sib_copy(side).start()
    with scope("proj_mine"):
        for side in range(2):
            part = early[1, side] + project(yb[:, c].reshape(NX * OWN, DK), g1a, side)
            part = part.reshape(NX, OWN, half_d)
            sib_copy(side).wait_recv()
            red_out[side] = (part + sib_in[side].astype(F32)).astype(BF16)
            for u in range(2):
                over[side][u].start()
        for k in range(2):
            near[k].start()
    with scope("red_mid"):
        for u in range(2):
            for k in range(2):
                over[k][u].wait_recv()
                place = (right, left)[k]
                red_out[k, place, piece[u]] = (
                    red_out[k, place, piece[u]].astype(F32) + mid_in[k, piece[u]].astype(F32)
                ).astype(BF16)
                merged[k][u].start()
    with scope("red_wait"):
        red_copy(4, red_in, red_in, 1).wait_recv()
    with scope("final"):
        low = red_out[0, x].astype(F32) + red_in[2].astype(F32) + red_in[1].astype(F32)
        high = red_out[1, x].astype(F32) + red_in[0].astype(F32) + red_in[3].astype(F32)
        squares = jnp.sum(low * low, axis=1, keepdims=True) + jnp.sum(high * high, axis=1, keepdims=True)
        scale = lax.rsqrt(squares * (1.0 / D) + EPS)
        out[:, :half_d] = (low * scale * post[:, :half_d]).astype(BF16)
        out[:, half_d:] = (high * scale * post[:, half_d:]).astype(BF16)

    with scope("drain"):
        for one in [one for pair in streams for one in pair] + rest + [to_slices, over_z, back]:
            one.drain()
        seven = xg.at[pl.ds(0, 2 * NX - 1)]
        remote(seven, seven, ts.at[0], tr.at[0], {C: other}).wait_send()
        remote(sib_out, sib_out, bs.at[0], br.at[0], {C: other}).wait_send()
        six = red_out.at[:, pl.ds(0, NX - 1)]
        remote(six, six, xs.at[0], xr.at[0], {X: right}).wait_send()
        shift.wait_send()


def per_device(
    tokens_in, norm_gain, w_query, w_forget, w_input, w_rgate, w_pool_in, w_pgate,
    floor_rate, extra_logdecay, state_gain, pool_mix, pool_gain, out_rec, out_pool, post_gain,
):
    anywhere = pl.BlockSpec(memory_space=pl.ANY)
    dma = pltpu.SemaphoreType.DMA
    rows = D // 64
    run = pl.pallas_call(
        layer,
        name="layer",
        out_shape=jax.ShapeDtypeStruct((OWN, D), BF16),
        in_specs=[anywhere] * 16,
        out_specs=pl.BlockSpec(memory_space=pltpu.VMEM),
        scratch_shapes=[
            pltpu.VMEM((NR, NR, rows, DK), BF16),
            pltpu.VMEM((NR, NR, rows, DK), BF16),
            pltpu.VMEM((3, NR, NR, rows, DK), BF16),
            pltpu.VMEM((3, NR, NR, rows, DK), BF16),
            pltpu.VMEM((2 * NX, T, D // (2 * NX)), BF16),
            pltpu.VMEM((T, D), BF16),
            pltpu.VMEM((1, D), F32),
            pltpu.VMEM((1, DK), F32),
            pltpu.VMEM((1, T), F32),
            pltpu.VMEM((1, DK), F32),
            pltpu.VMEM((DK, DK), BF16),
            pltpu.VMEM((1, DK), F32),
            pltpu.VMEM((1, D), F32),
            pltpu.VMEM((NR, 32, DK), BF16),
            pltpu.VMEM((NR, 32, DK), BF16),
            pltpu.VMEM((NR, 32, DK), BF16),
            pltpu.VMEM((NR, 16, DK), BF16),
            pltpu.VMEM((NR, 16, DK), BF16),
            pltpu.VMEM((16, DK), BF16),
            pltpu.VMEM((16, DK), BF16),
            pltpu.VMEM((NX, 2, OWN, DK), BF16),
            pltpu.VMEM((2, 2, NX * OWN, D // 2), F32),
            pltpu.VMEM((2, NX, OWN, D // 2), BF16),
            pltpu.VMEM((2, NX, OWN, D // 2), BF16),
            pltpu.VMEM((2, NX, OWN, D // 2), BF16),
            pltpu.VMEM((4, OWN, D // 2), BF16),
            pltpu.VMEM((2, OWN, D // 2), BF16),
            dma((5,)),
            dma((7,)),
            dma((NR // 2,)),
            dma((13,)),
            dma((4,)),
            dma((2, 3)),
            dma((8,)),
            dma((3, 2 + CUTS * (NR - 3))),
            dma((1,)),
            dma((NX,)),
            dma((3,)),
            dma((3,)),
            dma((1,)),
            dma((1,)),
            dma((1,)),
            dma((2,)),
            dma((1,)),
            dma((5,)),
        ],
        compiler_params=pltpu.CompilerParams(
            collective_id=0, has_side_effects=True, vmem_limit_bytes=32 * 1024 * 1024
        ),
    )
    operands = (
        tokens_in,
        w_query,
        w_forget,
        w_input,
        w_rgate,
        w_pool_in,
        w_pgate,
        out_rec.T,
        out_pool.T,
        norm_gain.reshape(1, -1),
        floor_rate.reshape(1, -1),
        extra_logdecay.reshape(1, -1),
        state_gain.reshape(1, -1),
        pool_mix.reshape(DK, DK),
        pool_gain.reshape(1, -1),
        post_gain.reshape(1, -1),
    )
    return run(*[pltpu.with_memory_space_constraint(a, pltpu.HBM) for a in operands])


def solution(mesh):
    torus = Mesh(mesh.devices.reshape(8, 8, 4, 2), ("sp_0", "sp_1", "tp_0", "tp_1"))
    return jax.shard_map(
        per_device,
        mesh=torus,
        in_specs=(
            P(SP, TP),
            P(),
            P(SP, TP),
            P(SP, TP),
            P(SP, TP),
            P(SP, TP),
            P(SP, TP),
            P(SP, TP),
            P(TP),
            P(SP, TP),
            P(TP),
            P(TP, None, None),
            P(TP),
            P(TP, SP),
            P(TP, SP),
            P(),
        ),
        out_specs=P(SP_TP, None),
        check_vma=False,
    )
```

```python
import functools

import jax
import jax.numpy as jnp
from jax import lax
from jax.experimental import pallas as pl
from jax.experimental.pallas import tpu as pltpu
from jax.sharding import Mesh
from jax.sharding import PartitionSpec as P

SP = ("sp_0", "sp_1")
TP = ("tp_0", "tp_1")
SP_TP = ("sp_0", "sp_1", "tp_0", "tp_1")
Z, Y, X, C = "sp_0", "sp_1", "tp_0", "tp_1"
MESH = pl.DeviceIdType.MESH
EPS = 1e-06
DK = 128
NR = 8
NX = 4
T = 256
D = 2048
OWN = T // (2 * NX)
F32 = jnp.float32
BF16 = jnp.bfloat16
CUTS = 2
SPAN = NR // CUTS
ORDER = (4, 3, 5, 2, 6, 1, 7)


def mm(a, b, ca=1, cb=0):
    return lax.dot_general(a, b, (((ca,), (cb,)), ((), ())), preferred_element_type=F32)


def halves(a):
    hi = a.astype(BF16)
    return hi, (a - hi.astype(F32)).astype(BF16)


def mm2(a, b, ca=1, cb=0):
    ah, al = halves(a)
    return mm(ah, b, ca, cb) + mm(al, b, ca, cb)


def silu(a):
    return a / (1.0 + jnp.exp(-a))


def around(value, count):
    return lax.rem(value + 2 * count, count)


def remote(src, dst, send, recv, where):
    return pltpu.make_async_remote_copy(
        src_ref=src, dst_ref=dst, send_sem=send, recv_sem=recv, device_id=where, device_id_type=MESH
    )


class Stream:
    def __init__(self, at, wide, long, w, l, sign, sems):
        self.at, self.wide, self.long, self.w, self.l, self.sign = at, wide, long, w, l, sign
        self.send1, self.send2, self.recv1, self.recv2 = sems

    def drain(self):
        view = self.at(pl.ds(0, NR), pl.ds(0, NR - 1))
        remote(view, view, self.send2, self.send2, {self.long: around(self.l + 1, NR)}).wait_send()

    def origin(self, step, back):
        sign = -self.sign if back else self.sign
        return around(self.l - sign * step, NR)

    def steps(self, back):
        return NR // 2 - 1 if back else NR // 2

    def sem(self, step, back, cut):
        if step == self.steps(back) - 1:
            return self.recv2.at[1 if back else 0]
        return self.recv2.at[2 + CUTS * (NR // 2 - 1 + step if back else step) + cut]

    def copy(self, step, back, cut, origin):
        sign = -self.sign if back else self.sign
        block = self.at(pl.ds(SPAN * cut, SPAN), pl.ds(origin, 1))
        where = {self.long: around(self.l + sign, NR)}
        return remote(block, block, self.send2, self.sem(step, back, cut), where)

    def start(self, step, back, cut):
        if step < self.steps(back):
            self.copy(step, back, cut, self.origin(step, back)).start()

    def arrive(self, step, back, cut):
        last = step == self.steps(back) - 1
        if step < self.steps(back) and (not last or cut == CUTS - 1):
            view = self.at(pl.ds(0, NR), pl.ds(0, 2)) if last else self.at(pl.ds(0, 2 * SPAN), pl.ds(0, 1))
            where = {self.long: around(self.l + self.sign, NR)}
            remote(view, view, self.send2, self.sem(step, back, cut), where).wait_recv()


class Leaps:
    def __init__(self, part, axis, me, sign, send, recv):
        self.part, self.axis, self.me, self.sign, self.send, self.recv = part, axis, me, sign, send, recv

    def copy(self, move, origin, sem, count=1):
        block = self.part(origin, count)
        where = {self.axis: around(self.me + self.sign * move, NR)}
        return remote(block, block, self.send, self.recv.at[sem], where)

    def start(self):
        for move, sem in ((2, 0), (-2, 1), (1, 2), (-1, 2)):
            self.copy(move, self.me, sem).start()

    def go_on(self):
        origin = around(self.me - 2 * self.sign, NR)
        self.copy(2, origin, 0).wait_recv()
        self.copy(2, origin, 2).start()
        self.copy(1, origin, 2).start()
        origin = around(self.me + 2 * self.sign, NR)
        self.copy(-2, origin, 1).wait_recv()
        self.copy(-1, origin, 2).start()

    def arrive(self):
        self.copy(1, 0, 2, 5).wait_recv()

    def drain(self):
        self.copy(1, 0, 2, 7).wait_send()


class FastStream(Stream):
    def drain(self):
        view = self.at(pl.ds(0, NR - 1), pl.ds(self.l, 1))
        remote(view, view, self.send1, self.send1, {self.wide: around(self.w + 1, NR)}).wait_send()
        Stream.drain(self)

    def first_start(self):
        pair, twin = self.w // 2, self.w + 1 - 2 * lax.rem(self.w, 2)
        block = self.at(pl.ds(self.w, 1), pl.ds(self.l, 1))
        remote(block, block, self.send1, self.recv1.at[0], {self.wide: twin}).start()
        for ahead in (2, 1, 3):
            for k in range(2):
                place = 2 * lax.rem(pair + ahead, NR // 2) + k
                remote(block, block, self.send1, self.recv1.at[NR // 2 - ahead], {self.wide: place}).start()

    def pair_at(self, ahead):
        return 2 * lax.rem(self.w // 2 + ahead, NR // 2)

    def wait(self, view, sem):
        where = {self.long: around(self.l + self.sign, NR)}
        remote(view, view, self.send2, sem, where).wait_recv()

    def first_arrive(self, ahead):
        self.wait(self.at(pl.ds(0, 4 if ahead else 2), pl.ds(0, 1)), self.recv1.at[ahead])

    def arrive(self, ahead, back):
        self.wait(self.at(pl.ds(0, 4), pl.ds(0, 1)), self.recv2.at[(9 if back else 5) + ahead])

    def finish(self):
        for sem in (0, 3, 1, 4, 2):
            self.wait(self.at(pl.ds(0, NR), pl.ds(0, 2)), self.recv2.at[sem])

    def hop(self, ahead, origin, move, sem):
        block = self.at(pl.ds(self.pair_at(ahead), 2), pl.ds(origin, 1))
        where = {self.long: around(self.l + self.sign * move, NR)}
        return remote(block, block, self.send2, self.recv2.at[sem], where)

    def send_two(self, ahead):
        self.hop(ahead, self.l, 2, 5 + ahead).start()
        self.hop(ahead, self.l, -2, 9 + ahead).start()

    def send_one(self, ahead):
        self.hop(ahead, self.l, 1, 0).start()
        self.hop(ahead, self.l, -1, 3).start()

    def send_on(self, ahead, back):
        if back:
            self.hop(ahead, around(self.l + 2 * self.sign, NR), -1, 4).start()
        else:
            origin = around(self.l - 2 * self.sign, NR)
            self.hop(ahead, origin, 2, 2).start()
            self.hop(ahead, origin, 1, 1).start()


class Direct:
    def __init__(self, held, axis, me, send, recv, out=None):
        self.out, self.held, self.axis, self.me, self.send, self.recv = out, held, axis, me, send, recv

    def start(self):
        for distance in ORDER:
            place = around(self.me + distance, NR)
            src = self.held.at[self.me] if self.out is None else self.out.at[place]
            remote(src, self.held.at[self.me], self.send, self.recv, {self.axis: place}).start()

    def whole(self):
        view = self.held.at[pl.ds(0, NR - 1)]
        return remote(view, view, self.send, self.recv, {self.axis: around(self.me + 1, NR)})

    def arrive(self):
        self.whole().wait_recv()

    def drain(self):
        self.whole().wait_send()


def thirds(a):
    hi = a.astype(BF16)
    rest = a - hi.astype(F32)
    mid = rest.astype(BF16)
    return hi, mid, (rest - mid.astype(F32)).astype(BF16)


def log_rows(total):
    hi, mid, low = thirds(total)
    place = lax.broadcasted_iota(jnp.int32, (8, DK), 0)
    parts = jnp.where(place == 1, mid.astype(F32), jnp.where(place == 2, low.astype(F32), 0.0))
    return jnp.where(place == 0, hi.astype(F32), parts).astype(BF16)


def from_message(ref, k):
    whole = ref[k].astype(F32)
    return whole[:16], jnp.sum(whole[16:], axis=0, keepdims=True)


def layer(
    tok, wq, wf, wi, wr, wp, wg, orec, opool,
    ngain_in, rate_in, extra_in, sgain_in, pmix_in, pgain_in, post_in,
    out,
    g0a, g0b, g1a, g1b, xg, sc,
    ngain, rate, extra, sgain, pmix, pgain, post,
    st_out, st1, st2, st3_out, st3, rows_out, rows_in, yb, yo, yi, early, o2a, o2b, red_out, red_in, mid_in,
    lsem, vsem, f1r, f2r, p1s, p1r, p2s, p2r, ts, tr, ss, sr, ps, pr, bs, br, cs, cr, xs, xr,
):
    scope = jax.named_scope
    z, y, x, c = lax.axis_index(Z), lax.axis_index(Y), lax.axis_index(X), lax.axis_index(C)
    tp = 2 * x + c
    sign = 1 - 2 * c
    other = 1 - c

    after_y = around(y + 1, NR)
    after_z = jnp.where(y == NR - 1, around(z + 1, NR), z)
    before_y = around(y - 1, NR)
    before_z = jnp.where(y == 0, around(z - 1, NR), z)
    with scope("barrier"):
        barrier = pltpu.get_barrier_semaphore()
        for k in ORDER:
            pl.semaphore_signal(barrier, 1, device_id={Y: around(y + k, NR)}, device_id_type=MESH)
            pl.semaphore_signal(barrier, 1, device_id={Z: around(z + k, NR)}, device_id_type=MESH)
        for k in range(1, NX):
            pl.semaphore_signal(barrier, 1, device_id={X: around(x + k, NX)}, device_id_type=MESH)
        pl.semaphore_signal(barrier, 1, device_id={C: other}, device_id_type=MESH)
        pl.semaphore_signal(barrier, 1, device_id={Z: before_z, Y: before_y}, device_id_type=MESH)

    local = [
        pltpu.make_async_copy(src, dst, lsem.at[k])
        for k, src, dst in (
            (0, wf, g0a.at[z, y]),
            (1, wi, g0b.at[z, y]),
            (2, tok, xg.at[tp]),
            (3, wq, g1a.at[0, z, y]),
            (3, wr, g1a.at[1, z, y]),
            (3, orec, g1a.at[2, z, y]),
            (4, wp, g1b.at[0, z, y]),
            (4, wg, g1b.at[1, z, y]),
            (4, opool, g1b.at[2, z, y]),
        )
    ]
    vectors = [
        pltpu.make_async_copy(src, dst, vsem.at[k])
        for k, (src, dst) in enumerate(
            (
                (ngain_in, ngain),
                (rate_in, rate),
                (extra_in, extra),
                (sgain_in, sgain),
                (pmix_in, pmix),
                (pgain_in, pgain),
                (post_in, post),
            )
        )
    ]
    for copy in local + vectors:
        copy.start()
    with scope("barrier"):
        pl.semaphore_wait(barrier, 2 * (NR - 1) + NX - 1 + 2)

    def stream(kind, buffer, flip, at, recv1, recv2):
        sems = (p1s.at[flip], p2s.at[at], recv1, recv2)
        if flip:
            return kind(lambda w, l: buffer.at[w, l], Z, Y, z, y, sign, sems)
        return kind(lambda w, l: buffer.at[l, w], Y, Z, y, z, sign, sems)

    fast = [
        stream(FastStream, buffer, flip, flip, f1r, f2r)
        for flip, buffer in enumerate((g0a, g0b))
    ]
    streams = [fast] + [
        [
            stream(Stream, buffer.at[k], flip, 2 * k + 2 + flip, None, p2r.at[k])
            for flip, buffer in enumerate((g1a, g1b))
        ]
        for k in range(3)
    ]
    rest = [
        Leaps(lambda o, n: g1a.at[:, z, pl.ds(o, n)], Y, y, sign, p1s.at[2], p1r.at[0]),
        Leaps(lambda o, n: g1b.at[:, pl.ds(o, n), y], Z, z, sign, p1s.at[3], p1r.at[1]),
    ]

    def start(k):
        with scope("first%d" % k):
            for cut in range(CUTS):
                for back in (False, True):
                    for one in streams[k]:
                        one.start(0, back, cut)

    def relay(k, step):
        with scope("relay%d%d" % (k, step)):
            for cut in range(CUTS):
                for back in (False, True):
                    streams[k][0].arrive(step, back, cut)
                    for one in streams[k]:
                        one.start(step + 1, back, cut)

    def pass_on(step):
        for k, (src, dst) in enumerate(((g1a, o2a), (g1b, o2b))):
            me = (z, y)[k]
            for move in sorted({step, -step}) if step < NR // 2 else [step * sign]:
                o = around(me + move, NR)
                place = (2, o) if k == 0 else (2, slice(None), o)
                to = (o,) if k == 0 else (slice(None), o)
                remote(src.at[place], dst.at[to], cs.at[k], cr.at[k], {C: other}).start()

    def tok_copy(at, slot, where):
        return remote(xg.at[slot], xg.at[slot], ts.at[0], tr.at[at], where)

    def tok_from(distance):
        return 2 * around(x - distance, NX)

    with scope("sends"):
        local[0].wait()
        fast[0].first_start()
        local[1].wait()
        fast[1].first_start()
        local[2].wait()
        for distance in (2, 1, 3):
            tok_copy(distance, tp, {X: around(x + distance, NX)}).start()
        tok_copy(0, tp, {C: other}).start()
        pltpu.make_async_copy(g1a.at[:, z, y], g1a.at[:, z, y], lsem.at[3]).wait()
        pltpu.make_async_copy(g1b.at[:, z, y], g1b.at[:, z, y], lsem.at[4]).wait()
        for one in rest:
            one.start()
        for copy in vectors:
            copy.wait()

    for ahead in (0, 1, 3, 2):
        with scope("own%d" % ahead):
            fast[0].first_arrive(ahead)
            for one in fast:
                one.send_two(ahead)
    for ahead in (0, 1, 3, 2):
        for one in fast:
            one.send_one(ahead)
    with scope("leap"):
        for one in rest:
            one.go_on()
    for ahead in (0, 1, 3, 2):
        with scope("on%d" % ahead):
            for back in (False, True):
                fast[0].arrive(ahead, back)
                for one in fast:
                    one.send_on(ahead, back)
    with scope("tokens"):
        for distance in (1, 3, 2):
            tok_copy(distance, tok_from(distance) + c, {X: around(x + distance, NX)}).wait_recv()
            tok_copy(0, tok_from(distance) + c, {C: other}).start()
    with scope("rest"):
        for one in rest:
            one.arrive()
    start(1)
    start(2)
    start(3)
    pass_on(0)
    with scope("tokens2"):
        four = xg.at[pl.ds(0, NX)]
        remote(four, four, ts.at[0], tr.at[0], {C: other}).wait_recv()
    with scope("scale"):
        squares = jnp.zeros((T, 1), F32)
        for k in range(2 * NX):
            block = xg[k].astype(F32)
            squares = squares + jnp.sum(block * block, axis=1, keepdims=True)
            at = slice(k * (D // (2 * NX)), (k + 1) * (D // (2 * NX)))
            sc[:, at] = (block * ngain[:, at]).astype(BF16)
        inv_rms = lax.rsqrt(squares * (1.0 / D) + EPS)
        more = lax.dot_general(
            extra[...],
            jnp.ones((1, DK), F32),
            (((0,), (0,)), ((), ())),
            precision=lax.Precision.HIGHEST,
            preferred_element_type=F32,
        )
        row = lax.broadcasted_iota(jnp.int32, (T, T), 0)
        col = lax.broadcasted_iota(jnp.int32, (T, T), 1)
        lower = jnp.where(row >= col, 1.0, 0.0).astype(BF16)
    with scope("finish"):
        fast[0].finish()

    with scope("proj_fv"):
        scaled = sc[...]
        forget = (mm(scaled, g0a[...].reshape(D, DK)) * inv_rms).astype(BF16).astype(F32)
        value = (mm(scaled, g0b[...].reshape(D, DK)) * inv_rms).astype(BF16)
    with scope("gates"):
        r = rate[...]
        series = r * (1.0 - r / 2 * (1.0 - r / 3 * (1.0 - r / 4 * (1.0 - r / 5 * (1.0 - r / 6)))))
        reach = jnp.where(r < 0.1, series, 1.0 - jnp.exp(-r))
        key = reach * (1.0 / (1.0 + jnp.exp(forget)))
        logs = jnp.log1p(-key) + more
        cum = mm(lower, jnp.concatenate(thirds(logs), axis=1))
        cum = cum[:, :DK] + (cum[:, DK : 2 * DK] + cum[:, 2 * DK :])
        last = cum[T - 1 : T, :]
        hi, low = halves(key * jnp.exp(last - cum))
        memory = mm(value, hi, 0, 0) + mm(value, low, 0, 0)
        st_out[:, 0:16] = memory.astype(BF16).reshape(NR, 16, DK)
        st_out[:, 16:24] = jnp.broadcast_to(log_rows(last)[None], (NR, 8, DK))

    to_slices = Direct(st1, Y, y, ss.at[0], sr.at[0], st_out)
    over_z = Direct(st2, Z, z, ss.at[1], sr.at[1])
    back = Direct(st3, Y, y, ss.at[2], sr.at[2], st3_out)
    to_slices.start()
    st1[y] = st_out[y]
    relay(1, 0)
    relay(2, 0)
    relay(3, 0)
    pass_on(1)
    relay(1, 1)
    with scope("wait_y"):
        to_slices.arrive()
    with scope("chain_y"):
        state, total = jnp.zeros((16, DK), F32), jnp.zeros((1, DK), F32)
        inside, before = [], []
        for k in range(NR):
            inside.append(state)
            before.append(total)
            new_state, new_total = from_message(st1, k)
            state = jnp.exp(new_total) * state + new_state
            total = total + new_total
        st2[z] = jnp.concatenate([state.astype(BF16), log_rows(total)], axis=0)
    over_z.start()
    relay(2, 1)
    relay(3, 1)
    pass_on(2)
    relay(1, 2)
    with scope("wait_z"):
        over_z.arrive()
    with scope("chain_z"):
        state = jnp.zeros((16, DK), F32)
        outer = state
        for k in range(NR):
            new_state, new_total = from_message(st2, k)
            state = jnp.exp(new_total) * state + new_state
            outer = jnp.where(k < z, state, outer)
        for k in range(NR):
            st3_out[k] = (jnp.exp(before[k]) * outer + inside[k]).astype(BF16)
    back.start()
    st3[y] = st3_out[y]
    relay(2, 2)
    relay(1, 3)
    with scope("proj_p"):
        pool = (mm(scaled, g1b[0].reshape(D, DK)) * inv_rms).astype(BF16)
        rows_out[...] = pool[T - 16 :, :]
    shift = remote(rows_out, rows_in, ps.at[0], pr.at[0], {Z: after_z, Y: after_y})
    shift.start()
    relay(3, 2)
    pass_on(3)
    with scope("proj_q"):
        query = (mm(scaled, g1a[0].reshape(D, DK)) * inv_rms).astype(BF16)
        query = query.astype(F32) * DK ** (-0.5)
    with scope("diag"):
        value32 = value.astype(F32)
        in_block = lax.rem(lax.broadcasted_iota(jnp.int32, (T, 1), 0), 8)
        decay = jnp.exp(logs)
        weight = query
        rec = jnp.sum(query * key, axis=1, keepdims=True) * value32
        for d in range(1, 8):
            weight = weight * (decay if d == 1 else pltpu.roll(decay, d - 1, 0))
            score = jnp.sum(weight * pltpu.roll(key, d, 0), axis=1, keepdims=True)
            rec = rec + jnp.where(in_block >= d, score, 0.0) * pltpu.roll(value32, d, 0)
    with scope("levels"):
        scores = jnp.zeros((T, T), F32)
        for half in (8, 16, 32, 64, 128):
            apart = cum.reshape(T // (2 * half), 2 * half, DK)
            apart = jnp.abs(apart - apart[:, half - 1 : half, :]).reshape(T, DK)
            fade = jnp.exp(-apart)
            level = mm((query * fade).astype(BF16), (key * fade).astype(BF16), 1, 1)
            mask = (row // (2 * half) == col // (2 * half)) & (row // half > col // half)
            scores = jnp.where(mask, level, scores)
        rec = rec + mm2(scores, value)
    relay(2, 3)
    with scope("proj_rg"):
        rgate = (mm(scaled, g1a[1].reshape(D, DK)) * inv_rms).astype(BF16).astype(F32)
        pgate = (mm(scaled, g1b[1].reshape(D, DK)) * inv_rms).astype(BF16).astype(F32)
        gate = sgain[...] * silu(rgate)
    with scope("pool"):
        shift.wait_recv()
        at_start = (z == 0) & (y == 0)
        earlier = jnp.where(at_start, 0.0, rows_in[...].astype(F32))
        pool32 = pool.astype(F32)
        two = jnp.concatenate([earlier, pool32], axis=0)
        two = two + pltpu.roll(two, 1, 0)
        four = two + pltpu.roll(two, 2, 0)
        eight = four + pltpu.roll(four, 4, 0)
        sixteen = eight + pltpu.roll(eight, 8, 0)
        kind = lax.rem(tp, 4)
        sums = jnp.where(kind == 2, eight, sixteen)
        sums = jnp.where(kind == 0, two, jnp.where(kind == 1, four, sums))
        width = jnp.where(kind == 0, 2, jnp.where(kind == 1, 4, jnp.where(kind == 2, 8, 16)))
        place = (z * NR + y) * T + lax.broadcasted_iota(jnp.int32, (T, 1), 0)
        count = jnp.minimum(place + 1, width).astype(F32)
        mixed = (sums[16:] / count - pool32).astype(BF16)
        mapped = mm(mixed, pmix[...]) * pgain[...]
        faded = query * jnp.exp(cum)
        y_pool = (mapped * silu(pgate)).astype(BF16)
    relay(3, 3)
    pass_on(4)
    half_d = D // 2

    def project(left, weight, side):
        at = slice(side * (NR // 2), (side + 1) * (NR // 2))
        return mm(left.reshape(NX * OWN, DK), weight[at].reshape(half_d, DK), 1, 1)

    def rows_copy(k):
        return remote(yo.at[k], yi.at[k], bs.at[k], br.at[k], {C: other})

    def give(k, value):
        yb[k] = value.reshape(NX, 2, OWN, DK)
        yo[k] = yb[k, :, other]
        rows_copy(k).start()

    with scope("pooled"):
        give(0, y_pool)
        for side in range(2):
            early[side] = project(yb[0, :, c], g1b.at[2], side)
    with scope("wait_back"):
        back.arrive()
    with scope("rec"):
        rec = rec + mm2(faded, st3[...].reshape(DK, DK), 1, 1)
        normed = rec * lax.rsqrt(jnp.mean(rec * rec, axis=1, keepdims=True) + EPS)
        y_rec = (normed * gate).astype(BF16)
        give(1, y_rec)

    def red_copy(at, src, dst, step):
        return remote(src, dst, xs.at[0], xr.at[at], {X: around(x + step, NX)})

    right, left, across = around(x + 1, NX), around(x - 1, NX), around(x + 2, NX)
    steps = (1, -1)
    piece = [pl.ds(0, OWN // 2), pl.ds(OWN // 2, OWN // 2)]
    over = [
        [red_copy(2 * k + u, red_out.at[k, across, piece[u]], mid_in.at[k, piece[u]], steps[k]) for u in range(2)]
        for k in range(2)
    ]
    near = [red_copy(4, red_out.at[1 - k, (right, left)[k]], red_in.at[k], steps[k]) for k in range(2)]
    merged = [
        [
            red_copy(4, red_out.at[k, (right, left)[k], piece[u]], red_in.at[2 + k, piece[u]], steps[k])
            for u in range(2)
        ]
        for k in range(2)
    ]
    with scope("proj_mine"):
        for side in range(2):
            early[side] = early[side] + project(yb[1, :, c], g1a.at[2], side)
    with scope("pooled_sib"):
        remote(o2b, o2b, cs.at[1], cr.at[1], {C: other}).wait_recv()
        rows_copy(0).wait_recv()
        for side in range(2):
            early[side] = early[side] + project(yi[0], o2b, side)
    with scope("proj_sib"):
        remote(o2a, o2a, cs.at[0], cr.at[0], {C: other}).wait_recv()
        rows_copy(1).wait_recv()
        for side in range(2):
            part = early[side] + project(yi[1], o2a, side)
            red_out[side] = part.astype(BF16).reshape(NX, OWN, half_d)
            for u in range(2):
                over[side][u].start()
        for k in range(2):
            near[k].start()
    with scope("red_mid"):
        for u in range(2):
            for k in range(2):
                over[k][u].wait_recv()
                place = (right, left)[k]
                red_out[k, place, piece[u]] = (
                    red_out[k, place, piece[u]].astype(F32) + mid_in[k, piece[u]].astype(F32)
                ).astype(BF16)
                merged[k][u].start()
    with scope("red_wait"):
        red_copy(4, red_in, red_in, 1).wait_recv()
    with scope("final"):
        low = red_out[0, x].astype(F32) + red_in[2].astype(F32) + red_in[1].astype(F32)
        high = red_out[1, x].astype(F32) + red_in[0].astype(F32) + red_in[3].astype(F32)
        squares = jnp.sum(low * low, axis=1, keepdims=True) + jnp.sum(high * high, axis=1, keepdims=True)
        scale = lax.rsqrt(squares * (1.0 / D) + EPS)
        out[:, :half_d] = (low * scale * post[:, :half_d]).astype(BF16)
        out[:, half_d:] = (high * scale * post[:, half_d:]).astype(BF16)

    with scope("drain"):
        for one in [one for pair in streams for one in pair] + rest + [to_slices, over_z, back]:
            one.drain()
        seven = xg.at[pl.ds(0, 2 * NX - 1)]
        remote(seven, seven, ts.at[0], tr.at[0], {C: other}).wait_send()
        for k in range(2):
            rows_copy(k).wait_send()
        remote(o2a, o2a, cs.at[0], cr.at[0], {C: other}).wait_send()
        remote(o2b, o2b, cs.at[1], cr.at[1], {C: other}).wait_send()
        six = red_out.at[:, pl.ds(0, NX - 1)]
        remote(six, six, xs.at[0], xr.at[0], {X: right}).wait_send()
        shift.wait_send()


def per_device(
    tokens_in, norm_gain, w_query, w_forget, w_input, w_rgate, w_pool_in, w_pgate,
    floor_rate, extra_logdecay, state_gain, pool_mix, pool_gain, out_rec, out_pool, post_gain,
):
    anywhere = pl.BlockSpec(memory_space=pl.ANY)
    dma = pltpu.SemaphoreType.DMA
    rows = D // 64
    run = pl.pallas_call(
        layer,
        name="layer",
        out_shape=jax.ShapeDtypeStruct((OWN, D), BF16),
        in_specs=[anywhere] * 16,
        out_specs=pl.BlockSpec(memory_space=pltpu.VMEM),
        scratch_shapes=[
            pltpu.VMEM((NR, NR, rows, DK), BF16),
            pltpu.VMEM((NR, NR, rows, DK), BF16),
            pltpu.VMEM((3, NR, NR, rows, DK), BF16),
            pltpu.VMEM((3, NR, NR, rows, DK), BF16),
            pltpu.VMEM((2 * NX, T, D // (2 * NX)), BF16),
            pltpu.VMEM((T, D), BF16),
            pltpu.VMEM((1, D), F32),
            pltpu.VMEM((1, DK), F32),
            pltpu.VMEM((1, T), F32),
            pltpu.VMEM((1, DK), F32),
            pltpu.VMEM((DK, DK), BF16),
            pltpu.VMEM((1, DK), F32),
            pltpu.VMEM((1, D), F32),
            pltpu.VMEM((NR, 24, DK), BF16),
            pltpu.VMEM((NR, 24, DK), BF16),
            pltpu.VMEM((NR, 24, DK), BF16),
            pltpu.VMEM((NR, 16, DK), BF16),
            pltpu.VMEM((NR, 16, DK), BF16),
            pltpu.VMEM((16, DK), BF16),
            pltpu.VMEM((16, DK), BF16),
            pltpu.VMEM((2, NX, 2, OWN, DK), BF16),
            pltpu.VMEM((2, NX, OWN, DK), BF16),
            pltpu.VMEM((2, NX, OWN, DK), BF16),
            pltpu.VMEM((2, NX * OWN, D // 2), F32),
            pltpu.VMEM((NR, NR, rows, DK), BF16),
            pltpu.VMEM((NR, NR, rows, DK), BF16),
            pltpu.VMEM((2, NX, OWN, D // 2), BF16),
            pltpu.VMEM((4, OWN, D // 2), BF16),
            pltpu.VMEM((2, OWN, D // 2), BF16),
            dma((5,)),
            dma((7,)),
            dma((NR // 2,)),
            dma((13,)),
            dma((4,)),
            dma((2, 3)),
            dma((8,)),
            dma((3, 2 + CUTS * (NR - 3))),
            dma((1,)),
            dma((NX,)),
            dma((3,)),
            dma((3,)),
            dma((1,)),
            dma((1,)),
            dma((2,)),
            dma((2,)),
            dma((2,)),
            dma((2,)),
            dma((1,)),
            dma((5,)),
        ],
        compiler_params=pltpu.CompilerParams(
            collective_id=0, has_side_effects=True, vmem_limit_bytes=32 * 1024 * 1024
        ),
    )
    operands = (
        tokens_in,
        w_query,
        w_forget,
        w_input,
        w_rgate,
        w_pool_in,
        w_pgate,
        out_rec.T,
        out_pool.T,
        norm_gain.reshape(1, -1),
        floor_rate.reshape(1, -1),
        extra_logdecay.reshape(1, -1),
        state_gain.reshape(1, -1),
        pool_mix.reshape(DK, DK),
        pool_gain.reshape(1, -1),
        post_gain.reshape(1, -1),
    )
    return run(*[pltpu.with_memory_space_constraint(a, pltpu.HBM) for a in operands])


def solution(mesh):
    torus = Mesh(mesh.devices.reshape(8, 8, 4, 2), ("sp_0", "sp_1", "tp_0", "tp_1"))
    return jax.shard_map(
        per_device,
        mesh=torus,
        in_specs=(
            P(SP, TP),
            P(),
            P(SP, TP),
            P(SP, TP),
            P(SP, TP),
            P(SP, TP),
            P(SP, TP),
            P(SP, TP),
            P(TP),
            P(SP, TP),
            P(TP),
            P(TP, None, None),
            P(TP),
            P(TP, SP),
            P(TP, SP),
            P(),
        ),
        out_specs=P(SP_TP, None),
        check_vma=False,
    )
```
